32 devices in a mesh: kv: 16 (over z, y, x), tp: 2 (over core).
Axes of the slice: x: 2, y: 2, z: 4, core: 2. Of those that a mesh axis runs over, the one named last changes fastest.
Arguments:
- tokens: bfloat16 [64, 4096], P(None, 'kv')
- lengths: int32 [16], replicated, may hold values from 1 to 4, 28 in all
- memory: float32 [16, 16, 128, 128], P('kv', 'tp'), may hold values from -0.6 to 0.6
- norm_gain: float32 [4096], P('kv'), may hold values from 0.1 to 1.9
- w_query: bfloat16 [4096, 2048], P('kv', 'tp'), may hold values from -0.09375 to 0.09375
- w_key: bfloat16 [4096, 2048], P('kv', 'tp'), may hold values from -0.09375 to 0.09375
- w_value: bfloat16 [4096, 2048], P('kv', 'tp'), may hold values from -0.09375 to 0.09375
- w_outgate: bfloat16 [4096, 2048], P('kv', 'tp'), may hold values from -0.09375 to 0.09375
- w_alpha: bfloat16 [4096, 16], P('kv'), may hold values from -0.09375 to 0.09375
- w_beta: bfloat16 [4096, 16], P('kv'), may hold values from -0.09375 to 0.09375
- decay_log: float32 [16], P('tp'), may hold values from -4 to 0.5
- decay_bias: float32 [16], P('tp'), may hold values from -1 to 1
- head_gain: float32 [128], replicated, may hold values from 0.1 to 1.9
- w_output: bfloat16 [2048, 4096], P('tp', 'kv'), may hold values from -0.125 to 0.125
- mlp_gain: float32 [4096], P('kv'), may hold values from 0.1 to 1.9
- w_gate: bfloat16 [4096, 11264], P('kv', 'tp'), may hold values from -0.09375 to 0.09375
- w_up: bfloat16 [4096, 11264], P('kv', 'tp'), may hold values from -0.09375 to 0.09375
- w_down: bfloat16 [11264, 4096], P('tp', 'kv'), may hold values from -0.0546875 to 0.0546875
Outputs:
- layer_out: bfloat16 [64, 4096], P(None, 'kv')
- new_memory: float32 [16, 16, 128, 128], P('kv', 'tp')
The draws below stay inside these ranges and needn't reach their ends.
Inputs may be any that keep to these rules, and one draw needn't show every extreme that they name: How many of a sequence's 4 slots hold live tokens; the live ones come first; the lengths add up to seven quarters of 16, rounded down.
All inputs are finite; a program needn't handle non-finite values.
Results may differ from the reference program's by a relative error of at most 0.012.
Values may be sent and summed in bfloat16 or wider, within the bound.
No kernel may reach another device: no remote copies, remote signals or barrier semaphores. Data moves between devices by JAX's collectives and lax.ppermute only.
A program may use at most 64 MiB of HBM per device.

```python
import math
import jax
import jax.numpy as jnp
import numpy as np
from jax import lax

D = 4096
H = 16
DK = 128
DV = 128
FF = 11264
NEW = 4
SEQS = 16


def draw_tokens(key, part):
    first, second, third = jax.random.split(key, 3)
    total_rows = SEQS * NEW
    column_ramp = jnp.exp(jnp.linspace(math.log(0.5), math.log(2.0), D))
    column_noise = jnp.exp(jax.random.uniform(second, (D,), jnp.float32, math.log(0.7), math.log(1.4)))
    row_scale = jnp.exp(jax.random.uniform(third, (total_rows, 1), jnp.float32, math.log(0.3), math.log(3.0)))
    base = jax.random.normal(first, (total_rows, D), jnp.float32)
    return (base * column_ramp * column_noise * row_scale).astype(jnp.bfloat16)


def level_of(key, extent, pieces, least, largest):
    level = 1.0
    for position, parts in pieces:
        draws = jax.random.uniform(jax.random.fold_in(jax.random.fold_in(key, 6), position), (parts,), jnp.float32, least / len(pieces), largest / len(pieces))
        level = level * jnp.repeat(jnp.exp(draws), extent[position] // parts).reshape((-1,) + (1,) * (len(extent) - 1 - position))
    return level


def length_profile(count, total, reach, slope):
    weights = [(1 << 20) // math.isqrt(rank ** slope) + 1 for rank in range(2, count + 1)]
    surplus, counts = total - reach - (count - 1), [1] * (count - 1)
    while surplus > 0:
        movable = [i for i in range(count - 1) if counts[i] < reach]
        whole, budget = sum([weights[i] for i in movable]), surplus
        for i in movable:
            more = min(reach - counts[i], max(1, budget * weights[i] // whole), surplus)
            counts[i] = counts[i] + more
            surplus = surplus - more
    return np.array([reach] + counts)


def ragged(stream_key, count, total, bound, slope):
    if count == 2:
        one = jax.random.randint(stream_key, (), max(1, total - bound), min(bound, total - 1) + 1)
        return jnp.stack([one, total - one])
    sizes = jnp.asarray(length_profile(count, total, bound, slope), jnp.int32)
    pairs = (count - 1) // 2
    giver, sink = sizes[1:1 + 2 * pairs:2], sizes[2:2 + 2 * pairs:2]
    room = jnp.minimum(giver - 1, bound - sink)
    passed = jax.random.randint(jax.random.fold_in(stream_key, 1), (pairs,), 0, 1 << 20) % (room + 1)
    sizes = sizes.at[1:1 + 2 * pairs:2].set(giver - passed).at[2:2 + 2 * pairs:2].set(sink + passed)
    return sizes[jax.random.permutation(jax.random.fold_in(stream_key, 2), count)]


def centred(rng, extent, spread, bound, cuts=(), held_as=jnp.bfloat16):
    gain = level_of(rng, extent, cuts, -0.22, 0.18) if cuts else 1.0
    values = jax.random.normal(rng, extent, jnp.float32) * spread * gain
    return jnp.minimum(jnp.maximum(values, -bound), bound).astype(held_as)


def setup_inputs(seed: int = 0) -> dict:
    streams_of = jax.random.split(jax.random.key(seed), 19)
    return {
        "tokens": draw_tokens(jax.random.fold_in(streams_of[18], 71), 0),
        "lengths": ragged(streams_of[1], SEQS, SEQS * 7 // 4, NEW, 2).astype(jnp.int32),
        "memory": centred(streams_of[2], (SEQS, H, DK, DV), 0.1, 0.6, ((0, 16), (1, 2)), jnp.float32),
        "norm_gain": jnp.clip(1.0 + 0.18 * jax.random.normal(streams_of[3], (D,), jnp.float32), 0.1, 1.9),
        "w_query": centred(streams_of[4], (D, H * DK), D ** -0.5, 0.09375, ((0, 16), (1, 2))),
        "w_key": centred(streams_of[5], (D, H * DK), D ** -0.5, 0.09375, ((0, 16), (1, 2))),
        "w_value": centred(streams_of[6], (D, H * DV), D ** -0.5, 0.09375, ((0, 16), (1, 2))),
        "w_outgate": centred(streams_of[7], (D, H * DV), D ** -0.5, 0.09375, ((0, 16), (1, 2))),
        "w_alpha": centred(streams_of[8], (D, H), D ** -0.5, 0.09375, ((0, 16),)),
        "w_beta": centred(streams_of[9], (D, H), D ** -0.5, 0.09375, ((0, 16),)),
        "decay_log": jnp.clip(-4.0 + 4.5 * jax.random.uniform(streams_of[10], (H,), jnp.float32) ** level_of(streams_of[10], (H,), ((0, 2),), -0.2, 0.2), -4.0, 0.5),
        "decay_bias": jnp.clip(jax.random.uniform(streams_of[11], (H,), jnp.float32, -1.0, 1.0) * level_of(streams_of[11], (H,), ((0, 2),), -0.4, 0.0), -1.0, 1.0),
        "head_gain": jnp.clip(1.0 + 0.18 * jax.random.normal(streams_of[12], (DV,), jnp.float32), 0.1, 1.9),
        "w_output": centred(streams_of[13], (H * DV, D), (H * DV) ** -0.5, 0.125, ((0, 2), (1, 16))),
        "mlp_gain": jnp.clip(1.0 + 0.18 * jax.random.normal(streams_of[14], (D,), jnp.float32), 0.1, 1.9),
        "w_gate": centred(streams_of[15], (D, FF), D ** -0.5, 0.09375, ((0, 16), (1, 2))),
        "w_up": centred(streams_of[16], (D, FF), D ** -0.5, 0.09375, ((0, 16), (1, 2))),
        "w_down": centred(streams_of[17], (FF, D), FF ** -0.5, 0.0546875, ((0, 2), (1, 16))),
    }


epsilon = 1e-06

def unit_rows(values):
    return values * lax.rsqrt(lax.optimization_barrier(jnp.sum(values * values, axis=-1, keepdims=True)) + epsilon)

def advance(memory, queries, key_rows, value_rows, decays, betas):
    outputs = []
    for step in range(queries.shape[1]):
        memory = jnp.exp(decays[:, step])[:, :, None, None] * memory
        predicted = jnp.einsum('shde,shd->she', memory, key_rows[:, step], precision=lax.Precision.HIGHEST)
        correction = betas[:, step][:, :, None] * (value_rows[:, step] - predicted)
        memory = memory + key_rows[:, step][:, :, :, None] * correction[:, :, None, :]
        outputs.append(jnp.einsum('shde,shd->she', memory, queries[:, step], precision=lax.Precision.HIGHEST))
    return (memory, jnp.stack(outputs, axis=1))

def reference(tokens, lengths, memory, norm_gain, w_query, w_key, w_value, w_outgate, w_alpha, w_beta, decay_log, decay_bias, head_gain, w_output, mlp_gain, w_gate, w_up, w_down):
    total_rows = tokens.shape[0]
    token_f = tokens.astype(jnp.float32)
    rstd = lax.rsqrt(lax.optimization_barrier(jnp.mean(token_f * token_f, axis=1, keepdims=True)) + epsilon)
    scaled = (token_f * norm_gain).astype(jnp.bfloat16)

    def project(weight):
        return jnp.dot(scaled, weight, preferred_element_type=jnp.float32) * rstd
    queries = project(w_query).astype(jnp.bfloat16)
    key_rows = project(w_key).astype(jnp.bfloat16)
    value_rows = project(w_value).astype(jnp.bfloat16)
    outgate = project(w_outgate).astype(jnp.bfloat16)
    alphas = project(w_alpha)
    beta_pre = project(w_beta)
    live = jnp.arange(NEW, dtype=jnp.int32)[None, :] < lengths[:, None]
    query_h = unit_rows(queries.astype(jnp.float32).reshape(SEQS, NEW, H, DK)) * DK ** (-0.5)
    key_h = unit_rows(key_rows.astype(jnp.float32).reshape(SEQS, NEW, H, DK))
    value_h = value_rows.astype(jnp.float32).reshape(SEQS, NEW, H, DV)
    decays = -jnp.exp(decay_log) * jax.nn.softplus(alphas + decay_bias)
    decays = jnp.where(live[:, :, None], decays.reshape(SEQS, NEW, H), 0.0)
    betas = jnp.where(live[:, :, None], jax.nn.sigmoid(beta_pre).reshape(SEQS, NEW, H), 0.0)
    new_memory, attended = advance(memory, query_h, key_h, value_h, decays, betas)
    attended = attended * lax.rsqrt(lax.optimization_barrier(jnp.mean(attended * attended, axis=-1, keepdims=True)) + epsilon)
    gate_h = outgate.astype(jnp.float32).reshape(SEQS, NEW, H, DV)
    mixed = (attended * head_gain * jax.nn.silu(gate_h)).astype(jnp.bfloat16).reshape(total_rows, H * DV)
    hidden = (token_f + jnp.dot(mixed, w_output, preferred_element_type=jnp.float32)).astype(jnp.bfloat16)
    hidden_f = hidden.astype(jnp.float32)
    rstd2 = lax.rsqrt(lax.optimization_barrier(jnp.mean(hidden_f * hidden_f, axis=1, keepdims=True)) + epsilon)
    hscaled = (hidden_f * mlp_gain).astype(jnp.bfloat16)
    gate_rows = jnp.dot(hscaled, w_gate, preferred_element_type=jnp.float32) * rstd2
    up_rows = jnp.dot(hscaled, w_up, preferred_element_type=jnp.float32) * rstd2
    active = (jax.nn.silu(gate_rows) * up_rows).astype(jnp.bfloat16)
    result = hidden_f + jnp.dot(active, w_down, preferred_element_type=jnp.float32)
    layer_out = jnp.where(live.reshape(total_rows)[:, None], result, 0.0).astype(jnp.bfloat16)
    return (layer_out, new_memory)
```

```python
import jax
import jax.numpy as jnp
from jax import lax
from jax.sharding import PartitionSpec as P

D = 4096
DK = 128
DV = 128
NEW = 4


epsilon = 1e-06


def unit_rows(values):
    return values * lax.rsqrt(jnp.sum(values * values, axis=-1, keepdims=True) + epsilon)


def advance(memory, queries, key_rows, value_rows, decays, betas):
    outputs = []
    for step in range(queries.shape[1]):
        memory = jnp.exp(decays[:, step])[:, :, None, None] * memory
        predicted = jnp.einsum(
            "shde,shd->she", memory, key_rows[:, step], precision=lax.Precision.HIGHEST
        )
        correction = betas[:, step][:, :, None] * (value_rows[:, step] - predicted)
        memory = memory + key_rows[:, step][:, :, :, None] * correction[:, :, None, :]
        outputs.append(
            jnp.einsum("shde,shd->she", memory, queries[:, step], precision=lax.Precision.HIGHEST)
        )
    return (memory, jnp.stack(outputs, axis=1))


def two_halves(values):
    high = values.astype(jnp.bfloat16)
    return high, (values - lax.reduce_precision(values, 8, 7)).astype(jnp.bfloat16)


def exchange(blocks):
    return lax.all_to_all(blocks, "kv", 0, 0)


def to_everyone(block, count):
    return lax.all_to_all(jnp.broadcast_to(block[None], (count, *block.shape)), "kv", 0, 0)


def over_tp(terms):
    if lax.axis_size("tp") == 2:
        return terms + lax.ppermute(terms, "tp", [(0, 1), (1, 0)])
    return lax.psum(terms, "tp")


def per_device(
    tokens,
    lengths,
    memory,
    norm_gain,
    w_query,
    w_key,
    w_value,
    w_outgate,
    w_alpha,
    w_beta,
    decay_log,
    decay_bias,
    head_gain,
    w_output,
    mlp_gain,
    w_gate,
    w_up,
    w_down,
):
    total_rows = tokens.shape[0]
    kv_count = lax.axis_size("kv")
    kv_place = lax.axis_index("kv")
    tp_place = lax.axis_index("tp")
    own_rows = total_rows // kv_count
    seq_dev = memory.shape[0]
    heads_dev = memory.shape[1]
    sequences = lengths.shape[0]
    width = heads_dev * DK
    packed = -(-(sequences * 7 // 4) // kv_count) * kv_count
    token_f = tokens.astype(jnp.float32)
    squares = jnp.sum(token_f * token_f, axis=1)
    scaled = (token_f * norm_gain).astype(jnp.bfloat16)
    parts = [
        jnp.dot(scaled, w, preferred_element_type=jnp.float32).astype(jnp.bfloat16)
        for w in (w_query, w_key, w_value, w_outgate)
    ]
    small = jnp.concatenate(
        [
            jnp.dot(scaled, w_alpha, preferred_element_type=jnp.float32),
            jnp.dot(scaled, w_beta, preferred_element_type=jnp.float32),
            squares[:, None],
        ],
        axis=1,
    )
    small_n = small.shape[1]
    high, low = two_halves(small)
    pad = jnp.zeros((total_rows, -(2 * small_n) % 128), jnp.bfloat16)
    sent = jnp.concatenate([*parts, high, low, pad], axis=1).reshape(kv_count, own_rows, -1)
    summed = jnp.sum(exchange(sent).astype(jnp.float32), axis=0)
    small = summed[:, 4 * width : 4 * width + small_n] + summed[:, 4 * width + small_n : 4 * width + 2 * small_n]
    heads_all = w_alpha.shape[1]
    rstd = lax.rsqrt(small[:, 2 * heads_all] / D + epsilon)[:, None]
    queries, key_rows, value_rows, outgate = (
        (summed[:, i * width : (i + 1) * width] * rstd).astype(jnp.bfloat16) for i in range(4)
    )
    alphas = lax.dynamic_slice_in_dim(small[:, :heads_all] * rstd, tp_place * heads_dev, heads_dev, 1)
    beta_pre = lax.dynamic_slice_in_dim(
        small[:, heads_all : 2 * heads_all] * rstd, tp_place * heads_dev, heads_dev, 1
    )
    own_lengths = lax.dynamic_slice_in_dim(lengths, kv_place * seq_dev, seq_dev)
    live = jnp.arange(NEW, dtype=jnp.int32)[None, :] < own_lengths[:, None]
    query_h = unit_rows(queries.astype(jnp.float32).reshape(seq_dev, NEW, heads_dev, DK)) * DK ** (
        -0.5
    )
    key_h = unit_rows(key_rows.astype(jnp.float32).reshape(seq_dev, NEW, heads_dev, DK))
    value_h = value_rows.astype(jnp.float32).reshape(seq_dev, NEW, heads_dev, DV)
    decays = -jnp.exp(decay_log) * jax.nn.softplus(alphas + decay_bias)
    decays = jnp.where(live[:, :, None], decays.reshape(seq_dev, NEW, heads_dev), 0.0)
    betas = jnp.where(
        live[:, :, None], jax.nn.sigmoid(beta_pre).reshape(seq_dev, NEW, heads_dev), 0.0
    )
    new_memory, attended = advance(memory, query_h, key_h, value_h, decays, betas)
    attended = attended * lax.rsqrt(jnp.mean(attended * attended, axis=-1, keepdims=True) + epsilon)
    gate_h = outgate.astype(jnp.float32).reshape(seq_dev, NEW, heads_dev, DV)
    mixed = (
        (attended * head_gain * jax.nn.silu(gate_h))
        .astype(jnp.bfloat16)
        .reshape(own_rows, heads_dev * DV)
    )
    order = jnp.arange(sequences, dtype=jnp.int32)
    starts = jnp.sum(jnp.where(order[None, :] < order[:, None], lengths[None, :], 0), axis=1)
    slot = jnp.arange(NEW, dtype=jnp.int32)
    place = jnp.where(slot[None, :] < lengths[:, None], starts[:, None] + slot[None, :], packed)
    pick = (jnp.arange(packed)[:, None] == place.reshape(1, total_rows)).astype(jnp.bfloat16)
    packed_tokens = jnp.dot(pick, tokens, preferred_element_type=jnp.float32)
    all_mixed = to_everyone(mixed, kv_count).reshape(total_rows, width)
    packed_mixed = jnp.dot(pick, all_mixed, preferred_element_type=jnp.float32).astype(jnp.bfloat16)
    attn_terms = jnp.dot(packed_mixed, w_output, preferred_element_type=jnp.float32)
    attn_total = over_tp(attn_terms)
    hidden = (packed_tokens + attn_total).astype(jnp.bfloat16)
    hidden_f = hidden.astype(jnp.float32)
    hidden_squares = jnp.sum(hidden_f * hidden_f, axis=1, keepdims=True)
    hscaled = (hidden_f * mlp_gain).astype(jnp.bfloat16)
    units = w_gate.shape[1]
    part_gate_rows = jnp.dot(hscaled, w_gate, preferred_element_type=jnp.float32)
    part_up_rows = jnp.dot(hscaled, w_up, preferred_element_type=jnp.float32)
    high, low = two_halves(jnp.broadcast_to(hidden_squares, (packed, 64)))
    sent = jnp.concatenate(
        [
            part_gate_rows.astype(jnp.bfloat16),
            part_up_rows.astype(jnp.bfloat16),
            high,
            low,
        ],
        axis=1,
    ).reshape(kv_count, packed // kv_count, -1)
    summed = jnp.sum(exchange(sent).astype(jnp.float32), axis=0)
    mlp_squares = summed[:, 2 * units] + summed[:, 2 * units + 64]
    rstd2 = lax.rsqrt(mlp_squares / D + epsilon)[:, None]
    active = (jax.nn.silu(summed[:, :units] * rstd2) * (summed[:, units : 2 * units] * rstd2)).astype(
        jnp.bfloat16
    )
    all_active = to_everyone(active, kv_count).reshape(packed, units)
    feed_terms = jnp.dot(all_active, w_down, preferred_element_type=jnp.float32)
    feed_total = over_tp(feed_terms.astype(jnp.bfloat16)).astype(jnp.float32)
    result = (hidden_f + feed_total).astype(jnp.bfloat16)
    layer_out = lax.dot_general(
        pick, result, (((0,), (0,)), ((), ())), preferred_element_type=jnp.float32
    ).astype(jnp.bfloat16)
    return (layer_out, new_memory)


def solution(mesh):
    placed = (
        P(None, "kv"),
        P(),
        P("kv", "tp", None, None),
        P("kv"),
        P("kv", "tp"),
        P("kv", "tp"),
        P("kv", "tp"),
        P("kv", "tp"),
        P("kv", None),
        P("kv", None),
        P("tp"),
        P("tp"),
        P(),
        P("tp", "kv"),
        P("kv"),
        P("kv", "tp"),
        P("kv", "tp"),
        P("tp", "kv"),
    )
    return jax.shard_map(
        per_device,
        mesh=mesh,
        in_specs=placed,
        out_specs=(P(None, "kv"), P("kv", "tp", None, None)),
        check_vma=False,
    )
```

```python
import functools

import jax
import jax.numpy as jnp
from jax import lax
from jax.experimental import pallas as pl
from jax.experimental.pallas import tpu as pltpu
from jax.sharding import PartitionSpec as P

D = 4096
DK = 128
DV = 128
NEW = 4
LANES = 128
SUBS = 8

epsilon = 1e-06

F32 = jnp.float32
BF16 = jnp.bfloat16
VMEM = pl.BlockSpec(memory_space=pltpu.VMEM)
SMEM = pl.BlockSpec(memory_space=pltpu.SMEM)


def call(body, outs, ins, limit, flops, name):
    moved = sum(x.size * x.dtype.itemsize for x in (*outs, *ins))
    return pl.pallas_call(
        body,
        out_shape=outs,
        in_specs=[SMEM if x.dtype == jnp.int32 else VMEM for x in ins],
        out_specs=[VMEM] * len(outs),
        compiler_params=pltpu.CompilerParams(vmem_limit_bytes=limit << 20),
        cost_estimate=pl.CostEstimate(flops=flops, bytes_accessed=moved, transcendentals=0),
        name=name,
    )(*ins)


def shape(dims, dtype):
    return jax.ShapeDtypeStruct(dims, dtype)


def iota(dims, axis):
    return lax.broadcasted_iota(jnp.int32, dims, axis)


def dot(a, b):
    return jnp.dot(a, b, preferred_element_type=F32)


def dot_nt(a, b):
    return lax.dot_general(a, b, (((1,), (1,)), ((), ())), preferred_element_type=F32)


def places(lengths_ref, sequence_of, slot_of):
    place = jnp.full(sequence_of.shape, -1, jnp.int32)
    start = 0
    for s in range(lengths_ref.shape[0]):
        held = lengths_ref[s]
        mine = (sequence_of == s) & (slot_of < held)
        place = jnp.where(mine, slot_of + start, place)
        start = start + held
    return place


def log2(n):
    assert n & (n - 1) == 0
    return n.bit_length() - 1


def front_kernel(tokens_ref, gain_ref, wq_ref, wk_ref, wv_ref, wg_ref, wa_ref, wb_ref, out_ref):
    total_rows = tokens_ref.shape[0]
    width = wq_ref.shape[1]
    heads = wa_ref.shape[0]
    tokens = tokens_ref[...]
    scaled = (tokens.astype(F32) * gain_ref[...]).astype(BF16)
    dims = (2 * total_rows, total_rows)
    row, col = iota(dims, 0), iota(dims, 1)
    target = lax.shift_left(lax.shift_right_logical(row, 3), 2) + (row & 3)
    hit = target == col
    upper = (row & 7) < NEW
    zero, one = jnp.zeros(dims, F32), jnp.ones(dims, F32)
    place_a = jnp.where(hit & upper, one, zero).astype(BF16)
    place_b = jnp.where(hit & ~upper, one, zero).astype(BF16)
    left = dot(place_a, scaled).astype(BF16)
    right = dot(place_b, scaled).astype(BF16)
    out_ref[:, :width] = (dot(left, wq_ref[...]) + dot(right, wk_ref[...])).astype(BF16)
    out_ref[:, width : 2 * width] = (dot(left, wv_ref[...]) + dot(right, wg_ref[...])).astype(BF16)
    both = dot(place_a + place_b, tokens)
    squares = jnp.sum(both * both, axis=1, keepdims=True)
    fill = jnp.zeros((LANES - 2 * heads, wa_ref.shape[1]), BF16)
    small = dot_nt(left + right, jnp.concatenate([wa_ref[...], wb_ref[...], fill], axis=0))
    lane = iota(small.shape, 1)
    small = jnp.where(lane == 2 * heads, jnp.broadcast_to(squares, small.shape), small)
    high = small.astype(BF16).astype(F32)
    first = (iota(small.shape, 0) & 7) < NEW
    out_ref[:, 2 * width :] = jnp.where(first, high, small - high).astype(BF16)


def row_sum(ref, start, columns):
    block = ref[:, start : start + columns].astype(F32)
    return jnp.sum(block.reshape(-1, SUBS, columns), axis=0)


def recur_kernel(
    lengths_ref, got_ref, memory_ref, log_ref, bias_ref, gain_ref, memory_out, mixed_out, unit, vals, preds, copies
):
    heads = memory_ref.shape[0]
    width = heads * DK
    all_heads = heads * lax.axis_size("tp")
    kv_place = lax.axis_index("kv")
    tp_place = lax.axis_index("tp")
    small = row_sum(got_ref, 2 * width, LANES)
    small = small + pltpu.roll(small, NEW, 0)
    rstd = lax.rsqrt(small[:, 2 * all_heads : 2 * all_heads + 1] / D + epsilon)
    small = small * rstd
    alphas = pltpu.roll(small, LANES - tp_place * heads, 1)[:, :heads]
    betas = pltpu.roll(small, LANES - all_heads - tp_place * heads, 1)[:, :heads]
    x = alphas + bias_ref[...]
    soft = jnp.maximum(x, 0.0) + jnp.log1p(jnp.exp(-jnp.abs(x)))
    decay = -jnp.exp(log_ref[...]) * soft
    slot = iota(decay.shape, 0)
    live = (slot & 3) < lengths_ref[kv_place]
    keep = jnp.exp(jnp.where(live, decay, 0.0))
    write = jnp.where(live, 1.0 / (1.0 + jnp.exp(-betas)), 0.0)
    unit[...] = jnp.zeros(unit.shape, F32)
    unit[heads * SUBS : heads * SUBS + SUBS, :heads] = jnp.where(slot < NEW, keep, write)
    factor = jnp.where(iota((SUBS, 1), 0) < NEW, DK ** (-0.5), 1.0)
    for h in range(heads):
        block = (row_sum(got_ref, h * DK, DK) * rstd).astype(BF16).astype(F32)
        norm = lax.rsqrt(jnp.sum(block * block, axis=1, keepdims=True) + epsilon)
        unit[h * SUBS : (h + 1) * SUBS, :] = block * norm * factor
        vals[h * SUBS : (h + 1) * SUBS, :] = (
            (row_sum(got_ref, width + h * DV, DV) * rstd).astype(BF16).astype(F32)
        )
    turned = unit[...].T
    for h in range(heads):
        state = memory_ref[h]
        for j in range(SUBS):
            at = h * SUBS + j
            preds[at : at + 1, :] = jnp.sum(turned[:, at : at + 1] * state, axis=0, keepdims=True)

    def rows(ref, j):
        return ref[pl.ds(j, heads, stride=SUBS), :]

    base = heads * SUBS
    queries = [rows(unit, t) for t in range(NEW)]
    keys = [rows(unit, NEW + t) for t in range(NEW)]
    keeps = [turned[:heads, base + t : base + t + 1] for t in range(NEW)]
    writes = [turned[:heads, base + NEW + t : base + NEW + t + 1] for t in range(NEW)]

    def inner(a, b):
        return jnp.sum(a * b, axis=1, keepdims=True)

    updates = []
    passed = []
    total = jnp.ones((heads, 1), F32)
    for t in range(NEW):
        total = total * keeps[t]
        passed = [p * keeps[t] for p in passed]
        said = total * rows(preds, NEW + t)
        for i in range(t):
            said = said + (passed[i] * inner(keys[i], keys[t])) * updates[i]
        updates.append(writes[t] * (rows(vals, t) - said))
        passed.append(jnp.ones((heads, 1), F32))
        out = total * rows(preds, t)
        for i in range(t + 1):
            out = out + (passed[i] * inner(keys[i], queries[t])) * updates[i]
        out = out * lax.rsqrt(jnp.mean(out * out, axis=1, keepdims=True) + epsilon)
        gate = rows(vals, NEW + t)
        silu = gate * (1.0 / (1.0 + jnp.exp(-gate)))
        copies[t * heads : (t + 1) * heads, :] = out * gain_ref[...] * silu
    final = [passed[i] * updates[i] for i in range(NEW)]
    for h in range(heads):
        state = memory_ref[h] * total[h : h + 1, :]
        for i in range(NEW):
            at = h * SUBS + NEW + i
            state = state + turned[:, at : at + 1] * final[i][h : h + 1, :]
        memory_out[h] = state
    mixed = copies[...].astype(BF16)
    for d in range(mixed_out.shape[0]):
        mixed_out[d] = mixed


def project_kernel(lengths_ref, mixed_ref, w_ref, out_ref):
    heads = w_ref.shape[0] // DV
    total = mixed_ref.shape[0]
    packed = out_ref.shape[0]
    col = iota((1, total), 1)
    place = places(
        lengths_ref,
        lax.shift_right_logical(col, log2(NEW * heads)),
        lax.shift_right_logical(col, log2(heads)) & 3,
    )
    wanted = jnp.where((col & (heads - 1)) == 0, place, -1)
    mixed = mixed_ref[...]
    row = iota((packed, total), 0)
    head_of = col & (heads - 1)
    sum_ = None
    for h in range(heads):
        wanted = jnp.where(head_of == h, place, -1)
        pick = jnp.where(row == wanted, 1.0, 0.0).astype(BF16)
        term = dot(dot(pick, mixed).astype(BF16), w_ref[h * DV : (h + 1) * DV, :])
        sum_ = term if sum_ is None else sum_ + term
    out_ref[...] = sum_


def picker(lengths_ref, packed, total_rows):
    col = iota((1, total_rows), 1)
    place = places(lengths_ref, lax.shift_right_logical(col, 2), col & 3)
    return jnp.where(iota((packed, total_rows), 0) == place, 1.0, 0.0).astype(BF16)


def blocks_of(granules, tiles, receiver):
    first = (receiver * granules) // tiles
    last = (receiver * granules + granules - 1) // tiles
    return first, last


def up_kernel(granules, extra, lengths_ref, *refs):
    *terms, tokens_ref, gain_ref, wg_ref, wu_ref, hidden_out, out_ref = refs
    packed = hidden_out.shape[0]
    pick = picker(lengths_ref, packed, tokens_ref.shape[0])
    hidden = dot(pick, tokens_ref[...])
    for term in terms:
        hidden = hidden + term[...]
    hidden = hidden.astype(BF16)
    hidden_out[...] = hidden
    hidden_f = hidden.astype(F32)
    scaled = (hidden_f * gain_ref[...]).astype(BF16)
    tiles = wg_ref.shape[1] // LANES
    row_blocks = packed // SUBS
    squares = jnp.sum(hidden_f * hidden_f, axis=1, keepdims=True)
    squares = jnp.broadcast_to(squares, (packed, LANES))
    high = squares.astype(BF16).astype(F32)
    halves = jnp.where(iota(squares.shape, 1) < LANES // 2, high, squares - high).astype(BF16)
    step = 4
    for start in range(0, tiles, step):
        stop = min(start + step, tiles)
        span = slice(start * LANES, stop * LANES)
        gate = dot(scaled, wg_ref[:, span])
        up = dot(scaled, wu_ref[:, span])
        for t in range(start, stop):
            lanes = slice((t - start) * LANES, (t - start + 1) * LANES)
            for b in range(row_blocks):
                rows = slice(b * SUBS, (b + 1) * SUBS)
                pair = jnp.concatenate([gate[rows, lanes], up[rows, lanes]], axis=0).astype(BF16)
                d, i = divmod(b * tiles + t, granules)
                out_ref[d, i * 16 : i * 16 + 16, :] = pair
    for d in range(out_ref.shape[0]):
        first, _ = blocks_of(granules, tiles, d)
        for e in range(extra):
            b = min(first + e, row_blocks - 1)
            at = granules * 16 + e * SUBS
            out_ref[d, at : at + SUBS, :] = halves[b * SUBS : (b + 1) * SUBS, :]


def active_kernel(granules, extra, tiles, got_ref, out_ref):
    senders = got_ref.shape[0]
    scales = []
    for e in range(extra):
        at = granules * 16 + e * SUBS
        squares = jnp.sum(got_ref[:, at : at + SUBS, :].astype(F32), axis=0)
        squares = squares[:, :1] + squares[:, LANES // 2 : LANES // 2 + 1]
        scales.append(lax.rsqrt(squares / D + epsilon))
    place = lax.axis_index("kv") if extra > 1 else 0
    for i in range(granules):
        pair = got_ref[0, i * 16 : i * 16 + 16, :].astype(F32)
        for s in range(1, senders):
            pair = pair + got_ref[s, i * 16 : i * 16 + 16, :].astype(F32)
        scale = scales[0]
        if extra > 1:
            ahead = lax.div(place * granules + i, tiles) - lax.div(place * granules, tiles)
            for e in range(1, extra):
                scale = jnp.where(ahead >= e, scales[e], scale)
        gate, up = pair[:SUBS] * scale, pair[SUBS:] * scale
        active = (gate * (1.0 / (1.0 + jnp.exp(-gate))) * up).astype(BF16)
        for d in range(senders):
            out_ref[d, i * SUBS : (i + 1) * SUBS, :] = active


def down_kernel(got_ref, w_ref, out_ref):
    packed = out_ref.shape[0]
    tiles = w_ref.shape[0] // LANES
    sum_ = None
    for t in range(tiles):
        parts = [
            got_ref[(b * tiles + t) * SUBS : (b * tiles + t + 1) * SUBS, :].astype(F32)
            for b in range(packed // SUBS)
        ]
        term = dot(jnp.concatenate(parts, axis=0).astype(BF16), w_ref[t * LANES : (t + 1) * LANES, :])
        sum_ = term if sum_ is None else sum_ + term
    out_ref[...] = sum_


def last_kernel(lengths_ref, *refs):
    *terms, hidden_ref, out_ref = refs
    packed = hidden_ref.shape[0]
    result = terms[0][...]
    for term in terms[1:]:
        result = result + term[...]
    result = (hidden_ref[...].astype(F32) + result).astype(BF16)
    pick = picker(lengths_ref, packed, out_ref.shape[0])
    out_ref[...] = lax.dot_general(
        pick, result, (((0,), (0,)), ((), ())), preferred_element_type=F32
    ).astype(BF16)


def exchange(blocks):
    return lax.all_to_all(blocks, "kv", 0, 0)


def over_tp(terms):
    if lax.axis_size("tp") == 2:
        return [terms, lax.ppermute(terms, "tp", [(0, 1), (1, 0)])]
    return [lax.psum(terms, "tp")]


def per_device(
    tokens,
    lengths,
    memory,
    norm_gain,
    w_query,
    w_key,
    w_value,
    w_outgate,
    w_alpha,
    w_beta,
    decay_log,
    decay_bias,
    head_gain,
    w_output,
    mlp_gain,
    w_gate,
    w_up,
    w_down,
):
    total_rows, own_width = tokens.shape
    kv = lax.axis_size("kv")
    seq_dev, heads = memory.shape[:2]
    assert seq_dev == 1
    width = heads * DK
    sequences = lengths.shape[0]
    units = w_gate.shape[1]
    packed = -(-(sequences * 7 // 4) // SUBS) * SUBS
    tiles = units // LANES
    granules = -(-(tiles * packed // SUBS) // kv)
    last_receiver = (tiles * packed // SUBS - 1) // granules
    extra = max(b - a + 1 for a, b in (blocks_of(granules, tiles, d) for d in range(last_receiver + 1)))
    columns = 2 * width + LANES

    (sent,) = call(
        front_kernel,
        [shape((2 * total_rows, columns), BF16)],
        [tokens, norm_gain[None], w_query, w_key, w_value, w_outgate, w_alpha.T, w_beta.T],
        16,
        4 * total_rows * own_width * 4 * width,
        "front",
    )
    got = exchange(sent.reshape(kv, SUBS, columns)).reshape(kv * SUBS, columns)
    new_memory, sent = pl.pallas_call(
        recur_kernel,
        out_shape=[shape((heads, DK, DV), F32), shape((kv, NEW * heads, DV), BF16)],
        in_specs=[SMEM] + [VMEM] * 5,
        out_specs=[VMEM] * 2,
        scratch_shapes=[
            pltpu.VMEM((LANES, LANES), F32),
            pltpu.VMEM((heads * SUBS, DV), F32),
            pltpu.VMEM((heads * SUBS, DV), F32),
            pltpu.VMEM((NEW * heads, DV), F32),
        ],
        compiler_params=pltpu.CompilerParams(vmem_limit_bytes=16 << 20),
        cost_estimate=pl.CostEstimate(flops=4 << 20, bytes_accessed=2 << 20, transcendentals=0),
        name="recur",
    )(lengths, got, memory[0], decay_log[None], decay_bias[None], head_gain[None])
    got = exchange(sent).reshape(kv * NEW * heads, DV)
    (attn,) = call(
        project_kernel, [shape((packed, own_width), F32)], [lengths, got, w_output], 8, 32 << 20, "project"
    )
    hidden, sent = call(
        functools.partial(up_kernel, granules, extra),
        [shape((packed, own_width), BF16), shape((kv, granules * 16 + extra * SUBS, LANES), BF16)],
        [lengths, *over_tp(attn), tokens, mlp_gain[None], w_gate, w_up],
        16,
        4 * packed * own_width * units,
        "up",
    )
    (sent,) = call(
        functools.partial(active_kernel, granules, extra, tiles),
        [shape((kv, granules * SUBS, LANES), BF16)],
        [exchange(sent)],
        8,
        1 << 20,
        "active",
    )
    got = exchange(sent).reshape(kv * granules * SUBS, LANES)
    (feed,) = call(
        down_kernel,
        [shape((packed, own_width), F32)],
        [got, w_down],
        16,
        2 * packed * own_width * units,
        "down",
    )
    (layer_out,) = call(
        last_kernel,
        [shape((total_rows, own_width), BF16)],
        [lengths, *over_tp(feed), hidden],
        8,
        1 << 20,
        "last",
    )
    return (layer_out, new_memory[None])


def solution(mesh):
    placed = (
        P(None, "kv"),
        P(),
        P("kv", "tp", None, None),
        P("kv"),
        P("kv", "tp"),
        P("kv", "tp"),
        P("kv", "tp"),
        P("kv", "tp"),
        P("kv", None),
        P("kv", None),
        P("tp"),
        P("tp"),
        P(),
        P("tp", "kv"),
        P("kv"),
        P("kv", "tp"),
        P("kv", "tp"),
        P("tp", "kv"),
    )
    return jax.shard_map(
        per_device,
        mesh=mesh,
        in_specs=placed,
        out_specs=(P(None, "kv"), P("kv", "tp", None, None)),
        check_vma=False,
    )
```

```python
import functools

import jax
import jax.numpy as jnp
from jax import lax
from jax.experimental import pallas as pl
from jax.experimental.pallas import tpu as pltpu
from jax.sharding import PartitionSpec as P

D = 4096
DK = 128
DV = 128
NEW = 4
LANES = 128
SUBS = 8

epsilon = 1e-06

F32 = jnp.float32
BF16 = jnp.bfloat16
VMEM = pl.BlockSpec(memory_space=pltpu.VMEM)
HBM = pl.BlockSpec(memory_space=pltpu.HBM)


def call(body, outs, ins, specs, limit, flops, name, scratch=(), out_specs=None):
    moved = sum(x.size * x.dtype.itemsize for x in (*outs, *ins))
    ins = [pltpu.with_memory_space_constraint(x, pltpu.HBM) if s is HBM else x for x, s in zip(ins, specs)]
    return pl.pallas_call(
        body,
        out_shape=outs,
        in_specs=specs,
        out_specs=out_specs or [VMEM] * len(outs),
        scratch_shapes=list(scratch),
        compiler_params=pltpu.CompilerParams(vmem_limit_bytes=limit << 20),
        cost_estimate=pl.CostEstimate(flops=flops, bytes_accessed=moved, transcendentals=0),
        name=name,
    )(*ins)


def room(x):
    return pltpu.VMEM(x.shape, x.dtype)


def shape(dims, dtype):
    return jax.ShapeDtypeStruct(dims, dtype)


def iota(dims, axis):
    return lax.broadcasted_iota(jnp.int32, dims, axis)


def dot(a, b):
    return jnp.dot(a, b, preferred_element_type=F32)


def dot_nt(a, b):
    return lax.dot_general(a, b, (((1,), (1,)), ((), ())), preferred_element_type=F32)


def places(lengths_ref, sequence_of, slot_of):
    place = jnp.full(sequence_of.shape, -1, jnp.int32)
    start = 0
    for s in range(lengths_ref.shape[0]):
        held = lengths_ref[s]
        mine = (sequence_of == s) & (slot_of < held)
        place = jnp.where(mine, slot_of + start, place)
        start = start + held
    return place


def log2(n):
    assert n & (n - 1) == 0
    return n.bit_length() - 1


def front_kernel(heads, *refs):
    count = 9
    sources, (out_ref, base_ref, pick_ref, place_ref, own_ref) = refs[:count], refs[count : count + 5]
    held, sems = refs[count + 5 : 2 * count + 5], refs[2 * count + 5]
    copies = [pltpu.make_async_copy(a, b, sems.at[i]) for i, (a, b) in enumerate(zip(sources, held))]
    for copy in copies:
        copy.start()
    lengths_ref, tokens_ref, gain_ref, wa_ref, wb_ref, wq_ref, wk_ref, wv_ref, wg_ref = held
    total_rows = tokens_ref.shape[0]
    width = wq_ref.shape[1]
    all_heads = wa_ref.shape[0]
    packed = pick_ref.shape[0]
    copies[0].wait()
    own_ref[...] = jnp.full(own_ref.shape, lengths_ref[lax.axis_index("kv")], jnp.int32)
    col = iota(place_ref.shape, 1)
    place_ref[...] = places(
        lengths_ref,
        lax.shift_right_logical(col, log2(NEW * heads)),
        lax.shift_right_logical(col, log2(heads)) & 3,
    )
    pick = picker(lengths_ref, packed, total_rows)
    pick_ref[...] = pick
    dims = (2 * total_rows, total_rows)
    row, col = iota(dims, 0), iota(dims, 1)
    target = lax.shift_left(lax.shift_right_logical(row, 3), 2) + (row & 3)
    hit = target == col
    upper = (row & 7) < NEW
    zero, one = jnp.zeros(dims, F32), jnp.ones(dims, F32)
    place_a = jnp.where(hit & upper, one, zero).astype(BF16)
    place_b = jnp.where(hit & ~upper, one, zero).astype(BF16)
    fill = jnp.zeros((LANES - 2 * all_heads, wa_ref.shape[1]), BF16)
    for copy in copies[1:5]:
        copy.wait()
    tokens = tokens_ref[...]
    base_ref[...] = dot(pick, tokens)
    scaled = (tokens.astype(F32) * gain_ref[...]).astype(BF16)
    left = dot(place_a, scaled).astype(BF16)
    right = dot(place_b, scaled).astype(BF16)
    both = dot(place_a + place_b, tokens)
    squares = jnp.sum(both * both, axis=1, keepdims=True)
    small = dot_nt(left + right, jnp.concatenate([wa_ref[...], wb_ref[...], fill], axis=0))
    lane = iota(small.shape, 1)
    small = jnp.where(lane == 2 * all_heads, jnp.broadcast_to(squares, small.shape), small)
    high = small.astype(BF16).astype(F32)
    first = (iota(small.shape, 0) & 7) < NEW
    out_ref[:, 2 * width :] = jnp.where(first, high, small - high).astype(BF16)
    copies[5].wait()
    copies[6].wait()
    out_ref[:, :width] = (dot(left, wq_ref[...]) + dot(right, wk_ref[...])).astype(BF16)
    copies[7].wait()
    copies[8].wait()
    out_ref[:, width : 2 * width] = (dot(left, wv_ref[...]) + dot(right, wg_ref[...])).astype(BF16)


def row_sum(ref, start, columns):
    block = ref[:, start : start + columns].astype(F32)
    return jnp.sum(block.reshape(-1, SUBS, columns), axis=0)


def recur_kernel(
    own_ref,
    got_ref,
    memory_hbm,
    log_ref,
    bias_ref,
    gain_ref,
    memory_out,
    mixed_out,
    unit,
    vals,
    preds,
    copies,
    memory_ref,
    fresh_ref,
    sem,
    out_sem,
):
    heads = memory_ref.shape[0]
    fetch = pltpu.make_async_copy(memory_hbm, memory_ref, sem)
    fetch.start()
    width = heads * DK
    all_heads = heads * lax.axis_size("tp")
    tp_place = lax.axis_index("tp")
    small = row_sum(got_ref, 2 * width, LANES)
    small = small + pltpu.roll(small, NEW, 0)
    rstd = lax.rsqrt(small[:, 2 * all_heads : 2 * all_heads + 1] / D + epsilon)
    small = small * rstd
    alphas = pltpu.roll(small, LANES - tp_place * heads, 1)[:, :heads]
    betas = pltpu.roll(small, LANES - all_heads - tp_place * heads, 1)[:, :heads]
    x = alphas + bias_ref[...]
    soft = jnp.maximum(x, 0.0) + jnp.log1p(jnp.exp(-jnp.abs(x)))
    decay = -jnp.exp(log_ref[...]) * soft
    slot = iota(decay.shape, 0)
    live = (slot & 3) < own_ref[:, :heads]
    keep = jnp.exp(jnp.where(live, decay, 0.0))
    write = jnp.where(live, 1.0 / (1.0 + jnp.exp(-betas)), 0.0)
    unit[...] = jnp.zeros(unit.shape, F32)
    unit[heads * SUBS : heads * SUBS + SUBS, :heads] = jnp.where(slot < NEW, keep, write)
    factor = jnp.where(iota((SUBS, 1), 0) < NEW, DK ** (-0.5), 1.0)
    for h in range(heads):
        block = (row_sum(got_ref, h * DK, DK) * rstd).astype(BF16).astype(F32)
        norm = lax.rsqrt(jnp.sum(block * block, axis=1, keepdims=True) + epsilon)
        unit[h * SUBS : (h + 1) * SUBS, :] = block * norm * factor
        vals[h * SUBS : (h + 1) * SUBS, :] = (
            (row_sum(got_ref, width + h * DV, DV) * rstd).astype(BF16).astype(F32)
        )
    turned = unit[...].T
    fetch.wait()
    for h in range(heads):
        state = memory_ref[h]
        for j in range(SUBS):
            at = h * SUBS + j
            preds[at : at + 1, :] = jnp.sum(turned[:, at : at + 1] * state, axis=0, keepdims=True)

    def rows(ref, j):
        return ref[pl.ds(j, heads, stride=SUBS), :]

    base = heads * SUBS
    queries = [rows(unit, t) for t in range(NEW)]
    keys = [rows(unit, NEW + t) for t in range(NEW)]
    keeps = [turned[:heads, base + t : base + t + 1] for t in range(NEW)]
    writes = [turned[:heads, base + NEW + t : base + NEW + t + 1] for t in range(NEW)]

    def inner(a, b):
        return jnp.sum(a * b, axis=1, keepdims=True)

    updates, outs = [], []
    passed = []
    total = jnp.ones((heads, 1), F32)
    for t in range(NEW):
        total = total * keeps[t]
        passed = [p * keeps[t] for p in passed]
        said = total * rows(preds, NEW + t)
        for i in range(t):
            said = said + (passed[i] * inner(keys[i], keys[t])) * updates[i]
        updates.append(writes[t] * (rows(vals, t) - said))
        passed.append(jnp.ones((heads, 1), F32))
        out = total * rows(preds, t)
        for i in range(t + 1):
            out = out + (passed[i] * inner(keys[i], queries[t])) * updates[i]
        outs.append(out)
    final = [passed[i] * updates[i] for i in range(NEW)]
    for h in range(heads):
        state = memory_ref[h] * total[h : h + 1, :]
        for i in range(NEW):
            at = h * SUBS + NEW + i
            state = state + turned[:, at : at + 1] * final[i][h : h + 1, :]
        fresh_ref[h] = state
    store = pltpu.make_async_copy(fresh_ref, memory_out, out_sem)
    store.start()
    for t, out in enumerate(outs):
        out = out * lax.rsqrt(jnp.mean(out * out, axis=1, keepdims=True) + epsilon)
        gate = rows(vals, NEW + t)
        silu = gate * (1.0 / (1.0 + jnp.exp(-gate)))
        copies[t * heads : (t + 1) * heads, :] = out * gain_ref[...] * silu
    mixed = copies[...].astype(BF16)
    for d in range(mixed_out.shape[0]):
        mixed_out[d] = mixed
    store.wait()


def project_kernel(place_ref, mixed_ref, w_hbm, out_ref, w_ref, sem):
    fetch = pltpu.make_async_copy(w_hbm, w_ref, sem)
    fetch.start()
    heads = w_ref.shape[0] // DV
    total = mixed_ref.shape[0]
    packed = out_ref.shape[0]
    place = place_ref[...]
    head_of = iota((1, total), 1) & (heads - 1)
    row = iota((packed, total), 0)
    mixed = mixed_ref[...]
    rows = []
    for h in range(heads):
        pick = jnp.where(row == jnp.where(head_of == h, place, -1), 1.0, 0.0).astype(BF16)
        rows.append(dot(pick, mixed).astype(BF16))
    fetch.wait()
    sum_ = None
    for h in range(heads):
        term = dot(rows[h], w_ref[h * DV : (h + 1) * DV, :])
        sum_ = term if sum_ is None else sum_ + term
    out_ref[...] = sum_


def picker(lengths_ref, packed, total_rows):
    col = iota((1, total_rows), 1)
    place = places(lengths_ref, lax.shift_right_logical(col, 2), col & 3)
    return jnp.where(iota((packed, total_rows), 0) == place, 1.0, 0.0).astype(BF16)


def blocks_of(granules, tiles, receiver):
    first = (receiver * granules) // tiles
    last = (receiver * granules + granules - 1) // tiles
    return first, last


def up_kernel(granules, extra, *refs):
    *terms, base_ref, gain_ref, wg_ref, wu_ref, hidden_out, out_ref = refs
    packed = hidden_out.shape[0]
    hidden = base_ref[...]
    for term in terms:
        hidden = hidden + term[...]
    hidden = hidden.astype(BF16)
    hidden_out[...] = hidden
    hidden_f = hidden.astype(F32)
    scaled = (hidden_f * gain_ref[...]).astype(BF16)
    tiles = wg_ref.shape[1] // LANES
    row_blocks = packed // SUBS
    squares = jnp.sum(hidden_f * hidden_f, axis=1, keepdims=True)
    squares = jnp.broadcast_to(squares, (packed, LANES))
    high = squares.astype(BF16).astype(F32)
    halves = jnp.where(iota(squares.shape, 1) < LANES // 2, high, squares - high).astype(BF16)
    step = 4
    for start in range(0, tiles, step):
        stop = min(start + step, tiles)
        span = slice(start * LANES, stop * LANES)
        gate = dot(scaled, wg_ref[:, span])
        up = dot(scaled, wu_ref[:, span])
        for t in range(start, stop):
            lanes = slice((t - start) * LANES, (t - start + 1) * LANES)
            for b in range(row_blocks):
                rows = slice(b * SUBS, (b + 1) * SUBS)
                pair = jnp.concatenate([gate[rows, lanes], up[rows, lanes]], axis=0).astype(BF16)
                d, i = divmod(b * tiles + t, granules)
                out_ref[d, i * 16 : i * 16 + 16, :] = pair
    for d in range(out_ref.shape[0]):
        first, _ = blocks_of(granules, tiles, d)
        for e in range(extra):
            b = min(first + e, row_blocks - 1)
            at = granules * 16 + e * SUBS
            out_ref[d, at : at + SUBS, :] = halves[b * SUBS : (b + 1) * SUBS, :]


def active_kernel(granules, extra, tiles, got_ref, out_ref):
    senders = got_ref.shape[0]
    scales = []
    for e in range(extra):
        at = granules * 16 + e * SUBS
        squares = jnp.sum(got_ref[:, at : at + SUBS, :].astype(F32), axis=0)
        squares = squares[:, :1] + squares[:, LANES // 2 : LANES // 2 + 1]
        scales.append(lax.rsqrt(squares / D + epsilon))
    place = lax.axis_index("kv") if extra > 1 else 0
    for i in range(granules):
        pair = got_ref[0, i * 16 : i * 16 + 16, :].astype(F32)
        for s in range(1, senders):
            pair = pair + got_ref[s, i * 16 : i * 16 + 16, :].astype(F32)
        scale = scales[0]
        if extra > 1:
            ahead = lax.div(place * granules + i, tiles) - lax.div(place * granules, tiles)
            for e in range(1, extra):
                scale = jnp.where(ahead >= e, scales[e], scale)
        gate, up = pair[:SUBS] * scale, pair[SUBS:] * scale
        active = (gate * (1.0 / (1.0 + jnp.exp(-gate))) * up).astype(BF16)
        for d in range(senders):
            out_ref[d, i * SUBS : (i + 1) * SUBS, :] = active


def down_kernel(got_ref, w_ref, out_ref):
    packed = out_ref.shape[0]
    tiles = w_ref.shape[0] // LANES
    sum_ = None
    for t in range(tiles):
        parts = [
            got_ref[(b * tiles + t) * SUBS : (b * tiles + t + 1) * SUBS, :].astype(F32)
            for b in range(packed // SUBS)
        ]
        term = dot(jnp.concatenate(parts, axis=0).astype(BF16), w_ref[t * LANES : (t + 1) * LANES, :])
        sum_ = term if sum_ is None else sum_ + term
    out_ref[...] = sum_


def last_kernel(*refs):
    *terms, hidden_ref, pick_ref, out_ref = refs
    result = terms[0][...]
    for term in terms[1:]:
        result = result + term[...]
    result = (hidden_ref[...].astype(F32) + result).astype(BF16)
    out_ref[...] = lax.dot_general(
        pick_ref[...], result, (((0,), (0,)), ((), ())), preferred_element_type=F32
    ).astype(BF16)


def exchange(blocks):
    return lax.all_to_all(blocks, "kv", 0, 0)


def over_tp(terms):
    if lax.axis_size("tp") == 2:
        return [terms, lax.ppermute(terms, "tp", [(0, 1), (1, 0)])]
    return [lax.psum(terms, "tp")]


def per_device(
    tokens,
    lengths,
    memory,
    norm_gain,
    w_query,
    w_key,
    w_value,
    w_outgate,
    w_alpha,
    w_beta,
    decay_log,
    decay_bias,
    head_gain,
    w_output,
    mlp_gain,
    w_gate,
    w_up,
    w_down,
):
    total_rows, own_width = tokens.shape
    kv = lax.axis_size("kv")
    seq_dev, heads = memory.shape[:2]
    assert seq_dev == 1
    width = heads * DK
    sequences = lengths.shape[0]
    units = w_gate.shape[1]
    packed = -(-(sequences * 7 // 4) // SUBS) * SUBS
    tiles = units // LANES
    granules = -(-(tiles * packed // SUBS) // kv)
    last_receiver = (tiles * packed // SUBS - 1) // granules
    extra = max(b - a + 1 for a, b in (blocks_of(granules, tiles, d) for d in range(last_receiver + 1)))
    columns = 2 * width + LANES

    operands = [lengths, tokens, norm_gain[None], w_alpha.T, w_beta.T, w_query, w_key, w_value, w_outgate]
    sent, base, pick, place, own = call(
        functools.partial(front_kernel, heads),
        [
            shape((2 * total_rows, columns), BF16),
            shape((packed, own_width), F32),
            shape((packed, total_rows), BF16),
            shape((1, kv * NEW * heads), jnp.int32),
            shape((SUBS, LANES), jnp.int32),
        ],
        operands,
        [HBM] * len(operands),
        16,
        4 * total_rows * own_width * 4 * width,
        "front",
        [pltpu.SMEM(lengths.shape, jnp.int32), *(room(x) for x in operands[1:]), pltpu.SemaphoreType.DMA((len(operands),))],
    )
    got = exchange(sent.reshape(kv, SUBS, columns)).reshape(kv * SUBS, columns)
    new_memory, sent = call(
        recur_kernel,
        [shape((heads, DK, DV), F32), shape((kv, NEW * heads, DV), BF16)],
        [own, got, memory[0], decay_log[None], decay_bias[None], head_gain[None]],
        [VMEM, VMEM, HBM, VMEM, VMEM, VMEM],
        16,
        4 << 30,
        "recur",
        [
            pltpu.VMEM((LANES, LANES), F32),
            pltpu.VMEM((heads * SUBS, DV), F32),
            pltpu.VMEM((heads * SUBS, DV), F32),
            pltpu.VMEM((NEW * heads, DV), F32),
            pltpu.VMEM((heads, DK, DV), F32),
            pltpu.VMEM((heads, DK, DV), F32),
            pltpu.SemaphoreType.DMA,
            pltpu.SemaphoreType.DMA,
        ],
        [HBM, VMEM],
    )
    got = exchange(sent).reshape(kv * NEW * heads, DV)
    (attn,) = call(
        project_kernel,
        [shape((packed, own_width), F32)],
        [place, got, w_output],
        [VMEM, VMEM, HBM],
        8,
        32 << 20,
        "project",
        [room(w_output), pltpu.SemaphoreType.DMA],
    )
    terms = over_tp(attn)
    hidden, sent = call(
        functools.partial(up_kernel, granules, extra),
        [shape((packed, own_width), BF16), shape((kv, granules * 16 + extra * SUBS, LANES), BF16)],
        [*terms, base, mlp_gain[None], w_gate, w_up],
        [VMEM] * (len(terms) + 4),
        16,
        4 * packed * own_width * units,
        "up",
    )
    (sent,) = call(
        functools.partial(active_kernel, granules, extra, tiles),
        [shape((kv, granules * SUBS, LANES), BF16)],
        [exchange(sent)],
        [VMEM],
        8,
        1 << 20,
        "active",
    )
    got = exchange(sent).reshape(kv * granules * SUBS, LANES)
    (feed,) = call(
        down_kernel,
        [shape((packed, own_width), F32)],
        [got, w_down],
        [VMEM] * 2,
        16,
        2 * packed * own_width * units,
        "down",
    )
    terms = over_tp(feed)
    (layer_out,) = call(
        last_kernel,
        [shape((total_rows, own_width), BF16)],
        [*terms, hidden, pick],
        [VMEM] * (len(terms) + 2),
        8,
        1 << 20,
        "last",
    )
    return (layer_out, new_memory[None])


def solution(mesh):
    placed = (
        P(None, "kv"),
        P(),
        P("kv", "tp", None, None),
        P("kv"),
        P("kv", "tp"),
        P("kv", "tp"),
        P("kv", "tp"),
        P("kv", "tp"),
        P("kv", None),
        P("kv", None),
        P("tp"),
        P("tp"),
        P(),
        P("tp", "kv"),
        P("kv"),
        P("kv", "tp"),
        P("kv", "tp"),
        P("tp", "kv"),
    )
    return jax.shard_map(
        per_device,
        mesh=mesh,
        in_specs=placed,
        out_specs=(P(None, "kv"), P("kv", "tp", None, None)),
        check_vma=False,
    )
```

```python
import functools

import jax
import jax.numpy as jnp
from jax import lax
from jax.experimental import pallas as pl
from jax.experimental.pallas import tpu as pltpu
from jax.sharding import PartitionSpec as P

D = 4096
DK = 128
DV = 128
NEW = 4
LANES = 128
PLANE = 4
SUBS = 8

epsilon = 1e-06


F32 = jnp.float32
BF16 = jnp.bfloat16
VMEM = pl.BlockSpec(memory_space=pltpu.VMEM)
HBM = pl.BlockSpec(memory_space=pltpu.HBM)


def call(body, outs, ins, specs, limit, flops, name, scratch=(), out_specs=None):
    moved = sum(x.size * x.dtype.itemsize for x in (*outs, *ins))
    ins = [pltpu.with_memory_space_constraint(x, pltpu.HBM) if s is HBM else x for x, s in zip(ins, specs)]
    return pl.pallas_call(
        body,
        out_shape=outs,
        in_specs=specs,
        out_specs=out_specs or [VMEM] * len(outs),
        scratch_shapes=list(scratch),
        compiler_params=pltpu.CompilerParams(vmem_limit_bytes=limit << 20),
        cost_estimate=pl.CostEstimate(flops=flops, bytes_accessed=moved, transcendentals=0),
        name=name,
    )(*ins)


def room(x):
    return pltpu.VMEM(x.shape, x.dtype)


def shape(dims, dtype):
    return jax.ShapeDtypeStruct(dims, dtype)


def iota(dims, axis):
    return lax.broadcasted_iota(jnp.int32, dims, axis)


def dot(a, b):
    return jnp.dot(a, b, preferred_element_type=F32)


def dot_nt(a, b):
    return lax.dot_general(a, b, (((1,), (1,)), ((), ())), preferred_element_type=F32)


def places(lengths_ref, sequence_of, slot_of):
    place = jnp.full(sequence_of.shape, -1, jnp.int32)
    start = 0
    for s in range(lengths_ref.shape[0]):
        held = lengths_ref[s]
        mine = (sequence_of == s) & (slot_of < held)
        place = jnp.where(mine, slot_of + start, place)
        start = start + held
    return place


def log2(n):
    assert n & (n - 1) == 0
    return n.bit_length() - 1


def front_kernel(heads, *refs):
    count = 9
    sources, refs = refs[:count], refs[count:]
    *outs, base_ref, pick_ref, place_ref, own_ref = refs[: -count - 2]
    *held, sems, out_ref = refs[-count - 2 :]
    copies = [pltpu.make_async_copy(a, b, sems.at[i]) for i, (a, b) in enumerate(zip(sources, held))]
    for copy in copies:
        copy.start()
    lengths_ref, tokens_ref, gain_ref, wa_ref, wb_ref, wq_ref, wk_ref, wv_ref, wg_ref = held
    total_rows = tokens_ref.shape[0]
    width = wq_ref.shape[1]
    all_heads = wa_ref.shape[0]
    packed = pick_ref.shape[0]
    copies[0].wait()
    own_ref[...] = jnp.full(own_ref.shape, lengths_ref[lax.axis_index("kv")], jnp.int32)
    col = iota(place_ref.shape, 1)
    place_ref[...] = places(
        lengths_ref,
        lax.shift_right_logical(col, log2(NEW * heads)),
        lax.shift_right_logical(col, log2(heads)) & 3,
    )
    pick = picker(lengths_ref, packed, total_rows)
    pick_ref[...] = pick
    dims = (2 * total_rows, total_rows)
    row, col = iota(dims, 0), iota(dims, 1)
    target = lax.shift_left(lax.shift_right_logical(row, 3), 2) + (row & 3)
    hit = target == col
    upper = (row & 7) < NEW
    zero, one = jnp.zeros(dims, F32), jnp.ones(dims, F32)
    place_a = jnp.where(hit & upper, one, zero).astype(BF16)
    place_b = jnp.where(hit & ~upper, one, zero).astype(BF16)
    fill = jnp.zeros((LANES - 2 * all_heads, wa_ref.shape[1]), BF16)
    for copy in copies[1:5]:
        copy.wait()
    tokens = tokens_ref[...]
    base_ref[...] = dot(pick, tokens)
    scaled = (tokens.astype(F32) * gain_ref[...]).astype(BF16)
    left = dot(place_a, scaled).astype(BF16)
    right = dot(place_b, scaled).astype(BF16)
    both = dot(place_a + place_b, tokens)
    squares = jnp.sum(both * both, axis=1, keepdims=True)
    small = dot_nt(left + right, jnp.concatenate([wa_ref[...], wb_ref[...], fill], axis=0))
    lane = iota(small.shape, 1)
    small = jnp.where(lane == 2 * all_heads, jnp.broadcast_to(squares, small.shape), small)
    high = small.astype(BF16).astype(F32)
    first = (iota(small.shape, 0) & 7) < NEW

    def put(columns, values):
        out_ref[:, :, columns] = values.reshape(-1, SUBS, values.shape[1]).astype(BF16)

    put(slice(2 * width, 2 * width + LANES), jnp.where(first, high, small - high))
    copies[5].wait()
    copies[6].wait()
    put(slice(0, width), dot(left, wq_ref[...]) + dot(right, wk_ref[...]))
    copies[7].wait()
    copies[8].wait()
    put(slice(width, 2 * width), dot(left, wv_ref[...]) + dot(right, wg_ref[...]))
    deal(out_ref, outs)


def deal(blocks_ref, outs):
    if len(outs) == 1:
        outs[0][...] = blocks_ref[...]
        return
    plane = lax.axis_index("kv") & (PLANE - 1)
    for d, out in enumerate(outs):
        for z in range(out.shape[0]):
            out[z] = blocks_ref[z * PLANE + (plane ^ d)]


def fold_kernel(rows, columns, axis, half, *refs):
    parts, outs = refs[:PLANE], refs[PLANE:]
    high = lax.shift_right_logical(lax.axis_index("kv"), log2(PLANE))
    for e, out in enumerate(outs):
        total = parts[0][high ^ e].astype(F32)
        for part in parts[1:]:
            total = total + part[high ^ e].astype(F32)
        out[...] = total.astype(out.dtype)
        value = total[rows, columns]
        value = value + pltpu.roll(value, half, axis)
        top = value.astype(BF16).astype(F32)
        value = jnp.where(iota(value.shape, axis) < half, top, value - top)
        out[rows, columns] = value.astype(out.dtype)


def partners(values, shift):
    count = lax.axis_size("kv")
    moved = [lax.ppermute(x, "kv", [(i, i ^ (d << shift)) for i in range(count)]) for d, x in enumerate(values) if d]
    return [values[0], *moved]


def staged():
    return lax.axis_size("kv") == PLANE * PLANE


def dealt(dims, kv):
    if staged():
        return [shape((PLANE, *dims), BF16)] * PLANE
    return [shape((kv, *dims), BF16)]


def reduce_scatter(outs, name, *halves):
    if not staged():
        return [exchange(outs[0])]
    dims = outs[0].shape[1:]
    parts = partners(outs, 0)
    sums = call(
        functools.partial(fold_kernel, *halves),
        [shape(dims, F32 if e == 0 else BF16) for e in range(PLANE)],
        parts,
        [VMEM] * PLANE,
        8,
        1 << 20,
        name,
    )
    return [x[None] for x in partners(sums, log2(PLANE))]


def block_sum(refs, rows, columns):
    total = None
    for ref in refs:
        for i in range(ref.shape[0]):
            term = ref[i, rows, columns].astype(F32)
            total = term if total is None else total + term
    return total


def row_sum(refs, start, columns):
    return block_sum(refs, slice(None), slice(start, start + columns))


def recur_kernel(*refs):
    own_ref, *got_ref = refs[:-17]
    sources, (memory_out, mixed_out) = refs[-17:-13], refs[-13:-11]
    unit, vals, preds, copies, fresh_ref, *held, sems, out_sem = refs[-11:]
    memory_ref, log_ref, bias_ref, gain_ref = held
    heads = memory_ref.shape[0]
    fetches = [pltpu.make_async_copy(a, b, sems.at[i]) for i, (a, b) in enumerate(zip(sources, held))]
    for fetch in fetches[1:] + fetches[:1]:
        fetch.start()
    width = heads * DK
    all_heads = heads * lax.axis_size("tp")
    tp_place = lax.axis_index("tp")
    small = row_sum(got_ref, 2 * width, LANES)
    small = small + pltpu.roll(small, NEW, 0)
    rstd = lax.rsqrt(small[:, 2 * all_heads : 2 * all_heads + 1] / D + epsilon)
    unit[...] = jnp.zeros(unit.shape, F32)
    factor = jnp.where(iota((SUBS, 1), 0) < NEW, DK ** (-0.5), 1.0)
    for h in range(heads):
        block = (row_sum(got_ref, h * DK, DK) * rstd).astype(BF16).astype(F32)
        norm = lax.rsqrt(jnp.sum(block * block, axis=1, keepdims=True) + epsilon)
        unit[h * SUBS : (h + 1) * SUBS, :] = block * norm * factor
        vals[h * SUBS : (h + 1) * SUBS, :] = (
            (row_sum(got_ref, width + h * DV, DV) * rstd).astype(BF16).astype(F32)
        )
    for fetch in fetches[1:]:
        fetch.wait()
    small = small * rstd
    alphas = pltpu.roll(small, LANES - tp_place * heads, 1)[:, :heads]
    betas = pltpu.roll(small, LANES - all_heads - tp_place * heads, 1)[:, :heads]
    x = alphas + bias_ref[...]
    soft = jnp.maximum(x, 0.0) + jnp.log1p(jnp.exp(-jnp.abs(x)))
    decay = -jnp.exp(log_ref[...]) * soft
    slot = iota(decay.shape, 0)
    live = (slot & 3) < own_ref[:, :heads]
    keep = jnp.exp(jnp.where(live, decay, 0.0))
    write = jnp.where(live, 1.0 / (1.0 + jnp.exp(-betas)), 0.0)
    unit[heads * SUBS : heads * SUBS + SUBS, :heads] = jnp.where(slot < NEW, keep, write)
    turned = unit[...].T
    fetches[0].wait()
    for h in range(heads):
        state = memory_ref[h]
        for j in range(SUBS):
            at = h * SUBS + j
            preds[at : at + 1, :] = jnp.sum(turned[:, at : at + 1] * state, axis=0, keepdims=True)

    def rows(ref, j):
        return ref[pl.ds(j, heads, stride=SUBS), :]

    base = heads * SUBS
    queries = [rows(unit, t) for t in range(NEW)]
    keys = [rows(unit, NEW + t) for t in range(NEW)]
    keeps = [turned[:heads, base + t : base + t + 1] for t in range(NEW)]
    writes = [turned[:heads, base + NEW + t : base + NEW + t + 1] for t in range(NEW)]

    def inner(a, b):
        return jnp.sum(a * b, axis=1, keepdims=True)

    updates, outs = [], []
    passed = []
    total = jnp.ones((heads, 1), F32)
    for t in range(NEW):
        total = total * keeps[t]
        passed = [p * keeps[t] for p in passed]
        said = total * rows(preds, NEW + t)
        for i in range(t):
            said = said + (passed[i] * inner(keys[i], keys[t])) * updates[i]
        updates.append(writes[t] * (rows(vals, t) - said))
        passed.append(jnp.ones((heads, 1), F32))
        out = total * rows(preds, t)
        for i in range(t + 1):
            out = out + (passed[i] * inner(keys[i], queries[t])) * updates[i]
        outs.append(out)
    final = [passed[i] * updates[i] for i in range(NEW)]
    for h in range(heads):
        state = memory_ref[h] * total[h : h + 1, :]
        for i in range(NEW):
            at = h * SUBS + NEW + i
            state = state + turned[:, at : at + 1] * final[i][h : h + 1, :]
        fresh_ref[h] = state
    store = pltpu.make_async_copy(fresh_ref, memory_out, out_sem)
    store.start()
    for t, out in enumerate(outs):
        out = out * lax.rsqrt(jnp.mean(out * out, axis=1, keepdims=True) + epsilon)
        gate = rows(vals, NEW + t)
        silu = gate * (1.0 / (1.0 + jnp.exp(-gate)))
        copies[t * heads : (t + 1) * heads, :] = out * gain_ref[...] * silu
    mixed = copies[...].astype(BF16)
    for d in range(mixed_out.shape[0]):
        mixed_out[d] = mixed
    store.wait()


def project_kernel(place_ref, mixed_ref, w_hbm, out_ref, w_ref, sem):
    fetch = pltpu.make_async_copy(w_hbm, w_ref, sem)
    fetch.start()
    heads = w_ref.shape[0] // DV
    total = mixed_ref.shape[0]
    packed = out_ref.shape[0]
    place = place_ref[...]
    head_of = iota((1, total), 1) & (heads - 1)
    row = iota((packed, total), 0)
    mixed = mixed_ref[...]
    rows = []
    for h in range(heads):
        pick = jnp.where(row == jnp.where(head_of == h, place, -1), 1.0, 0.0).astype(BF16)
        rows.append(dot(pick, mixed).astype(BF16))
    fetch.wait()
    sum_ = None
    for h in range(heads):
        term = dot(rows[h], w_ref[h * DV : (h + 1) * DV, :])
        sum_ = term if sum_ is None else sum_ + term
    out_ref[...] = sum_


def picker(lengths_ref, packed, total_rows):
    col = iota((1, total_rows), 1)
    place = places(lengths_ref, lax.shift_right_logical(col, 2), col & 3)
    return jnp.where(iota((packed, total_rows), 0) == place, 1.0, 0.0).astype(BF16)


def blocks_of(granules, tiles, receiver):
    first = (receiver * granules) // tiles
    last = (receiver * granules + granules - 1) // tiles
    return first, last


def up_kernel(granules, extra, inputs, *refs):
    *terms, base_ref, gain_ref, wg_ref, wu_ref = refs[:inputs]
    hidden_out, *outs = refs[inputs:-1]
    out_ref = refs[-1]
    packed = hidden_out.shape[0]
    hidden = base_ref[...]
    for term in terms:
        hidden = hidden + term[...]
    hidden = hidden.astype(BF16)
    hidden_out[...] = hidden
    hidden_f = hidden.astype(F32)
    scaled = (hidden_f * gain_ref[...]).astype(BF16)
    tiles = wg_ref.shape[1] // LANES
    row_blocks = packed // SUBS
    squares = jnp.sum(hidden_f * hidden_f, axis=1, keepdims=True)
    squares = jnp.broadcast_to(squares, (packed, LANES))
    high = squares.astype(BF16).astype(F32)
    halves = jnp.where(iota(squares.shape, 1) < LANES // 2, high, squares - high).astype(BF16)
    step = 4
    for start in range(0, tiles, step):
        stop = min(start + step, tiles)
        span = slice(start * LANES, stop * LANES)
        gate = dot(scaled, wg_ref[:, span])
        up = dot(scaled, wu_ref[:, span])
        for t in range(start, stop):
            lanes = slice((t - start) * LANES, (t - start + 1) * LANES)
            for b in range(row_blocks):
                rows = slice(b * SUBS, (b + 1) * SUBS)
                pair = jnp.concatenate([gate[rows, lanes], up[rows, lanes]], axis=0).astype(BF16)
                d, i = divmod(b * tiles + t, granules)
                out_ref[d, i * 16 : i * 16 + 16, :] = pair
    for d in range(out_ref.shape[0]):
        first, _ = blocks_of(granules, tiles, d)
        for e in range(extra):
            b = min(first + e, row_blocks - 1)
            at = granules * 16 + e * SUBS
            out_ref[d, at : at + SUBS, :] = halves[b * SUBS : (b + 1) * SUBS, :]
    deal(out_ref, outs)


def active_kernel(granules, extra, tiles, *refs):
    *got, out_ref = refs
    scales = []
    for e in range(extra):
        at = granules * 16 + e * SUBS
        squares = block_sum(got, slice(at, at + SUBS), slice(None))
        squares = squares[:, :1] + squares[:, LANES // 2 : LANES // 2 + 1]
        scales.append(lax.rsqrt(squares / D + epsilon))
    place = lax.axis_index("kv") if extra > 1 else 0
    for i in range(granules):
        pair = block_sum(got, slice(i * 16, i * 16 + 16), slice(None))
        scale = scales[0]
        if extra > 1:
            ahead = lax.div(place * granules + i, tiles) - lax.div(place * granules, tiles)
            for e in range(1, extra):
                scale = jnp.where(ahead >= e, scales[e], scale)
        gate, up = pair[:SUBS] * scale, pair[SUBS:] * scale
        active = (gate * (1.0 / (1.0 + jnp.exp(-gate))) * up).astype(BF16)
        for d in range(out_ref.shape[0]):
            out_ref[d, i * SUBS : (i + 1) * SUBS, :] = active


def down_kernel(got_ref, w_ref, out_ref):
    packed = out_ref.shape[0]
    tiles = w_ref.shape[0] // LANES
    sum_ = None
    for t in range(tiles):
        parts = [
            got_ref[(b * tiles + t) * SUBS : (b * tiles + t + 1) * SUBS, :].astype(F32)
            for b in range(packed // SUBS)
        ]
        term = dot(jnp.concatenate(parts, axis=0).astype(BF16), w_ref[t * LANES : (t + 1) * LANES, :])
        sum_ = term if sum_ is None else sum_ + term
    out_ref[...] = sum_


def last_kernel(*refs):
    *terms, hidden_ref, pick_ref, out_ref = refs
    result = terms[0][...]
    for term in terms[1:]:
        result = result + term[...]
    result = (hidden_ref[...].astype(F32) + result).astype(BF16)
    out_ref[...] = lax.dot_general(
        pick_ref[...], result, (((0,), (0,)), ((), ())), preferred_element_type=F32
    ).astype(BF16)


def exchange(blocks):
    return lax.all_to_all(blocks, "kv", 0, 0)


def over_tp(terms):
    if lax.axis_size("tp") == 2:
        return [terms, lax.ppermute(terms, "tp", [(0, 1), (1, 0)])]
    return [lax.psum(terms, "tp")]


def per_device(
    tokens,
    lengths,
    memory,
    norm_gain,
    w_query,
    w_key,
    w_value,
    w_outgate,
    w_alpha,
    w_beta,
    decay_log,
    decay_bias,
    head_gain,
    w_output,
    mlp_gain,
    w_gate,
    w_up,
    w_down,
):
    total_rows, own_width = tokens.shape
    kv = lax.axis_size("kv")
    seq_dev, heads = memory.shape[:2]
    assert seq_dev == 1
    width = heads * DK
    sequences = lengths.shape[0]
    units = w_gate.shape[1]
    packed = -(-(sequences * 7 // 4) // SUBS) * SUBS
    tiles = units // LANES
    granules = -(-(tiles * packed // SUBS) // kv)
    last_receiver = (tiles * packed // SUBS - 1) // granules
    extra = max(b - a + 1 for a, b in (blocks_of(granules, tiles, d) for d in range(last_receiver + 1)))
    columns = 2 * width + LANES

    operands = [lengths, tokens, norm_gain[None], w_alpha.T, w_beta.T, w_query, w_key, w_value, w_outgate]
    *sent, base, pick, place, own = call(
        functools.partial(front_kernel, heads),
        [
            *dealt((SUBS, columns), kv),
            shape((packed, own_width), F32),
            shape((packed, total_rows), BF16),
            shape((1, kv * NEW * heads), jnp.int32),
            shape((SUBS, LANES), jnp.int32),
        ],
        operands,
        [HBM] * len(operands),
        16,
        4 * total_rows * own_width * 4 * width,
        "front",
        [pltpu.SMEM(lengths.shape, jnp.int32), *(room(x) for x in operands[1:]), pltpu.SemaphoreType.DMA((len(operands),)), pltpu.VMEM((kv, SUBS, columns), BF16)],
    )
    got = reduce_scatter(sent, "fold_rows", slice(None), slice(2 * width, columns), 0, NEW)
    new_memory, sent = call(
        recur_kernel,
        [shape((heads, DK, DV), F32), shape((kv, NEW * heads, DV), BF16)],
        [own, *got, memory[0], decay_log[None], decay_bias[None], head_gain[None]],
        [VMEM] * (1 + len(got)) + [HBM] * 4,
        16,
        4 << 30,
        "recur",
        [
            pltpu.VMEM((LANES, LANES), F32),
            pltpu.VMEM((heads * SUBS, DV), F32),
            pltpu.VMEM((heads * SUBS, DV), F32),
            pltpu.VMEM((NEW * heads, DV), F32),
            pltpu.VMEM((heads, DK, DV), F32),
            pltpu.VMEM((heads, DK, DV), F32),
            pltpu.VMEM((1, heads), F32),
            pltpu.VMEM((1, heads), F32),
            pltpu.VMEM((1, DV), F32),
            pltpu.SemaphoreType.DMA((4,)),
            pltpu.SemaphoreType.DMA,
        ],
        [HBM, VMEM],
    )
    got = exchange(sent).reshape(kv * NEW * heads, DV)
    (attn,) = call(
        project_kernel,
        [shape((packed, own_width), F32)],
        [place, got, w_output],
        [VMEM, VMEM, HBM],
        8,
        32 << 20,
        "project",
        [room(w_output), pltpu.SemaphoreType.DMA],
    )
    terms = over_tp(attn)
    block = (granules * 16 + extra * SUBS, LANES)
    hidden, *sent = call(
        functools.partial(up_kernel, granules, extra, len(terms) + 4),
        [shape((packed, own_width), BF16), *dealt(block, kv)],
        [*terms, base, mlp_gain[None], w_gate, w_up],
        [VMEM] * (len(terms) + 4),
        16,
        4 * packed * own_width * units,
        "up",
        [pltpu.VMEM((kv, *block), BF16)],
    )
    got = reduce_scatter(sent, "fold_units", slice(granules * 16, None), slice(None), 1, LANES // 2)
    (sent,) = call(
        functools.partial(active_kernel, granules, extra, tiles),
        [shape((kv, granules * SUBS, LANES), BF16)],
        got,
        [VMEM] * len(got),
        8,
        1 << 20,
        "active",
    )
    got = exchange(sent).reshape(kv * granules * SUBS, LANES)
    (feed,) = call(
        down_kernel,
        [shape((packed, own_width), F32)],
        [got, w_down],
        [VMEM] * 2,
        16,
        2 * packed * own_width * units,
        "down",
    )
    terms = over_tp(feed)
    (layer_out,) = call(
        last_kernel,
        [shape((total_rows, own_width), BF16)],
        [*terms, hidden, pick],
        [VMEM] * (len(terms) + 2),
        8,
        1 << 20,
        "last",
    )
    return (layer_out, new_memory[None])


def solution(mesh):
    placed = (
        P(None, "kv"),
        P(),
        P("kv", "tp", None, None),
        P("kv"),
        P("kv", "tp"),
        P("kv", "tp"),
        P("kv", "tp"),
        P("kv", "tp"),
        P("kv", None),
        P("kv", None),
        P("tp"),
        P("tp"),
        P(),
        P("tp", "kv"),
        P("kv"),
        P("kv", "tp"),
        P("kv", "tp"),
        P("tp", "kv"),
    )
    return jax.shard_map(
        per_device,
        mesh=mesh,
        in_specs=placed,
        out_specs=(P(None, "kv"), P("kv", "tp", None, None)),
        check_vma=False,
    )
```

```python
import functools

import jax
import jax.numpy as jnp
from jax import lax
from jax.experimental import pallas as pl
from jax.experimental.pallas import tpu as pltpu
from jax.sharding import PartitionSpec as P

D = 4096
DK = 128
DV = 128
NEW = 4
LANES = 128
PLANE = 4
SUBS = 8

epsilon = 1e-06


F32 = jnp.float32
BF16 = jnp.bfloat16
VMEM = pl.BlockSpec(memory_space=pltpu.VMEM)
HBM = pl.BlockSpec(memory_space=pltpu.HBM)


def call(body, outs, ins, specs, limit, flops, name, scratch=(), out_specs=None):
    moved = sum(x.size * x.dtype.itemsize for x in (*outs, *ins))
    ins = [pltpu.with_memory_space_constraint(x, pltpu.HBM) if s is HBM else x for x, s in zip(ins, specs)]
    return pl.pallas_call(
        body,
        out_shape=outs,
        in_specs=specs,
        out_specs=out_specs or [VMEM] * len(outs),
        scratch_shapes=list(scratch),
        compiler_params=pltpu.CompilerParams(vmem_limit_bytes=limit << 20),
        cost_estimate=pl.CostEstimate(flops=flops, bytes_accessed=moved, transcendentals=0),
        name=name,
    )(*ins)


def room(x):
    return pltpu.VMEM(x.shape, x.dtype)


def shape(dims, dtype):
    return jax.ShapeDtypeStruct(dims, dtype)


def iota(dims, axis):
    return lax.broadcasted_iota(jnp.int32, dims, axis)


def dot(a, b):
    return jnp.dot(a, b, preferred_element_type=F32)


def dot_nt(a, b):
    return lax.dot_general(a, b, (((1,), (1,)), ((), ())), preferred_element_type=F32)


def places(lengths_ref, sequence_of, slot_of):
    place = jnp.full(sequence_of.shape, -1, jnp.int32)
    start = 0
    for s in range(lengths_ref.shape[0]):
        held = lengths_ref[s]
        mine = (sequence_of == s) & (slot_of < held)
        place = jnp.where(mine, slot_of + start, place)
        start = start + held
    return place


def log2(n):
    assert n & (n - 1) == 0
    return n.bit_length() - 1


def front_kernel(heads, *refs):
    count = 9
    sources, refs = refs[:count], refs[count:]
    *outs, base_ref, pick_ref, place_ref, own_ref = refs[: -count - 2]
    *held, sems, out_ref = refs[-count - 2 :]
    copies = [pltpu.make_async_copy(a, b, sems.at[i]) for i, (a, b) in enumerate(zip(sources, held))]
    for copy in copies:
        copy.start()
    lengths_ref, tokens_ref, gain_ref, wa_ref, wb_ref, wq_ref, wk_ref, wv_ref, wg_ref = held
    total_rows = tokens_ref.shape[0]
    width = wq_ref.shape[1]
    all_heads = wa_ref.shape[0]
    packed = pick_ref.shape[0]
    copies[0].wait()
    own_ref[...] = jnp.full(own_ref.shape, lengths_ref[lax.axis_index("kv")], jnp.int32)
    col = iota(place_ref.shape, 1)
    place_ref[...] = places(
        lengths_ref,
        lax.shift_right_logical(col, log2(NEW * heads)),
        lax.shift_right_logical(col, log2(heads)) & 3,
    )
    pick = picker(lengths_ref, packed, total_rows)
    pick_ref[...] = pick
    dims = (2 * total_rows, total_rows)
    row, col = iota(dims, 0), iota(dims, 1)
    target = lax.shift_left(lax.shift_right_logical(row, 3), 2) + (row & 3)
    hit = target == col
    upper = (row & 7) < NEW
    zero, one = jnp.zeros(dims, F32), jnp.ones(dims, F32)
    place_a = jnp.where(hit & upper, one, zero).astype(BF16)
    place_b = jnp.where(hit & ~upper, one, zero).astype(BF16)
    fill = jnp.zeros((LANES - 2 * all_heads, wa_ref.shape[1]), BF16)
    for copy in copies[1:5]:
        copy.wait()
    tokens = tokens_ref[...]
    base_ref[...] = dot(pick, tokens)
    scaled = (tokens.astype(F32) * gain_ref[...]).astype(BF16)
    left = dot(place_a, scaled).astype(BF16)
    right = dot(place_b, scaled).astype(BF16)
    both = dot(place_a + place_b, tokens)
    squares = jnp.sum(both * both, axis=1, keepdims=True)
    small = dot_nt(left + right, jnp.concatenate([wa_ref[...], wb_ref[...], fill], axis=0))
    lane = iota(small.shape, 1)
    small = jnp.where(lane == 2 * all_heads, jnp.broadcast_to(squares, small.shape), small)
    high = small.astype(BF16).astype(F32)
    first = (iota(small.shape, 0) & 7) < NEW

    def put(columns, values):
        out_ref[:, :, columns] = values.reshape(-1, SUBS, values.shape[1]).astype(BF16)

    put(slice(2 * width, 2 * width + LANES), jnp.where(first, high, small - high))
    copies[5].wait()
    copies[6].wait()
    put(slice(0, width), dot(left, wq_ref[...]) + dot(right, wk_ref[...]))
    copies[7].wait()
    copies[8].wait()
    put(slice(width, 2 * width), dot(left, wv_ref[...]) + dot(right, wg_ref[...]))
    deal(out_ref, outs)


def deal(blocks_ref, outs):
    if len(outs) == 1:
        outs[0][...] = blocks_ref[...]
        return
    plane = lax.axis_index("kv") & (PLANE - 1)
    for d, out in enumerate(outs):
        for z in range(out.shape[0]):
            out[z] = blocks_ref[z * PLANE + (plane ^ d)]


def fold_kernel(rows, columns, axis, half, *refs):
    parts, outs = refs[:PLANE], refs[PLANE:]
    high = lax.shift_right_logical(lax.axis_index("kv"), log2(PLANE))
    for e, out in enumerate(outs):
        total = parts[0][high ^ e].astype(F32)
        for part in parts[1:]:
            total = total + part[high ^ e].astype(F32)
        out[...] = total.astype(out.dtype)
        value = total[rows, columns]
        value = value + pltpu.roll(value, half, axis)
        top = value.astype(BF16).astype(F32)
        value = jnp.where(iota(value.shape, axis) < half, top, value - top)
        out[rows, columns] = value.astype(out.dtype)


def partners(values, shift):
    count = lax.axis_size("kv")
    moved = [lax.ppermute(x, "kv", [(i, i ^ (d << shift)) for i in range(count)]) for d, x in enumerate(values) if d]
    return [values[0], *moved]


def staged():
    return lax.axis_size("kv") == PLANE * PLANE


def dealt(dims, kv):
    if staged():
        return [shape((PLANE, *dims), BF16)] * PLANE
    return [shape((kv, *dims), BF16)]


def reduce_scatter(outs, name, *halves):
    if not staged():
        return [exchange(outs[0])]
    dims = outs[0].shape[1:]
    parts = partners(outs, 0)
    sums = call(
        functools.partial(fold_kernel, *halves),
        [shape(dims, F32 if e == 0 else BF16) for e in range(PLANE)],
        parts,
        [VMEM] * PLANE,
        8,
        1 << 20,
        name,
    )
    return [x[None] for x in partners(sums, log2(PLANE))]


def stack_kernel(*refs):
    *parts, out_ref = refs
    for e, part in enumerate(parts):
        out_ref[e] = part[...]


def copies_to_send(kv):
    return 1 if staged() else kv


def gather(sent, name):
    if not staged():
        return [exchange(sent)]
    block = sent[0]
    parts = partners([block] * PLANE, log2(PLANE))
    (stacked,) = call(
        stack_kernel, [shape((PLANE, *block.shape), block.dtype)], parts, [VMEM] * PLANE, 8, 1 << 20, name
    )
    return partners([stacked] * PLANE, 0)


def collect(refs, room_ref):
    if len(refs) == 1:
        return refs[0]
    place = lax.axis_index("kv")
    for d, ref in enumerate(refs):
        for e in range(PLANE):
            room_ref[place ^ (e * PLANE + d)] = ref[e]
    return room_ref


def block_sum(refs, rows, columns):
    total = None
    for ref in refs:
        for i in range(ref.shape[0]):
            term = ref[i, rows, columns].astype(F32)
            total = term if total is None else total + term
    return total


def row_sum(refs, start, columns):
    return block_sum(refs, slice(None), slice(start, start + columns))


def recur_kernel(*refs):
    own_ref, *got_ref = refs[:-17]
    sources, (memory_out, mixed_out) = refs[-17:-13], refs[-13:-11]
    unit, vals, preds, copies, fresh_ref, *held, sems, out_sem = refs[-11:]
    memory_ref, log_ref, bias_ref, gain_ref = held
    heads = memory_ref.shape[0]
    fetches = [pltpu.make_async_copy(a, b, sems.at[i]) for i, (a, b) in enumerate(zip(sources, held))]
    for fetch in fetches[1:] + fetches[:1]:
        fetch.start()
    width = heads * DK
    all_heads = heads * lax.axis_size("tp")
    tp_place = lax.axis_index("tp")
    small = row_sum(got_ref, 2 * width, LANES)
    small = small + pltpu.roll(small, NEW, 0)
    rstd = lax.rsqrt(small[:, 2 * all_heads : 2 * all_heads + 1] / D + epsilon)
    unit[...] = jnp.zeros(unit.shape, F32)
    factor = jnp.where(iota((SUBS, 1), 0) < NEW, DK ** (-0.5), 1.0)
    for h in range(heads):
        block = (row_sum(got_ref, h * DK, DK) * rstd).astype(BF16).astype(F32)
        norm = lax.rsqrt(jnp.sum(block * block, axis=1, keepdims=True) + epsilon)
        unit[h * SUBS : (h + 1) * SUBS, :] = block * norm * factor
        vals[h * SUBS : (h + 1) * SUBS, :] = (
            (row_sum(got_ref, width + h * DV, DV) * rstd).astype(BF16).astype(F32)
        )
    for fetch in fetches[1:]:
        fetch.wait()
    small = small * rstd
    alphas = pltpu.roll(small, LANES - tp_place * heads, 1)[:, :heads]
    betas = pltpu.roll(small, LANES - all_heads - tp_place * heads, 1)[:, :heads]
    x = alphas + bias_ref[...]
    soft = jnp.maximum(x, 0.0) + jnp.log1p(jnp.exp(-jnp.abs(x)))
    decay = -jnp.exp(log_ref[...]) * soft
    slot = iota(decay.shape, 0)
    live = (slot & 3) < own_ref[:, :heads]
    keep = jnp.exp(jnp.where(live, decay, 0.0))
    write = jnp.where(live, 1.0 / (1.0 + jnp.exp(-betas)), 0.0)
    unit[heads * SUBS : heads * SUBS + SUBS, :heads] = jnp.where(slot < NEW, keep, write)
    turned = unit[...].T
    fetches[0].wait()
    for h in range(heads):
        state = memory_ref[h]
        for j in range(SUBS):
            at = h * SUBS + j
            preds[at : at + 1, :] = jnp.sum(turned[:, at : at + 1] * state, axis=0, keepdims=True)

    def rows(ref, j):
        return ref[pl.ds(j, heads, stride=SUBS), :]

    base = heads * SUBS
    queries = [rows(unit, t) for t in range(NEW)]
    keys = [rows(unit, NEW + t) for t in range(NEW)]
    keeps = [turned[:heads, base + t : base + t + 1] for t in range(NEW)]
    writes = [turned[:heads, base + NEW + t : base + NEW + t + 1] for t in range(NEW)]

    def inner(a, b):
        return jnp.sum(a * b, axis=1, keepdims=True)

    updates, outs = [], []
    passed = []
    total = jnp.ones((heads, 1), F32)
    for t in range(NEW):
        total = total * keeps[t]
        passed = [p * keeps[t] for p in passed]
        said = total * rows(preds, NEW + t)
        for i in range(t):
            said = said + (passed[i] * inner(keys[i], keys[t])) * updates[i]
        updates.append(writes[t] * (rows(vals, t) - said))
        passed.append(jnp.ones((heads, 1), F32))
        out = total * rows(preds, t)
        for i in range(t + 1):
            out = out + (passed[i] * inner(keys[i], queries[t])) * updates[i]
        outs.append(out)
    final = [passed[i] * updates[i] for i in range(NEW)]
    for h in range(heads):
        state = memory_ref[h] * total[h : h + 1, :]
        for i in range(NEW):
            at = h * SUBS + NEW + i
            state = state + turned[:, at : at + 1] * final[i][h : h + 1, :]
        fresh_ref[h] = state
    store = pltpu.make_async_copy(fresh_ref, memory_out, out_sem)
    store.start()
    for t, out in enumerate(outs):
        out = out * lax.rsqrt(jnp.mean(out * out, axis=1, keepdims=True) + epsilon)
        gate = rows(vals, NEW + t)
        silu = gate * (1.0 / (1.0 + jnp.exp(-gate)))
        copies[t * heads : (t + 1) * heads, :] = out * gain_ref[...] * silu
    mixed = copies[...].astype(BF16)
    for d in range(mixed_out.shape[0]):
        mixed_out[d] = mixed
    store.wait()


def project_kernel(place_ref, *refs):
    *got, w_hbm, out_ref, w_ref, sem, room_ref = refs
    fetch = pltpu.make_async_copy(w_hbm, w_ref, sem)
    fetch.start()
    heads = w_ref.shape[0] // DV
    mixed_ref = collect(got, room_ref)
    total = mixed_ref.shape[0] * mixed_ref.shape[1]
    packed = out_ref.shape[0]
    place = place_ref[...]
    head_of = iota((1, total), 1) & (heads - 1)
    row = iota((packed, total), 0)
    mixed = mixed_ref[...].reshape(total, DV)
    rows = []
    for h in range(heads):
        pick = jnp.where(row == jnp.where(head_of == h, place, -1), 1.0, 0.0).astype(BF16)
        rows.append(dot(pick, mixed).astype(BF16))
    fetch.wait()
    sum_ = None
    for h in range(heads):
        term = dot(rows[h], w_ref[h * DV : (h + 1) * DV, :])
        sum_ = term if sum_ is None else sum_ + term
    out_ref[...] = sum_


def picker(lengths_ref, packed, total_rows):
    col = iota((1, total_rows), 1)
    place = places(lengths_ref, lax.shift_right_logical(col, 2), col & 3)
    return jnp.where(iota((packed, total_rows), 0) == place, 1.0, 0.0).astype(BF16)


def blocks_of(granules, tiles, receiver):
    first = (receiver * granules) // tiles
    last = (receiver * granules + granules - 1) // tiles
    return first, last


def up_kernel(granules, extra, inputs, *refs):
    *terms, base_ref, gain_ref, wg_ref, wu_ref = refs[:inputs]
    hidden_out, *outs = refs[inputs:-1]
    out_ref = refs[-1]
    packed = hidden_out.shape[0]
    hidden = base_ref[...]
    for term in terms:
        hidden = hidden + term[...]
    hidden = hidden.astype(BF16)
    hidden_out[...] = hidden
    hidden_f = hidden.astype(F32)
    scaled = (hidden_f * gain_ref[...]).astype(BF16)
    tiles = wg_ref.shape[1] // LANES
    row_blocks = packed // SUBS
    squares = jnp.sum(hidden_f * hidden_f, axis=1, keepdims=True)
    squares = jnp.broadcast_to(squares, (packed, LANES))
    high = squares.astype(BF16).astype(F32)
    halves = jnp.where(iota(squares.shape, 1) < LANES // 2, high, squares - high).astype(BF16)
    step = 4
    for start in range(0, tiles, step):
        stop = min(start + step, tiles)
        span = slice(start * LANES, stop * LANES)
        gate = dot(scaled, wg_ref[:, span])
        up = dot(scaled, wu_ref[:, span])
        for t in range(start, stop):
            lanes = slice((t - start) * LANES, (t - start + 1) * LANES)
            for b in range(row_blocks):
                rows = slice(b * SUBS, (b + 1) * SUBS)
                pair = jnp.concatenate([gate[rows, lanes], up[rows, lanes]], axis=0).astype(BF16)
                d, i = divmod(b * tiles + t, granules)
                out_ref[d, i * 16 : i * 16 + 16, :] = pair
    for d in range(out_ref.shape[0]):
        first, _ = blocks_of(granules, tiles, d)
        for e in range(extra):
            b = min(first + e, row_blocks - 1)
            at = granules * 16 + e * SUBS
            out_ref[d, at : at + SUBS, :] = halves[b * SUBS : (b + 1) * SUBS, :]
    deal(out_ref, outs)


def active_kernel(granules, extra, tiles, *refs):
    *got, out_ref = refs
    scales = []
    for e in range(extra):
        at = granules * 16 + e * SUBS
        squares = block_sum(got, slice(at, at + SUBS), slice(None))
        squares = squares[:, :1] + squares[:, LANES // 2 : LANES // 2 + 1]
        scales.append(lax.rsqrt(squares / D + epsilon))
    place = lax.axis_index("kv") if extra > 1 else 0
    for i in range(granules):
        pair = block_sum(got, slice(i * 16, i * 16 + 16), slice(None))
        scale = scales[0]
        if extra > 1:
            ahead = lax.div(place * granules + i, tiles) - lax.div(place * granules, tiles)
            for e in range(1, extra):
                scale = jnp.where(ahead >= e, scales[e], scale)
        gate, up = pair[:SUBS] * scale, pair[SUBS:] * scale
        active = (gate * (1.0 / (1.0 + jnp.exp(-gate))) * up).astype(BF16)
        for d in range(out_ref.shape[0]):
            out_ref[d, i * SUBS : (i + 1) * SUBS, :] = active


def down_kernel(granules, *refs):
    *got, w_ref, out_ref, room_ref = refs
    got_ref = collect(got, room_ref)
    packed = out_ref.shape[0]
    tiles = w_ref.shape[0] // LANES
    sum_ = None
    for t in range(tiles):
        spots = [divmod(b * tiles + t, granules) for b in range(packed // SUBS)]
        parts = [got_ref[d, i * SUBS : (i + 1) * SUBS, :].astype(F32) for d, i in spots]
        term = dot(jnp.concatenate(parts, axis=0).astype(BF16), w_ref[t * LANES : (t + 1) * LANES, :])
        sum_ = term if sum_ is None else sum_ + term
    out_ref[...] = sum_


def last_kernel(*refs):
    *terms, hidden_ref, pick_ref, out_ref = refs
    result = terms[0][...]
    for term in terms[1:]:
        result = result + term[...]
    result = (hidden_ref[...].astype(F32) + result).astype(BF16)
    out_ref[...] = lax.dot_general(
        pick_ref[...], result, (((0,), (0,)), ((), ())), preferred_element_type=F32
    ).astype(BF16)


def exchange(blocks):
    return lax.all_to_all(blocks, "kv", 0, 0)


def over_tp(terms):
    if lax.axis_size("tp") == 2:
        return [terms, lax.ppermute(terms, "tp", [(0, 1), (1, 0)])]
    return [lax.psum(terms, "tp")]


def per_device(
    tokens,
    lengths,
    memory,
    norm_gain,
    w_query,
    w_key,
    w_value,
    w_outgate,
    w_alpha,
    w_beta,
    decay_log,
    decay_bias,
    head_gain,
    w_output,
    mlp_gain,
    w_gate,
    w_up,
    w_down,
):
    total_rows, own_width = tokens.shape
    kv = lax.axis_size("kv")
    seq_dev, heads = memory.shape[:2]
    assert seq_dev == 1
    width = heads * DK
    sequences = lengths.shape[0]
    units = w_gate.shape[1]
    packed = -(-(sequences * 7 // 4) // SUBS) * SUBS
    tiles = units // LANES
    granules = -(-(tiles * packed // SUBS) // kv)
    last_receiver = (tiles * packed // SUBS - 1) // granules
    extra = max(b - a + 1 for a, b in (blocks_of(granules, tiles, d) for d in range(last_receiver + 1)))
    columns = 2 * width + LANES

    operands = [lengths, tokens, norm_gain[None], w_alpha.T, w_beta.T, w_query, w_key, w_value, w_outgate]
    *sent, base, pick, place, own = call(
        functools.partial(front_kernel, heads),
        [
            *dealt((SUBS, columns), kv),
            shape((packed, own_width), F32),
            shape((packed, total_rows), BF16),
            shape((1, kv * NEW * heads), jnp.int32),
            shape((SUBS, LANES), jnp.int32),
        ],
        operands,
        [HBM] * len(operands),
        16,
        4 * total_rows * own_width * 4 * width,
        "front",
        [pltpu.SMEM(lengths.shape, jnp.int32), *(room(x) for x in operands[1:]), pltpu.SemaphoreType.DMA((len(operands),)), pltpu.VMEM((kv, SUBS, columns), BF16)],
    )
    got = reduce_scatter(sent, "fold_rows", slice(None), slice(2 * width, columns), 0, NEW)
    new_memory, sent = call(
        recur_kernel,
        [shape((heads, DK, DV), F32), shape((copies_to_send(kv), NEW * heads, DV), BF16)],
        [own, *got, memory[0], decay_log[None], decay_bias[None], head_gain[None]],
        [VMEM] * (1 + len(got)) + [HBM] * 4,
        16,
        4 << 30,
        "recur",
        [
            pltpu.VMEM((LANES, LANES), F32),
            pltpu.VMEM((heads * SUBS, DV), F32),
            pltpu.VMEM((heads * SUBS, DV), F32),
            pltpu.VMEM((NEW * heads, DV), F32),
            pltpu.VMEM((heads, DK, DV), F32),
            pltpu.VMEM((heads, DK, DV), F32),
            pltpu.VMEM((1, heads), F32),
            pltpu.VMEM((1, heads), F32),
            pltpu.VMEM((1, DV), F32),
            pltpu.SemaphoreType.DMA((4,)),
            pltpu.SemaphoreType.DMA,
        ],
        [HBM, VMEM],
    )
    got = gather(sent, "stack_heads")
    (attn,) = call(
        project_kernel,
        [shape((packed, own_width), F32)],
        [place, *got, w_output],
        [VMEM] * (1 + len(got)) + [HBM],
        8,
        32 << 20,
        "project",
        [room(w_output), pltpu.SemaphoreType.DMA, pltpu.VMEM((kv, NEW * heads, DV), BF16)],
    )
    terms = over_tp(attn)
    block = (granules * 16 + extra * SUBS, LANES)
    hidden, *sent = call(
        functools.partial(up_kernel, granules, extra, len(terms) + 4),
        [shape((packed, own_width), BF16), *dealt(block, kv)],
        [*terms, base, mlp_gain[None], w_gate, w_up],
        [VMEM] * (len(terms) + 4),
        16,
        4 * packed * own_width * units,
        "up",
        [pltpu.VMEM((kv, *block), BF16)],
    )
    got = reduce_scatter(sent, "fold_units", slice(granules * 16, None), slice(None), 1, LANES // 2)
    (sent,) = call(
        functools.partial(active_kernel, granules, extra, tiles),
        [shape((copies_to_send(kv), granules * SUBS, LANES), BF16)],
        got,
        [VMEM] * len(got),
        8,
        1 << 20,
        "active",
    )
    got = gather(sent, "stack_units")
    (feed,) = call(
        functools.partial(down_kernel, granules),
        [shape((packed, own_width), F32)],
        [*got, w_down],
        [VMEM] * (1 + len(got)),
        16,
        2 * packed * own_width * units,
        "down",
        [pltpu.VMEM((kv, granules * SUBS, LANES), BF16)],
    )
    terms = over_tp(feed)
    (layer_out,) = call(
        last_kernel,
        [shape((total_rows, own_width), BF16)],
        [*terms, hidden, pick],
        [VMEM] * (len(terms) + 2),
        8,
        1 << 20,
        "last",
    )
    return (layer_out, new_memory[None])


def solution(mesh):
    placed = (
        P(None, "kv"),
        P(),
        P("kv", "tp", None, None),
        P("kv"),
        P("kv", "tp"),
        P("kv", "tp"),
        P("kv", "tp"),
        P("kv", "tp"),
        P("kv", None),
        P("kv", None),
        P("tp"),
        P("tp"),
        P(),
        P("tp", "kv"),
        P("kv"),
        P("kv", "tp"),
        P("kv", "tp"),
        P("tp", "kv"),
    )
    return jax.shard_map(
        per_device,
        mesh=mesh,
        in_specs=placed,
        out_specs=(P(None, "kv"), P("kv", "tp", None, None)),
        check_vma=False,
    )
```

```python
import functools

import jax
import jax.numpy as jnp
from jax import lax
from jax.experimental import pallas as pl
from jax.experimental.pallas import tpu as pltpu
from jax.sharding import PartitionSpec as P

D = 4096
DK = 128
DV = 128
NEW = 4
LANES = 128
PLANE = 4
SUBS = 8

epsilon = 1e-06


F32 = jnp.float32
BF16 = jnp.bfloat16
VMEM = pl.BlockSpec(memory_space=pltpu.VMEM)
HBM = pl.BlockSpec(memory_space=pltpu.HBM)


def call(body, outs, ins, specs, limit, flops, name, scratch=(), out_specs=None):
    moved = sum(x.size * x.dtype.itemsize for x in (*outs, *ins))
    ins = [pltpu.with_memory_space_constraint(x, pltpu.HBM) if s is HBM else x for x, s in zip(ins, specs)]
    return pl.pallas_call(
        body,
        out_shape=outs,
        in_specs=specs,
        out_specs=out_specs or [VMEM] * len(outs),
        scratch_shapes=list(scratch),
        compiler_params=pltpu.CompilerParams(vmem_limit_bytes=limit << 20),
        cost_estimate=pl.CostEstimate(flops=flops, bytes_accessed=moved, transcendentals=0),
        name=name,
    )(*ins)


def room(x):
    return pltpu.VMEM(x.shape, x.dtype)


def shape(dims, dtype):
    return jax.ShapeDtypeStruct(dims, dtype)


def iota(dims, axis):
    return lax.broadcasted_iota(jnp.int32, dims, axis)


def dot(a, b):
    return jnp.dot(a, b, preferred_element_type=F32)


def dot_nt(a, b):
    return lax.dot_general(a, b, (((1,), (1,)), ((), ())), preferred_element_type=F32)


def places(lengths_ref, sequence_of, slot_of):
    place = jnp.full(sequence_of.shape, -1, jnp.int32)
    start = 0
    for s in range(lengths_ref.shape[0]):
        held = lengths_ref[s]
        mine = (sequence_of == s) & (slot_of < held)
        place = jnp.where(mine, slot_of + start, place)
        start = start + held
    return place


def log2(n):
    assert n & (n - 1) == 0
    return n.bit_length() - 1


def front_kernel(heads, *refs):
    count = 9
    sources, refs = refs[:count], refs[count:]
    *outs, base_ref, pick_ref, place_ref, own_ref = refs[: -count - 2]
    *held, sems, out_ref = refs[-count - 2 :]
    copies = [pltpu.make_async_copy(a, b, sems.at[i]) for i, (a, b) in enumerate(zip(sources, held))]
    for copy in copies:
        copy.start()
    lengths_ref, tokens_ref, gain_ref, wa_ref, wb_ref, wq_ref, wk_ref, wv_ref, wg_ref = held
    total_rows = tokens_ref.shape[0]
    width = wq_ref.shape[1]
    all_heads = wa_ref.shape[0]
    packed = pick_ref.shape[0]
    copies[0].wait()
    own_ref[...] = jnp.full(own_ref.shape, lengths_ref[lax.axis_index("kv")], jnp.int32)
    col = iota(place_ref.shape, 1)
    place_ref[...] = places(
        lengths_ref,
        lax.shift_right_logical(col, log2(NEW * heads)),
        lax.shift_right_logical(col, log2(heads)) & 3,
    )
    pick = picker(lengths_ref, packed, total_rows)
    pick_ref[...] = pick
    dims = (2 * total_rows, total_rows)
    row, col = iota(dims, 0), iota(dims, 1)
    target = lax.shift_left(lax.shift_right_logical(row, 3), 2) + (row & 3)
    hit = target == col
    upper = (row & 7) < NEW
    zero, one = jnp.zeros(dims, F32), jnp.ones(dims, F32)
    place_a = jnp.where(hit & upper, one, zero).astype(BF16)
    place_b = jnp.where(hit & ~upper, one, zero).astype(BF16)
    fill = jnp.zeros((LANES - 2 * all_heads, wa_ref.shape[1]), BF16)
    for copy in copies[1:5]:
        copy.wait()
    tokens = tokens_ref[...]
    base_ref[...] = dot(pick, tokens)
    scaled = (tokens.astype(F32) * gain_ref[...]).astype(BF16)
    left = dot(place_a, scaled).astype(BF16)
    right = dot(place_b, scaled).astype(BF16)
    both = dot(place_a + place_b, tokens)
    squares = jnp.sum(both * both, axis=1, keepdims=True)
    small = dot_nt(left + right, jnp.concatenate([wa_ref[...], wb_ref[...], fill], axis=0))
    lane = iota(small.shape, 1)
    small = jnp.where(lane == 2 * all_heads, jnp.broadcast_to(squares, small.shape), small)
    high = small.astype(BF16).astype(F32)
    first = (iota(small.shape, 0) & 7) < NEW

    def put(columns, values):
        out_ref[:, :, columns] = values.reshape(-1, SUBS, values.shape[1]).astype(BF16)

    put(slice(2 * width, 2 * width + LANES), jnp.where(first, high, small - high))
    copies[5].wait()
    copies[6].wait()
    put(slice(0, width), dot(left, wq_ref[...]) + dot(right, wk_ref[...]))
    copies[7].wait()
    copies[8].wait()
    put(slice(width, 2 * width), dot(left, wv_ref[...]) + dot(right, wg_ref[...]))
    deal(out_ref, outs)


def deal(blocks_ref, outs):
    if len(outs) == 1:
        outs[0][...] = blocks_ref[...]
        return
    plane = lax.axis_index("kv") & (PLANE - 1)
    for d, out in enumerate(outs):
        for z in range(out.shape[0]):
            out[z] = blocks_ref[z * PLANE + (plane ^ d)]


def fold_kernel(rows, columns, axis, half, *refs):
    parts, outs = refs[:PLANE], refs[PLANE:]
    high = lax.shift_right_logical(lax.axis_index("kv"), log2(PLANE))
    for e, out in enumerate(outs):
        total = parts[0][high ^ e].astype(F32)
        for part in parts[1:]:
            total = total + part[high ^ e].astype(F32)
        out[...] = total.astype(out.dtype)
        value = total[rows, columns]
        value = value + pltpu.roll(value, half, axis)
        top = value.astype(BF16).astype(F32)
        value = jnp.where(iota(value.shape, axis) < half, top, value - top)
        out[rows, columns] = value.astype(out.dtype)


def partners(values, shift):
    count = lax.axis_size("kv")
    moved = []
    for d in reversed(range(1, len(values))):
        moved.append(lax.ppermute(values[d], "kv", [(i, i ^ (d << shift)) for i in range(count)]))
    return [values[0], *moved]


def staged():
    return lax.axis_size("kv") == PLANE * PLANE


def dealt(dims, kv):
    if staged():
        return [shape((PLANE, *dims), BF16)] * PLANE
    return [shape((kv, *dims), BF16)]


def reduce_scatter(outs, name, *halves):
    if not staged():
        return [exchange(outs[0])]
    dims = outs[0].shape[1:]
    parts = partners(outs, 0)
    sums = call(
        functools.partial(fold_kernel, *halves),
        [shape(dims, F32 if e == 0 else BF16) for e in range(PLANE)],
        parts,
        [VMEM] * PLANE,
        8,
        1 << 20,
        name,
    )
    return [x[None] for x in partners(sums, log2(PLANE))]


def block_sum(refs, rows, columns):
    total = None
    for ref in refs:
        for i in range(ref.shape[0]):
            term = ref[i, rows, columns].astype(F32)
            total = term if total is None else total + term
    return total


def row_sum(refs, start, columns):
    return block_sum(refs, slice(None), slice(start, start + columns))


def recur_kernel(*refs):
    own_ref, *got_ref = refs[:-19]
    sources, (memory_out, mixed_out) = refs[-19:-15], refs[-15:-13]
    gates, unit, vals, preds, late, copies, fresh_ref, *held, sems, out_sem = refs[-13:]
    memory_ref, log_ref, bias_ref, gain_ref = held
    heads = memory_ref.shape[0]
    fetches = [pltpu.make_async_copy(a, b, sems.at[i]) for i, (a, b) in enumerate(zip(sources, held))]
    for fetch in fetches[1:] + fetches[:1]:
        fetch.start()
    width = heads * DK
    all_heads = heads * lax.axis_size("tp")
    tp_place = lax.axis_index("tp")
    small = row_sum(got_ref, 2 * width, LANES)
    small = small + pltpu.roll(small, NEW, 0)
    rstd = lax.rsqrt(small[:, 2 * all_heads : 2 * all_heads + 1] / D + epsilon)
    gates[...] = jnp.zeros(gates.shape, F32)
    factor = jnp.where(iota((SUBS, 1), 0) < NEW, DK ** (-0.5), 1.0)
    for h in range(heads):
        block = (row_sum(got_ref, h * DK, DK) * rstd).astype(BF16).astype(F32)
        norm = lax.rsqrt(jnp.sum(block * block, axis=1, keepdims=True) + epsilon)
        unit[h * SUBS : (h + 1) * SUBS, :] = block * norm * factor
        vals[h * SUBS : (h + 1) * SUBS, :] = (
            (row_sum(got_ref, width + h * DV, DV) * rstd).astype(BF16).astype(F32)
        )
    for fetch in fetches[1:]:
        fetch.wait()
    small = small * rstd
    alphas = pltpu.roll(small, LANES - tp_place * heads, 1)[:, :heads]
    betas = pltpu.roll(small, LANES - all_heads - tp_place * heads, 1)[:, :heads]
    x = alphas + bias_ref[...]
    soft = jnp.maximum(x, 0.0) + jnp.log1p(jnp.exp(-jnp.abs(x)))
    decay = -jnp.exp(log_ref[...]) * soft
    slot = iota(decay.shape, 0)
    live = (slot & 3) < own_ref[:, :heads]
    keep = jnp.exp(jnp.where(live, decay, 0.0))
    write = jnp.where(live, 1.0 / (1.0 + jnp.exp(-betas)), 0.0)
    gates[:SUBS, :heads] = jnp.where(slot < NEW, keep, write)
    turned = gates[...].T
    fetches[0].wait()
    for h in range(heads):
        own = slice(h * SUBS, (h + 1) * SUBS)
        preds[own, :] = jnp.dot(
            unit[own, :], memory_ref[h], precision=lax.Precision.HIGHEST, preferred_element_type=F32
        )

    def rows(ref, j):
        return ref[pl.ds(j, heads, stride=SUBS), :]

    queries = [rows(unit, t) for t in range(NEW)]
    keys = [rows(unit, NEW + t) for t in range(NEW)]
    keeps = [turned[:heads, t : t + 1] for t in range(NEW)]
    writes = [turned[:heads, NEW + t : NEW + t + 1] for t in range(NEW)]

    def inner(a, b):
        return jnp.sum(a * b, axis=1, keepdims=True)

    updates, outs = [], []
    passed = []
    total = jnp.ones((heads, 1), F32)
    for t in range(NEW):
        total = total * keeps[t]
        passed = [p * keeps[t] for p in passed]
        said = total * rows(preds, NEW + t)
        for i in range(t):
            said = said + (passed[i] * inner(keys[i], keys[t])) * updates[i]
        updates.append(writes[t] * (rows(vals, t) - said))
        passed.append(jnp.ones((heads, 1), F32))
        out = total * rows(preds, t)
        for i in range(t + 1):
            out = out + (passed[i] * inner(keys[i], queries[t])) * updates[i]
        outs.append(out)
    for i in range(NEW):
        late[pl.ds(i, heads, stride=SUBS), :] = jnp.zeros((heads, DV), F32)
        late[pl.ds(NEW + i, heads, stride=SUBS), :] = passed[i] * updates[i]
    for h in range(heads):
        own = slice(h * SUBS, (h + 1) * SUBS)
        added = lax.dot_general(
            unit[own, :],
            late[own, :],
            (((0,), (0,)), ((), ())),
            precision=lax.Precision.HIGHEST,
            preferred_element_type=F32,
        )
        fresh_ref[h] = memory_ref[h] * total[h : h + 1, :] + added
    store = pltpu.make_async_copy(fresh_ref, memory_out, out_sem)
    store.start()
    for t, out in enumerate(outs):
        out = out * lax.rsqrt(jnp.mean(out * out, axis=1, keepdims=True) + epsilon)
        gate = rows(vals, NEW + t)
        silu = gate * (1.0 / (1.0 + jnp.exp(-gate)))
        copies[t * heads : (t + 1) * heads, :] = out * gain_ref[...] * silu
    mixed = copies[...].astype(BF16)
    for d in range(mixed_out.shape[0]):
        mixed_out[d] = mixed
    store.wait()


def project_kernel(place_ref, mixed_ref, w_ref, out_ref):
    heads = w_ref.shape[0] // DV
    total = mixed_ref.shape[0]
    packed = out_ref.shape[0]
    place = place_ref[...]
    head_of = iota((1, total), 1) & (heads - 1)
    row = iota((packed, total), 0)
    mixed = mixed_ref[...]
    rows = []
    for h in range(heads):
        pick = jnp.where(row == jnp.where(head_of == h, place, -1), 1.0, 0.0).astype(BF16)
        rows.append(dot(pick, mixed).astype(BF16))
    sum_ = None
    for h in range(heads):
        term = dot(rows[h], w_ref[h * DV : (h + 1) * DV, :])
        sum_ = term if sum_ is None else sum_ + term
    out_ref[...] = sum_


def picker(lengths_ref, packed, total_rows):
    col = iota((1, total_rows), 1)
    place = places(lengths_ref, lax.shift_right_logical(col, 2), col & 3)
    return jnp.where(iota((packed, total_rows), 0) == place, 1.0, 0.0).astype(BF16)


def blocks_of(granules, tiles, receiver):
    first = (receiver * granules) // tiles
    last = (receiver * granules + granules - 1) // tiles
    return first, last


def up_kernel(granules, extra, inputs, *refs):
    *terms, base_ref, gain_ref, wg_ref, wu_ref = refs[:inputs]
    hidden_out, *outs = refs[inputs:-1]
    out_ref = refs[-1]
    packed = hidden_out.shape[0]
    hidden = base_ref[...]
    for term in terms:
        hidden = hidden + term[...]
    hidden = hidden.astype(BF16)
    hidden_out[...] = hidden
    hidden_f = hidden.astype(F32)
    scaled = (hidden_f * gain_ref[...]).astype(BF16)
    tiles = wg_ref.shape[1] // LANES
    row_blocks = packed // SUBS
    squares = jnp.sum(hidden_f * hidden_f, axis=1, keepdims=True)
    squares = jnp.broadcast_to(squares, (packed, LANES))
    high = squares.astype(BF16).astype(F32)
    halves = jnp.where(iota(squares.shape, 1) < LANES // 2, high, squares - high).astype(BF16)
    step = 4
    for start in range(0, tiles, step):
        stop = min(start + step, tiles)
        span = slice(start * LANES, stop * LANES)
        gate = dot(scaled, wg_ref[:, span])
        up = dot(scaled, wu_ref[:, span])
        for t in range(start, stop):
            lanes = slice((t - start) * LANES, (t - start + 1) * LANES)
            for b in range(row_blocks):
                rows = slice(b * SUBS, (b + 1) * SUBS)
                pair = jnp.concatenate([gate[rows, lanes], up[rows, lanes]], axis=0).astype(BF16)
                d, i = divmod(b * tiles + t, granules)
                out_ref[d, i * 16 : i * 16 + 16, :] = pair
    for d in range(out_ref.shape[0]):
        first, _ = blocks_of(granules, tiles, d)
        for e in range(extra):
            b = min(first + e, row_blocks - 1)
            at = granules * 16 + e * SUBS
            out_ref[d, at : at + SUBS, :] = halves[b * SUBS : (b + 1) * SUBS, :]
    deal(out_ref, outs)


def active_kernel(granules, extra, tiles, *refs):
    *got, out_ref = refs
    scales = []
    for e in range(extra):
        at = granules * 16 + e * SUBS
        squares = block_sum(got, slice(at, at + SUBS), slice(None))
        squares = squares[:, :1] + squares[:, LANES // 2 : LANES // 2 + 1]
        scales.append(lax.rsqrt(squares / D + epsilon))
    place = lax.axis_index("kv") if extra > 1 else 0
    for i in range(granules):
        pair = block_sum(got, slice(i * 16, i * 16 + 16), slice(None))
        scale = scales[0]
        if extra > 1:
            ahead = lax.div(place * granules + i, tiles) - lax.div(place * granules, tiles)
            for e in range(1, extra):
                scale = jnp.where(ahead >= e, scales[e], scale)
        gate, up = pair[:SUBS] * scale, pair[SUBS:] * scale
        active = (gate * (1.0 / (1.0 + jnp.exp(-gate))) * up).astype(BF16)
        for d in range(out_ref.shape[0]):
            out_ref[d, i * SUBS : (i + 1) * SUBS, :] = active


def down_kernel(got_ref, w_ref, out_ref):
    packed = out_ref.shape[0]
    tiles = w_ref.shape[0] // LANES
    sum_ = None
    for t in range(tiles):
        parts = [
            got_ref[(b * tiles + t) * SUBS : (b * tiles + t + 1) * SUBS, :].astype(F32)
            for b in range(packed // SUBS)
        ]
        term = dot(jnp.concatenate(parts, axis=0).astype(BF16), w_ref[t * LANES : (t + 1) * LANES, :])
        sum_ = term if sum_ is None else sum_ + term
    out_ref[...] = sum_


def last_kernel(*refs):
    *terms, hidden_ref, pick_ref, out_ref = refs
    result = terms[0][...]
    for term in terms[1:]:
        result = result + term[...]
    result = (hidden_ref[...].astype(F32) + result).astype(BF16)
    out_ref[...] = lax.dot_general(
        pick_ref[...], result, (((0,), (0,)), ((), ())), preferred_element_type=F32
    ).astype(BF16)


def exchange(blocks):
    return lax.all_to_all(blocks, "kv", 0, 0)


def over_tp(terms):
    if lax.axis_size("tp") == 2:
        return [terms, lax.ppermute(terms, "tp", [(0, 1), (1, 0)])]
    return [lax.psum(terms, "tp")]


def per_device(
    tokens,
    lengths,
    memory,
    norm_gain,
    w_query,
    w_key,
    w_value,
    w_outgate,
    w_alpha,
    w_beta,
    decay_log,
    decay_bias,
    head_gain,
    w_output,
    mlp_gain,
    w_gate,
    w_up,
    w_down,
):
    total_rows, own_width = tokens.shape
    kv = lax.axis_size("kv")
    seq_dev, heads = memory.shape[:2]
    assert seq_dev == 1
    width = heads * DK
    sequences = lengths.shape[0]
    units = w_gate.shape[1]
    packed = -(-(sequences * 7 // 4) // SUBS) * SUBS
    tiles = units // LANES
    granules = -(-(tiles * packed // SUBS) // kv)
    last_receiver = (tiles * packed // SUBS - 1) // granules
    extra = max(b - a + 1 for a, b in (blocks_of(granules, tiles, d) for d in range(last_receiver + 1)))
    columns = 2 * width + LANES

    operands = [lengths, tokens, norm_gain[None], w_alpha.T, w_beta.T, w_query, w_key, w_value, w_outgate]
    *sent, base, pick, place, own = call(
        functools.partial(front_kernel, heads),
        [
            *dealt((SUBS, columns), kv),
            shape((packed, own_width), F32),
            shape((packed, total_rows), BF16),
            shape((1, kv * NEW * heads), jnp.int32),
            shape((SUBS, LANES), jnp.int32),
        ],
        operands,
        [HBM] * len(operands),
        16,
        4 * total_rows * own_width * 4 * width,
        "front",
        [pltpu.SMEM(lengths.shape, jnp.int32), *(room(x) for x in operands[1:]), pltpu.SemaphoreType.DMA((len(operands),)), pltpu.VMEM((kv, SUBS, columns), BF16)],
    )
    got = reduce_scatter(sent, "fold_rows", slice(None), slice(2 * width, columns), 0, NEW)
    new_memory, sent = call(
        recur_kernel,
        [shape((heads, DK, DV), F32), shape((kv, NEW * heads, DV), BF16)],
        [own, *got, memory[0], decay_log[None], decay_bias[None], head_gain[None]],
        [VMEM] * (1 + len(got)) + [HBM] * 4,
        16,
        4 << 30,
        "recur",
        [
            pltpu.VMEM((LANES, LANES), F32),
            *[pltpu.VMEM((heads * SUBS, DV), F32)] * 4,
            pltpu.VMEM((NEW * heads, DV), F32),
            pltpu.VMEM((heads, DK, DV), F32),
            pltpu.VMEM((heads, DK, DV), F32),
            pltpu.VMEM((1, heads), F32),
            pltpu.VMEM((1, heads), F32),
            pltpu.VMEM((1, DV), F32),
            pltpu.SemaphoreType.DMA((4,)),
            pltpu.SemaphoreType.DMA,
        ],
        [HBM, VMEM],
    )
    got = exchange(sent).reshape(kv * NEW * heads, DV)
    (attn,) = call(
        project_kernel,
        [shape((packed, own_width), F32)],
        [place, got, w_output],
        [VMEM] * 3,
        8,
        32 << 20,
        "project",
    )
    terms = over_tp(attn)
    block = (granules * 16 + extra * SUBS, LANES)
    hidden, *sent = call(
        functools.partial(up_kernel, granules, extra, len(terms) + 4),
        [shape((packed, own_width), BF16), *dealt(block, kv)],
        [*terms, base, mlp_gain[None], w_gate, w_up],
        [VMEM] * (len(terms) + 4),
        16,
        4 * packed * own_width * units,
        "up",
        [pltpu.VMEM((kv, *block), BF16)],
    )
    got = reduce_scatter(sent, "fold_units", slice(granules * 16, None), slice(None), 1, LANES // 2)
    (sent,) = call(
        functools.partial(active_kernel, granules, extra, tiles),
        [shape((kv, granules * SUBS, LANES), BF16)],
        got,
        [VMEM] * len(got),
        8,
        1 << 20,
        "active",
    )
    got = exchange(sent).reshape(kv * granules * SUBS, LANES)
    (feed,) = call(
        down_kernel,
        [shape((packed, own_width), F32)],
        [got, w_down],
        [VMEM] * 2,
        16,
        2 * packed * own_width * units,
        "down",
    )
    terms = over_tp(feed)
    (layer_out,) = call(
        last_kernel,
        [shape((total_rows, own_width), BF16)],
        [*terms, hidden, pick],
        [VMEM] * (len(terms) + 2),
        8,
        1 << 20,
        "last",
    )
    return (layer_out, new_memory[None])


def solution(mesh):
    placed = (
        P(None, "kv"),
        P(),
        P("kv", "tp", None, None),
        P("kv"),
        P("kv", "tp"),
        P("kv", "tp"),
        P("kv", "tp"),
        P("kv", "tp"),
        P("kv", None),
        P("kv", None),
        P("tp"),
        P("tp"),
        P(),
        P("tp", "kv"),
        P("kv"),
        P("kv", "tp"),
        P("kv", "tp"),
        P("tp", "kv"),
    )
    return jax.shard_map(
        per_device,
        mesh=mesh,
        in_specs=placed,
        out_specs=(P(None, "kv"), P("kv", "tp", None, None)),
        check_vma=False,
    )
```

```python
import functools

import jax
import jax.numpy as jnp
from jax import lax
from jax.experimental import pallas as pl
from jax.experimental.pallas import tpu as pltpu
from jax.sharding import PartitionSpec as P

D = 4096
DK = 128
DV = 128
NEW = 4
LANES = 128
PLANE = 4
SUBS = 8

epsilon = 1e-06


F32 = jnp.float32
BF16 = jnp.bfloat16
VMEM = pl.BlockSpec(memory_space=pltpu.VMEM)
HBM = pl.BlockSpec(memory_space=pltpu.HBM)


def call(body, outs, ins, specs, limit, flops, name, scratch=(), out_specs=None):
    moved = sum(x.size * x.dtype.itemsize for x in (*outs, *ins))
    ins = [pltpu.with_memory_space_constraint(x, pltpu.HBM) if s is HBM else x for x, s in zip(ins, specs)]
    return pl.pallas_call(
        body,
        out_shape=outs,
        in_specs=specs,
        out_specs=out_specs or [VMEM] * len(outs),
        scratch_shapes=list(scratch),
        compiler_params=pltpu.CompilerParams(vmem_limit_bytes=limit << 20),
        cost_estimate=pl.CostEstimate(flops=flops, bytes_accessed=moved, transcendentals=0),
        name=name,
    )(*ins)


def room(x):
    return pltpu.VMEM(x.shape, x.dtype)


def shape(dims, dtype):
    return jax.ShapeDtypeStruct(dims, dtype)


def iota(dims, axis):
    return lax.broadcasted_iota(jnp.int32, dims, axis)


def dot(a, b):
    return jnp.dot(a, b, preferred_element_type=F32)


def dot_nt(a, b):
    return lax.dot_general(a, b, (((1,), (1,)), ((), ())), preferred_element_type=F32)


def places(lengths_ref, sequence_of, slot_of):
    place = jnp.full(sequence_of.shape, -1, jnp.int32)
    start = 0
    for s in range(lengths_ref.shape[0]):
        held = lengths_ref[s]
        mine = (sequence_of == s) & (slot_of < held)
        place = jnp.where(mine, slot_of + start, place)
        start = start + held
    return place


def log2(n):
    assert n & (n - 1) == 0
    return n.bit_length() - 1


def front_kernel(heads, *refs):
    count = 9
    sources, refs = refs[:count], refs[count:]
    *outs, base_ref, pick_ref, place_ref, own_ref = refs[: -count - 2]
    *held, sems, out_ref = refs[-count - 2 :]
    copies = [pltpu.make_async_copy(a, b, sems.at[i]) for i, (a, b) in enumerate(zip(sources, held))]
    for copy in copies:
        copy.start()
    lengths_ref, tokens_ref, gain_ref, wa_ref, wb_ref, wq_ref, wk_ref, wv_ref, wg_ref = held
    total_rows = tokens_ref.shape[0]
    width = wq_ref.shape[1]
    all_heads = wa_ref.shape[0]
    packed = pick_ref.shape[0]
    copies[0].wait()
    own_ref[...] = jnp.full(own_ref.shape, lengths_ref[lax.axis_index("kv")], jnp.int32)
    col = iota(place_ref.shape, 1)
    place_ref[...] = places(
        lengths_ref,
        lax.shift_right_logical(col, log2(NEW * heads)),
        lax.shift_right_logical(col, log2(heads)) & 3,
    )
    pick = picker(lengths_ref, packed, total_rows)
    pick_ref[...] = pick
    dims = (2 * total_rows, total_rows)
    row, col = iota(dims, 0), iota(dims, 1)
    target = lax.shift_left(lax.shift_right_logical(row, 3), 2) + (row & 3)
    hit = target == col
    upper = (row & 7) < NEW
    zero, one = jnp.zeros(dims, F32), jnp.ones(dims, F32)
    place_a = jnp.where(hit & upper, one, zero).astype(BF16)
    place_b = jnp.where(hit & ~upper, one, zero).astype(BF16)
    fill = jnp.zeros((LANES - 2 * all_heads, wa_ref.shape[1]), BF16)
    for copy in copies[1:5]:
        copy.wait()
    tokens = tokens_ref[...]
    base_ref[...] = dot(pick, tokens)
    scaled = (tokens.astype(F32) * gain_ref[...]).astype(BF16)
    left = dot(place_a, scaled).astype(BF16)
    right = dot(place_b, scaled).astype(BF16)
    both = dot(place_a + place_b, tokens)
    squares = jnp.sum(both * both, axis=1, keepdims=True)
    small = dot_nt(left + right, jnp.concatenate([wa_ref[...], wb_ref[...], fill], axis=0))
    lane = iota(small.shape, 1)
    small = jnp.where(lane == 2 * all_heads, jnp.broadcast_to(squares, small.shape), small)
    high = small.astype(BF16).astype(F32)
    first = (iota(small.shape, 0) & 7) < NEW

    def put(columns, values):
        out_ref[:, :, columns] = values.reshape(-1, SUBS, values.shape[1]).astype(BF16)

    put(slice(2 * width, 2 * width + LANES), jnp.where(first, high, small - high))
    copies[5].wait()
    copies[6].wait()
    put(slice(0, width), dot(left, wq_ref[...]) + dot(right, wk_ref[...]))
    copies[7].wait()
    copies[8].wait()
    put(slice(width, 2 * width), dot(left, wv_ref[...]) + dot(right, wg_ref[...]))
    deal(out_ref, outs)


def deal(blocks_ref, outs):
    if len(outs) == 1:
        outs[0][...] = blocks_ref[...]
        return
    plane = lax.axis_index("kv") & (PLANE - 1)
    for d, out in enumerate(outs):
        for z in range(out.shape[0]):
            out[z] = blocks_ref[z * PLANE + (plane ^ d)]


def fold_kernel(rows, columns, axis, half, *refs):
    parts, outs = refs[:PLANE], refs[PLANE:]
    high = lax.shift_right_logical(lax.axis_index("kv"), log2(PLANE))
    for e, out in enumerate(outs):
        total = parts[0][high ^ e].astype(F32)
        for part in parts[1:]:
            total = total + part[high ^ e].astype(F32)
        out[...] = total.astype(out.dtype)
        value = total[rows, columns]
        value = value + pltpu.roll(value, half, axis)
        top = value.astype(BF16).astype(F32)
        value = jnp.where(iota(value.shape, axis) < half, top, value - top)
        out[rows, columns] = value.astype(out.dtype)


def partners(values, shift):
    count = lax.axis_size("kv")
    moved = []
    for d in reversed(range(1, len(values))):
        moved.append(lax.ppermute(values[d], "kv", [(i, i ^ (d << shift)) for i in range(count)]))
    return [values[0], *moved]


def staged():
    return lax.axis_size("kv") == PLANE * PLANE


def dealt(dims, kv):
    if staged():
        return [shape((PLANE, *dims), BF16)] * PLANE
    return [shape((kv, *dims), BF16)]


def reduce_scatter(outs, name, *halves, beside=None):
    if not staged():
        return [exchange(outs[0])], beside
    dims = outs[0].shape[1:]
    parts = partners(outs, 0)
    if beside is not None:
        parts, beside = lax.optimization_barrier((parts, beside))
    sums = call(
        functools.partial(fold_kernel, *halves),
        [shape(dims, F32 if e == 0 else BF16) for e in range(PLANE)],
        parts,
        [VMEM] * PLANE,
        8,
        1 << 20,
        name,
    )
    return [x[None] for x in partners(sums, log2(PLANE))], beside


def block_sum(refs, rows, columns):
    total = None
    for ref in refs:
        for i in range(ref.shape[0]):
            term = ref[i, rows, columns].astype(F32)
            total = term if total is None else total + term
    return total


def row_sum(refs, start, columns):
    return block_sum(refs, slice(None), slice(start, start + columns))


def recur_kernel(*refs):
    own_ref, *got_ref = refs[:-17]
    sources, (mixed_out, unit, late, left_ref) = refs[-17:-13], refs[-13:-9]
    gates, vals, preds, copies, *held, sems = refs[-9:]
    memory_ref, log_ref, bias_ref, gain_ref = held
    heads = memory_ref.shape[0]
    fetches = [pltpu.make_async_copy(a, b, sems.at[i]) for i, (a, b) in enumerate(zip(sources, held))]
    for fetch in fetches[1:] + fetches[:1]:
        fetch.start()
    width = heads * DK
    all_heads = heads * lax.axis_size("tp")
    tp_place = lax.axis_index("tp")
    small = row_sum(got_ref, 2 * width, LANES)
    small = small + pltpu.roll(small, NEW, 0)
    rstd = lax.rsqrt(small[:, 2 * all_heads : 2 * all_heads + 1] / D + epsilon)
    gates[...] = jnp.zeros(gates.shape, F32)
    factor = jnp.where(iota((SUBS, 1), 0) < NEW, DK ** (-0.5), 1.0)
    for h in range(heads):
        block = (row_sum(got_ref, h * DK, DK) * rstd).astype(BF16).astype(F32)
        norm = lax.rsqrt(jnp.sum(block * block, axis=1, keepdims=True) + epsilon)
        unit[h * SUBS : (h + 1) * SUBS, :] = block * norm * factor
        vals[h * SUBS : (h + 1) * SUBS, :] = (
            (row_sum(got_ref, width + h * DV, DV) * rstd).astype(BF16).astype(F32)
        )
    for fetch in fetches[1:]:
        fetch.wait()
    small = small * rstd
    alphas = pltpu.roll(small, LANES - tp_place * heads, 1)[:, :heads]
    betas = pltpu.roll(small, LANES - all_heads - tp_place * heads, 1)[:, :heads]
    x = alphas + bias_ref[...]
    soft = jnp.maximum(x, 0.0) + jnp.log1p(jnp.exp(-jnp.abs(x)))
    decay = -jnp.exp(log_ref[...]) * soft
    slot = iota(decay.shape, 0)
    live = (slot & 3) < own_ref[:, :heads]
    keep = jnp.exp(jnp.where(live, decay, 0.0))
    write = jnp.where(live, 1.0 / (1.0 + jnp.exp(-betas)), 0.0)
    gates[:SUBS, :heads] = jnp.where(slot < NEW, keep, write)
    turned = gates[...].T
    fetches[0].wait()
    for h in range(heads):
        own = slice(h * SUBS, (h + 1) * SUBS)
        preds[own, :] = jnp.dot(
            unit[own, :], memory_ref[h], precision=lax.Precision.HIGHEST, preferred_element_type=F32
        )

    def rows(ref, j):
        return ref[pl.ds(j, heads, stride=SUBS), :]

    queries = [rows(unit, t) for t in range(NEW)]
    keys = [rows(unit, NEW + t) for t in range(NEW)]
    keeps = [turned[:heads, t : t + 1] for t in range(NEW)]
    writes = [turned[:heads, NEW + t : NEW + t + 1] for t in range(NEW)]

    def inner(a, b):
        return jnp.sum(a * b, axis=1, keepdims=True)

    updates, outs = [], []
    passed = []
    total = jnp.ones((heads, 1), F32)
    for t in range(NEW):
        total = total * keeps[t]
        passed = [p * keeps[t] for p in passed]
        said = total * rows(preds, NEW + t)
        for i in range(t):
            said = said + (passed[i] * inner(keys[i], keys[t])) * updates[i]
        updates.append(writes[t] * (rows(vals, t) - said))
        passed.append(jnp.ones((heads, 1), F32))
        out = total * rows(preds, t)
        for i in range(t + 1):
            out = out + (passed[i] * inner(keys[i], queries[t])) * updates[i]
        outs.append(out)
    for i in range(NEW):
        late[pl.ds(i, heads, stride=SUBS), :] = jnp.zeros((heads, DV), F32)
        late[pl.ds(NEW + i, heads, stride=SUBS), :] = passed[i] * updates[i]
    left_ref[...] = jnp.broadcast_to(total, left_ref.shape)
    for t, out in enumerate(outs):
        out = out * lax.rsqrt(jnp.mean(out * out, axis=1, keepdims=True) + epsilon)
        gate = rows(vals, NEW + t)
        silu = gate * (1.0 / (1.0 + jnp.exp(-gate)))
        copies[t * heads : (t + 1) * heads, :] = out * gain_ref[...] * silu
    mixed = copies[...].astype(BF16)
    for d in range(mixed_out.shape[0]):
        mixed_out[d] = mixed


def advance_kernel(memory_ref, unit_ref, late_ref, left_ref, out_ref, fresh_ref, sems):
    stores = []
    for h in range(memory_ref.shape[0]):
        own = slice(h * SUBS, (h + 1) * SUBS)
        added = lax.dot_general(
            unit_ref[own, :],
            late_ref[own, :],
            (((0,), (0,)), ((), ())),
            precision=lax.Precision.HIGHEST,
            preferred_element_type=F32,
        )
        fresh_ref[h] = memory_ref[h] * left_ref[h : h + 1, :] + added
        stores.append(pltpu.make_async_copy(fresh_ref.at[h], out_ref.at[h], sems.at[h]))
        stores[-1].start()
    for store in stores:
        store.wait()


def project_kernel(place_ref, mixed_ref, w_ref, out_ref):
    heads = w_ref.shape[0] // DV
    total = mixed_ref.shape[0]
    packed = out_ref.shape[0]
    place = place_ref[...]
    head_of = iota((1, total), 1) & (heads - 1)
    row = iota((packed, total), 0)
    mixed = mixed_ref[...]
    rows = []
    for h in range(heads):
        pick = jnp.where(row == jnp.where(head_of == h, place, -1), 1.0, 0.0).astype(BF16)
        rows.append(dot(pick, mixed).astype(BF16))
    sum_ = None
    for h in range(heads):
        term = dot(rows[h], w_ref[h * DV : (h + 1) * DV, :])
        sum_ = term if sum_ is None else sum_ + term
    out_ref[...] = sum_


def picker(lengths_ref, packed, total_rows):
    col = iota((1, total_rows), 1)
    place = places(lengths_ref, lax.shift_right_logical(col, 2), col & 3)
    return jnp.where(iota((packed, total_rows), 0) == place, 1.0, 0.0).astype(BF16)


class Packing:
    def __init__(self, live, tiles, receivers):
        self.tiles = tiles
        self.shared = 0 < live % SUBS <= SUBS // 2 and tiles % 2 == 0
        self.whole = live // SUBS if self.shared else -(-live // SUBS)
        self.count = self.whole * tiles + (tiles // 2 if self.shared else 0)
        self.each = -(-self.count // receivers)

    def spot(self, block, tile):
        at = block * self.tiles + (tile if block < self.whole else tile // 2)
        return divmod(at, self.each)


def up_kernel(packing, inputs, *refs):
    *terms, base_ref, gain_ref, wg_ref, wu_ref = refs[:inputs]
    hidden_out, *outs = refs[inputs:-1]
    out_ref = refs[-1]
    packed = hidden_out.shape[0]
    hidden = base_ref[...]
    for term in terms:
        hidden = hidden + term[...]
    hidden = hidden.astype(BF16)
    hidden_out[...] = hidden
    hidden_f = hidden.astype(F32)
    scaled = (hidden_f * gain_ref[...]).astype(BF16)
    tiles = packing.tiles
    squares = jnp.broadcast_to(jnp.sum(hidden_f * hidden_f, axis=1, keepdims=True), (packed, LANES))
    own_lane = iota(squares.shape, 0) == iota(squares.shape, 1)
    squares = jnp.sum(jnp.where(own_lane, squares, 0.0), axis=0, keepdims=True)
    squares = jnp.broadcast_to(squares, (SUBS, LANES))
    high = squares.astype(BF16).astype(F32)
    halves = jnp.where(iota(squares.shape, 0) < NEW, high, squares - high).astype(BF16)
    step = 4
    for start in range(0, tiles, step):
        stop = min(start + step, tiles)
        span = slice(start * LANES, stop * LANES)
        gate = dot(scaled, wg_ref[:, span])
        up = dot(scaled, wu_ref[:, span])
        for t in range(start, stop):
            lanes = slice((t - start) * LANES, (t - start + 1) * LANES)
            for b in range(packed // SUBS):
                rows = slice(b * SUBS, (b + 1) * SUBS)
                one, two = gate[rows, lanes], up[rows, lanes]
                if b == packing.whole:
                    if t % 2 == 0:
                        held = one, two
                        continue
                    one = held[0] + pltpu.roll(one, SUBS // 2, 0)
                    two = held[1] + pltpu.roll(two, SUBS // 2, 0)
                d, i = packing.spot(b, t)
                out_ref[d, i * 16 : i * 16 + 16, :] = jnp.concatenate([one, two], axis=0).astype(BF16)
    for at in range(packing.count, out_ref.shape[0] * packing.each):
        d, i = divmod(at, packing.each)
        out_ref[d, i * 16 : i * 16 + 16, :] = jnp.zeros((16, LANES), BF16)
    for d in range(out_ref.shape[0]):
        out_ref[d, packing.each * 16 :, :] = halves
    deal(out_ref, outs)


def active_kernel(packing, *refs):
    *got, out_ref = refs
    end = packing.each * 16
    squares = block_sum(got, slice(end, end + SUBS), slice(None))
    squares = squares + pltpu.roll(squares, SUBS // 2, 0)
    rstd = lax.rsqrt(squares / D + epsilon)
    row, lane = iota(rstd.shape, 0), iota(rstd.shape, 1)
    first = lax.axis_index("kv") * packing.each
    for i in range(packing.each):
        block = lax.div(first + i, packing.tiles)
        row_of = block * SUBS + row
        if packing.shared:
            row_of = jnp.where(block >= packing.whole, packing.whole * SUBS + (row & (SUBS // 2 - 1)), row_of)
        scale = jnp.sum(jnp.where(lane == row_of, rstd, 0.0), axis=1, keepdims=True)
        pair = block_sum(got, slice(i * 16, i * 16 + 16), slice(None))
        gate, up = pair[:SUBS] * scale, pair[SUBS:] * scale
        active = (gate * (1.0 / (1.0 + jnp.exp(-gate))) * up).astype(BF16)
        for d in range(out_ref.shape[0]):
            out_ref[d, i * SUBS : (i + 1) * SUBS, :] = active


def down_kernel(packing, got_ref, w_ref, out_ref):
    packed = out_ref.shape[0]
    tiles = w_ref.shape[0] // LANES
    sum_ = None
    for t in range(tiles):
        parts = []
        for b in range(packed // SUBS):
            d, i = packing.spot(b, t)
            part = got_ref[d, i * SUBS : (i + 1) * SUBS, :].astype(F32)
            parts.append(pltpu.roll(part, SUBS // 2, 0) if b == packing.whole and t % 2 else part)
        term = dot(jnp.concatenate(parts, axis=0).astype(BF16), w_ref[t * LANES : (t + 1) * LANES, :])
        sum_ = term if sum_ is None else sum_ + term
    out_ref[...] = sum_


def last_kernel(*refs):
    *terms, hidden_ref, pick_ref, out_ref = refs
    result = terms[0][...]
    for term in terms[1:]:
        result = result + term[...]
    result = (hidden_ref[...].astype(F32) + result).astype(BF16)
    out_ref[...] = lax.dot_general(
        pick_ref[...], result, (((0,), (0,)), ((), ())), preferred_element_type=F32
    ).astype(BF16)


def exchange(blocks):
    return lax.all_to_all(blocks, "kv", 0, 0)


def over_tp(terms):
    if lax.axis_size("tp") == 2:
        return [terms, lax.ppermute(terms, "tp", [(0, 1), (1, 0)])]
    return [lax.psum(terms, "tp")]


def per_device(
    tokens,
    lengths,
    memory,
    norm_gain,
    w_query,
    w_key,
    w_value,
    w_outgate,
    w_alpha,
    w_beta,
    decay_log,
    decay_bias,
    head_gain,
    w_output,
    mlp_gain,
    w_gate,
    w_up,
    w_down,
):
    total_rows, own_width = tokens.shape
    kv = lax.axis_size("kv")
    seq_dev, heads = memory.shape[:2]
    assert seq_dev == 1
    width = heads * DK
    sequences = lengths.shape[0]
    units = w_gate.shape[1]
    live = sequences * 7 // 4
    packed = -(-live // SUBS) * SUBS
    assert packed <= LANES
    packing = Packing(live, units // LANES, kv)
    columns = 2 * width + LANES

    operands = [lengths, tokens, norm_gain[None], w_alpha.T, w_beta.T, w_query, w_key, w_value, w_outgate]
    *sent, base, pick, place, own = call(
        functools.partial(front_kernel, heads),
        [
            *dealt((SUBS, columns), kv),
            shape((packed, own_width), F32),
            shape((packed, total_rows), BF16),
            shape((1, kv * NEW * heads), jnp.int32),
            shape((SUBS, LANES), jnp.int32),
        ],
        operands,
        [HBM] * len(operands),
        16,
        4 * total_rows * own_width * 4 * width,
        "front",
        [pltpu.SMEM(lengths.shape, jnp.int32), *(room(x) for x in operands[1:]), pltpu.SemaphoreType.DMA((len(operands),)), pltpu.VMEM((kv, SUBS, columns), BF16)],
    )
    got, _ = reduce_scatter(sent, "fold_rows", slice(None), slice(2 * width, columns), 0, NEW)
    sent, unit, late, left = call(
        recur_kernel,
        [
            shape((kv, NEW * heads, DV), BF16),
            shape((heads * SUBS, DK), F32),
            shape((heads * SUBS, DV), F32),
            shape((heads, DV), F32),
        ],
        [own, *got, memory[0], decay_log[None], decay_bias[None], head_gain[None]],
        [VMEM] * (1 + len(got)) + [HBM] * 4,
        16,
        4 << 30,
        "recur",
        [
            pltpu.VMEM((LANES, LANES), F32),
            pltpu.VMEM((heads * SUBS, DV), F32),
            pltpu.VMEM((heads * SUBS, DV), F32),
            pltpu.VMEM((NEW * heads, DV), F32),
            pltpu.VMEM((heads, DK, DV), F32),
            pltpu.VMEM((1, heads), F32),
            pltpu.VMEM((1, heads), F32),
            pltpu.VMEM((1, DV), F32),
            pltpu.SemaphoreType.DMA((4,)),
        ],
    )
    (new_memory,) = call(
        advance_kernel,
        [shape((heads, DK, DV), F32)],
        [memory[0], unit, late, left],
        [VMEM] * 4,
        8,
        1 << 30,
        "advance",
        [pltpu.VMEM((heads, DK, DV), F32), pltpu.SemaphoreType.DMA((heads,))],
        [HBM],
    )
    got = exchange(sent).reshape(kv * NEW * heads, DV)
    (attn,) = call(
        project_kernel,
        [shape((packed, own_width), F32)],
        [place, got, w_output],
        [VMEM] * 3,
        8,
        32 << 20,
        "project",
    )
    terms = over_tp(attn)
    block = (packing.each * 16 + SUBS, LANES)
    hidden, *sent = call(
        functools.partial(up_kernel, packing, len(terms) + 4),
        [shape((packed, own_width), BF16), *dealt(block, kv)],
        [*terms, base, mlp_gain[None], w_gate, w_up],
        [VMEM] * (len(terms) + 4),
        16,
        4 * packed * own_width * units,
        "up",
        [pltpu.VMEM((kv, *block), BF16)],
    )
    got, new_memory = reduce_scatter(
        sent, "fold_units", slice(packing.each * 16, None), slice(None), 0, NEW, beside=new_memory
    )
    (sent,) = call(
        functools.partial(active_kernel, packing),
        [shape((kv, packing.each * SUBS, LANES), BF16)],
        got,
        [VMEM] * len(got),
        8,
        1 << 20,
        "active",
    )
    got = exchange(sent)
    (feed,) = call(
        functools.partial(down_kernel, packing),
        [shape((packed, own_width), F32)],
        [got, w_down],
        [VMEM] * 2,
        16,
        2 * packed * own_width * units,
        "down",
    )
    terms = over_tp(feed)
    (layer_out,) = call(
        last_kernel,
        [shape((total_rows, own_width), BF16)],
        [*terms, hidden, pick],
        [VMEM] * (len(terms) + 2),
        8,
        1 << 20,
        "last",
    )
    return (layer_out, new_memory[None])


def solution(mesh):
    placed = (
        P(None, "kv"),
        P(),
        P("kv", "tp", None, None),
        P("kv"),
        P("kv", "tp"),
        P("kv", "tp"),
        P("kv", "tp"),
        P("kv", "tp"),
        P("kv", None),
        P("kv", None),
        P("tp"),
        P("tp"),
        P(),
        P("tp", "kv"),
        P("kv"),
        P("kv", "tp"),
        P("kv", "tp"),
        P("tp", "kv"),
    )
    return jax.shard_map(
        per_device,
        mesh=mesh,
        in_specs=placed,
        out_specs=(P(None, "kv"), P("kv", "tp", None, None)),
        check_vma=False,
    )
```

```python
import functools

import jax
import jax.numpy as jnp
from jax import lax
from jax.experimental import pallas as pl
from jax.experimental.pallas import tpu as pltpu
from jax.sharding import PartitionSpec as P

D = 4096
DK = 128
DV = 128
NEW = 4
LANES = 128
PLANE = 4
SUBS = 8

epsilon = 1e-06


F32 = jnp.float32
BF16 = jnp.bfloat16
VMEM = pl.BlockSpec(memory_space=pltpu.VMEM)
HBM = pl.BlockSpec(memory_space=pltpu.HBM)


def call(body, outs, ins, specs, limit, flops, name, scratch=(), out_specs=None):
    moved = sum(x.size * x.dtype.itemsize for x in (*outs, *ins))
    ins = [pltpu.with_memory_space_constraint(x, pltpu.HBM) if s is HBM else x for x, s in zip(ins, specs)]
    return pl.pallas_call(
        body,
        out_shape=outs,
        in_specs=specs,
        out_specs=out_specs or [VMEM] * len(outs),
        scratch_shapes=list(scratch),
        compiler_params=pltpu.CompilerParams(vmem_limit_bytes=limit << 20),
        cost_estimate=pl.CostEstimate(flops=flops, bytes_accessed=moved, transcendentals=0),
        name=name,
    )(*ins)


def room(x):
    return pltpu.VMEM(x.shape, x.dtype)


def shape(dims, dtype):
    return jax.ShapeDtypeStruct(dims, dtype)


def iota(dims, axis):
    return lax.broadcasted_iota(jnp.int32, dims, axis)


def dot(a, b):
    return jnp.dot(a, b, preferred_element_type=F32)


def dot_nt(a, b):
    return lax.dot_general(a, b, (((1,), (1,)), ((), ())), preferred_element_type=F32)


def places(lengths_ref, sequence_of, slot_of):
    place = jnp.full(sequence_of.shape, -1, jnp.int32)
    start = 0
    for s in range(lengths_ref.shape[0]):
        held = lengths_ref[s]
        mine = (sequence_of == s) & (slot_of < held)
        place = jnp.where(mine, slot_of + start, place)
        start = start + held
    return place


def log2(n):
    assert n & (n - 1) == 0
    return n.bit_length() - 1


def front_kernel(heads, *refs):
    count = 9
    sources, refs = refs[:count], refs[count:]
    *outs, base_ref, pick_ref, place_ref, own_ref = refs[: -count - 2]
    *held, sems, out_ref = refs[-count - 2 :]
    copies = [pltpu.make_async_copy(a, b, sems.at[i]) for i, (a, b) in enumerate(zip(sources, held))]
    for copy in copies:
        copy.start()
    lengths_ref, tokens_ref, gain_ref, wa_ref, wb_ref, wq_ref, wk_ref, wv_ref, wg_ref = held
    total_rows = tokens_ref.shape[0]
    width = wq_ref.shape[1]
    all_heads = wa_ref.shape[0]
    packed = pick_ref.shape[0]
    copies[0].wait()
    own_ref[...] = jnp.full(own_ref.shape, lengths_ref[lax.axis_index("kv")], jnp.int32)
    col = iota(place_ref.shape, 1)
    place_ref[...] = places(
        lengths_ref,
        lax.shift_right_logical(col, log2(NEW * heads)),
        lax.shift_right_logical(col, log2(heads)) & 3,
    )
    pick = picker(lengths_ref, packed, total_rows)
    pick_ref[...] = pick
    dims = (2 * total_rows, total_rows)
    row, col = iota(dims, 0), iota(dims, 1)
    target = lax.shift_left(lax.shift_right_logical(row, 3), 2) + (row & 3)
    hit = target == col
    upper = (row & 7) < NEW
    zero, one = jnp.zeros(dims, F32), jnp.ones(dims, F32)
    place_a = jnp.where(hit & upper, one, zero).astype(BF16)
    place_b = jnp.where(hit & ~upper, one, zero).astype(BF16)
    fill = jnp.zeros((LANES - 2 * all_heads, wa_ref.shape[1]), BF16)
    for copy in copies[1:5]:
        copy.wait()
    tokens = tokens_ref[...]
    base_ref[...] = dot(pick, tokens)
    scaled = (tokens.astype(F32) * gain_ref[...]).astype(BF16)
    left = dot(place_a, scaled).astype(BF16)
    right = dot(place_b, scaled).astype(BF16)
    both = dot(place_a + place_b, tokens)
    squares = jnp.sum(both * both, axis=1, keepdims=True)
    small = dot_nt(left + right, jnp.concatenate([wa_ref[...], wb_ref[...], fill], axis=0))
    lane = iota(small.shape, 1)
    small = jnp.where(lane == 2 * all_heads, jnp.broadcast_to(squares, small.shape), small)
    high = small.astype(BF16).astype(F32)
    first = (iota(small.shape, 0) & 7) < NEW

    def put(columns, values):
        out_ref[:, :, columns] = values.reshape(-1, SUBS, values.shape[1]).astype(BF16)

    put(slice(2 * width, 2 * width + LANES), jnp.where(first, high, small - high))
    copies[5].wait()
    copies[6].wait()
    put(slice(0, width), dot(left, wq_ref[...]) + dot(right, wk_ref[...]))
    copies[7].wait()
    copies[8].wait()
    put(slice(width, 2 * width), dot(left, wv_ref[...]) + dot(right, wg_ref[...]))
    deal(out_ref, outs)


def deal(blocks_ref, outs, first=0):
    rows = slice(first, first + outs[0].shape[1])
    if len(outs) == 1:
        outs[0][...] = blocks_ref[:, rows, :]
        return
    plane = lax.axis_index("kv") & (PLANE - 1)
    for d, out in enumerate(outs):
        for z in range(out.shape[0]):
            out[z] = blocks_ref[z * PLANE + (plane ^ d), rows, :]


def fold_kernel(rows, columns, *refs):
    parts, outs = refs[:PLANE], refs[PLANE:]
    high = lax.shift_right_logical(lax.axis_index("kv"), log2(PLANE))
    for e, out in enumerate(outs):
        total = parts[0][high ^ e].astype(F32)
        for part in parts[1:]:
            total = total + part[high ^ e].astype(F32)
        out[...] = total.astype(out.dtype)
        if rows is None:
            continue
        value = total[rows, columns]
        value = value + pltpu.roll(value, NEW, 0)
        top = value.astype(BF16).astype(F32)
        value = jnp.where(iota(value.shape, 0) < NEW, top, value - top)
        out[rows, columns] = value.astype(out.dtype)


def partners(values, shift):
    count = lax.axis_size("kv")
    moved = []
    for d in reversed(range(1, len(values))):
        moved.append(lax.ppermute(values[d], "kv", [(i, i ^ (d << shift)) for i in range(count)]))
    return [values[0], *moved]


def staged():
    return lax.axis_size("kv") == PLANE * PLANE


def dealt(dims, kv):
    if staged():
        return [shape((PLANE, *dims), BF16)] * PLANE
    return [shape((kv, *dims), BF16)]


def reduce_scatter(outs, name, *halves, beside=None):
    if not staged():
        return [exchange(outs[0])], beside
    dims = outs[0].shape[1:]
    parts = partners(outs, 0)
    if beside is not None:
        parts, beside = lax.optimization_barrier((parts, beside))
    sums = call(
        functools.partial(fold_kernel, *halves),
        [shape(dims, F32 if e == 0 else BF16) for e in range(PLANE)],
        parts,
        [VMEM] * PLANE,
        8,
        1 << 20,
        name,
    )
    return [x[None] for x in partners(sums, log2(PLANE))], beside


def block_sum(refs, rows, columns):
    total = None
    for ref in refs:
        for i in range(ref.shape[0]):
            term = ref[i, rows, columns].astype(F32)
            total = term if total is None else total + term
    return total


def row_sum(refs, start, columns):
    return block_sum(refs, slice(None), slice(start, start + columns))


def recur_kernel(*refs):
    own_ref, *got_ref = refs[:-17]
    sources, (mixed_out, unit, late, left_ref) = refs[-17:-13], refs[-13:-9]
    gates, vals, preds, copies, *held, sems = refs[-9:]
    memory_ref, log_ref, bias_ref, gain_ref = held
    heads = memory_ref.shape[0]
    fetches = [pltpu.make_async_copy(a, b, sems.at[i]) for i, (a, b) in enumerate(zip(sources, held))]
    for fetch in fetches[1:] + fetches[:1]:
        fetch.start()
    width = heads * DK
    all_heads = heads * lax.axis_size("tp")
    tp_place = lax.axis_index("tp")
    small = row_sum(got_ref, 2 * width, LANES)
    small = small + pltpu.roll(small, NEW, 0)
    rstd = lax.rsqrt(small[:, 2 * all_heads : 2 * all_heads + 1] / D + epsilon)
    gates[...] = jnp.zeros(gates.shape, F32)
    factor = jnp.where(iota((SUBS, 1), 0) < NEW, DK ** (-0.5), 1.0)
    for h in range(heads):
        block = (row_sum(got_ref, h * DK, DK) * rstd).astype(BF16).astype(F32)
        norm = lax.rsqrt(jnp.sum(block * block, axis=1, keepdims=True) + epsilon)
        unit[h * SUBS : (h + 1) * SUBS, :] = block * norm * factor
        vals[h * SUBS : (h + 1) * SUBS, :] = (
            (row_sum(got_ref, width + h * DV, DV) * rstd).astype(BF16).astype(F32)
        )
    for fetch in fetches[1:]:
        fetch.wait()
    small = small * rstd
    alphas = pltpu.roll(small, LANES - tp_place * heads, 1)[:, :heads]
    betas = pltpu.roll(small, LANES - all_heads - tp_place * heads, 1)[:, :heads]
    x = alphas + bias_ref[...]
    soft = jnp.maximum(x, 0.0) + jnp.log1p(jnp.exp(-jnp.abs(x)))
    decay = -jnp.exp(log_ref[...]) * soft
    slot = iota(decay.shape, 0)
    live = (slot & 3) < own_ref[:, :heads]
    keep = jnp.exp(jnp.where(live, decay, 0.0))
    write = jnp.where(live, 1.0 / (1.0 + jnp.exp(-betas)), 0.0)
    gates[:SUBS, :heads] = jnp.where(slot < NEW, keep, write)
    turned = gates[...].T
    fetches[0].wait()
    for h in range(heads):
        own = slice(h * SUBS, (h + 1) * SUBS)
        preds[own, :] = jnp.dot(
            unit[own, :], memory_ref[h], precision=lax.Precision.HIGHEST, preferred_element_type=F32
        )

    def rows(ref, j):
        return ref[pl.ds(j, heads, stride=SUBS), :]

    queries = [rows(unit, t) for t in range(NEW)]
    keys = [rows(unit, NEW + t) for t in range(NEW)]
    keeps = [turned[:heads, t : t + 1] for t in range(NEW)]
    writes = [turned[:heads, NEW + t : NEW + t + 1] for t in range(NEW)]

    def inner(a, b):
        return jnp.sum(a * b, axis=1, keepdims=True)

    updates, outs = [], []
    passed = []
    total = jnp.ones((heads, 1), F32)
    for t in range(NEW):
        total = total * keeps[t]
        passed = [p * keeps[t] for p in passed]
        said = total * rows(preds, NEW + t)
        for i in range(t):
            said = said + (passed[i] * inner(keys[i], keys[t])) * updates[i]
        updates.append(writes[t] * (rows(vals, t) - said))
        passed.append(jnp.ones((heads, 1), F32))
        out = total * rows(preds, t)
        for i in range(t + 1):
            out = out + (passed[i] * inner(keys[i], queries[t])) * updates[i]
        outs.append(out)
    for i in range(NEW):
        late[pl.ds(i, heads, stride=SUBS), :] = jnp.zeros((heads, DV), F32)
        late[pl.ds(NEW + i, heads, stride=SUBS), :] = passed[i] * updates[i]
    left_ref[...] = jnp.broadcast_to(total, left_ref.shape)
    for t, out in enumerate(outs):
        out = out * lax.rsqrt(jnp.mean(out * out, axis=1, keepdims=True) + epsilon)
        gate = rows(vals, NEW + t)
        silu = gate * (1.0 / (1.0 + jnp.exp(-gate)))
        copies[t * heads : (t + 1) * heads, :] = out * gain_ref[...] * silu
    mixed = copies[...].astype(BF16)
    for d in range(mixed_out.shape[0]):
        mixed_out[d] = mixed


def advance_kernel(memory_ref, unit_ref, late_ref, left_ref, out_ref, fresh_ref, sems):
    stores = []
    for h in range(memory_ref.shape[0]):
        own = slice(h * SUBS, (h + 1) * SUBS)
        added = lax.dot_general(
            unit_ref[own, :],
            late_ref[own, :],
            (((0,), (0,)), ((), ())),
            precision=lax.Precision.HIGHEST,
            preferred_element_type=F32,
        )
        fresh_ref[h] = memory_ref[h] * left_ref[h : h + 1, :] + added
        stores.append(pltpu.make_async_copy(fresh_ref.at[h], out_ref.at[h], sems.at[h]))
        stores[-1].start()
    for store in stores:
        store.wait()


def project_kernel(place_ref, mixed_ref, w_ref, out_ref):
    heads = w_ref.shape[0] // DV
    total = mixed_ref.shape[0]
    packed = out_ref.shape[0]
    place = place_ref[...]
    head_of = iota((1, total), 1) & (heads - 1)
    row = iota((packed, total), 0)
    mixed = mixed_ref[...]
    rows = []
    for h in range(heads):
        pick = jnp.where(row == jnp.where(head_of == h, place, -1), 1.0, 0.0).astype(BF16)
        rows.append(dot(pick, mixed).astype(BF16))
    sum_ = None
    for h in range(heads):
        term = dot(rows[h], w_ref[h * DV : (h + 1) * DV, :])
        sum_ = term if sum_ is None else sum_ + term
    out_ref[...] = sum_


def picker(lengths_ref, packed, total_rows):
    col = iota((1, total_rows), 1)
    place = places(lengths_ref, lax.shift_right_logical(col, 2), col & 3)
    return jnp.where(iota((packed, total_rows), 0) == place, 1.0, 0.0).astype(BF16)


class Packing:
    def __init__(self, live, tiles, receivers):
        self.tiles = tiles
        self.shared = 0 < live % SUBS <= SUBS // 2 and tiles % 2 == 0
        self.whole = live // SUBS if self.shared else -(-live // SUBS)
        self.count = self.whole * tiles + (tiles // 2 if self.shared else 0)
        self.each = -(-self.count // receivers)

    def spot(self, block, tile):
        at = block * self.tiles + (tile if block < self.whole else tile // 2)
        return divmod(at, self.each)


def up_kernel(packing, inputs, *refs):
    *terms, base_ref, gain_ref, wg_ref, wu_ref = refs[:inputs]
    hidden_out, *outs = refs[inputs:-1]
    out_ref = refs[-1]
    packed = hidden_out.shape[0]
    hidden = base_ref[...]
    for term in terms:
        hidden = hidden + term[...]
    hidden = hidden.astype(BF16)
    hidden_out[...] = hidden
    hidden_f = hidden.astype(F32)
    scaled = (hidden_f * gain_ref[...]).astype(BF16)
    tiles = packing.tiles
    squares = jnp.broadcast_to(jnp.sum(hidden_f * hidden_f, axis=1, keepdims=True), (packed, LANES))
    own_lane = iota(squares.shape, 0) == iota(squares.shape, 1)
    squares = jnp.sum(jnp.where(own_lane, squares, 0.0), axis=0, keepdims=True)
    squares = jnp.broadcast_to(squares, (SUBS, LANES))
    high = squares.astype(BF16).astype(F32)
    halves = jnp.where(iota(squares.shape, 0) < NEW, high, squares - high).astype(BF16)
    step = 4
    for start in range(0, tiles, step):
        stop = min(start + step, tiles)
        span = slice(start * LANES, stop * LANES)
        gate = dot(scaled, wg_ref[:, span])
        up = dot(scaled, wu_ref[:, span])
        for t in range(start, stop):
            lanes = slice((t - start) * LANES, (t - start + 1) * LANES)
            for b in range(packed // SUBS):
                rows = slice(b * SUBS, (b + 1) * SUBS)
                one, two = gate[rows, lanes], up[rows, lanes]
                if b == packing.whole:
                    if t % 2 == 0:
                        held = one, two
                        continue
                    one = held[0] + pltpu.roll(one, SUBS // 2, 0)
                    two = held[1] + pltpu.roll(two, SUBS // 2, 0)
                d, i = packing.spot(b, t)
                out_ref[d, i * 16 : i * 16 + 16, :] = jnp.concatenate([one, two], axis=0).astype(BF16)
    for at in range(packing.count, out_ref.shape[0] * packing.each):
        d, i = divmod(at, packing.each)
        out_ref[d, i * 16 : i * 16 + 16, :] = jnp.zeros((16, LANES), BF16)
    for d in range(out_ref.shape[0]):
        out_ref[d, packing.each * 16 :, :] = halves
    half = len(outs) // 2
    deal(out_ref, outs[:half])
    deal(out_ref, outs[half:], outs[0].shape[1])


def active_kernel(packing, *refs):
    *got, out_ref = refs
    halves = got[: len(got) // 2], got[len(got) // 2 :]
    early = halves[0][0].shape[1]
    end = packing.each * 16 - early
    squares = block_sum(halves[1], slice(end, end + SUBS), slice(None))
    squares = squares + pltpu.roll(squares, SUBS // 2, 0)
    rstd = lax.rsqrt(squares / D + epsilon)
    row, lane = iota(rstd.shape, 0), iota(rstd.shape, 1)
    first = lax.axis_index("kv") * packing.each
    for i in range(packing.each):
        block = lax.div(first + i, packing.tiles)
        row_of = block * SUBS + row
        if packing.shared:
            row_of = jnp.where(block >= packing.whole, packing.whole * SUBS + (row & (SUBS // 2 - 1)), row_of)
        scale = jnp.sum(jnp.where(lane == row_of, rstd, 0.0), axis=1, keepdims=True)
        at = i * 16
        half, at = (halves[0], at) if at < early else (halves[1], at - early)
        pair = block_sum(half, slice(at, at + 16), slice(None))
        gate, up = pair[:SUBS] * scale, pair[SUBS:] * scale
        active = (gate * (1.0 / (1.0 + jnp.exp(-gate))) * up).astype(BF16)
        for d in range(out_ref.shape[0]):
            out_ref[d, i * SUBS : (i + 1) * SUBS, :] = active


def down_kernel(packing, got_ref, w_ref, out_ref):
    packed = out_ref.shape[0]
    tiles = w_ref.shape[0] // LANES
    sum_ = None
    for t in range(tiles):
        parts = []
        for b in range(packed // SUBS):
            d, i = packing.spot(b, t)
            part = got_ref[d, i * SUBS : (i + 1) * SUBS, :].astype(F32)
            parts.append(pltpu.roll(part, SUBS // 2, 0) if b == packing.whole and t % 2 else part)
        term = dot(jnp.concatenate(parts, axis=0).astype(BF16), w_ref[t * LANES : (t + 1) * LANES, :])
        sum_ = term if sum_ is None else sum_ + term
    out_ref[...] = sum_


def last_kernel(*refs):
    *terms, hidden_ref, pick_ref, out_ref = refs
    result = terms[0][...]
    for term in terms[1:]:
        result = result + term[...]
    result = (hidden_ref[...].astype(F32) + result).astype(BF16)
    out_ref[...] = lax.dot_general(
        pick_ref[...], result, (((0,), (0,)), ((), ())), preferred_element_type=F32
    ).astype(BF16)


def exchange(blocks):
    return lax.all_to_all(blocks, "kv", 0, 0)


def over_tp(terms):
    if lax.axis_size("tp") == 2:
        return [terms, lax.ppermute(terms, "tp", [(0, 1), (1, 0)])]
    return [lax.psum(terms, "tp")]


def per_device(
    tokens,
    lengths,
    memory,
    norm_gain,
    w_query,
    w_key,
    w_value,
    w_outgate,
    w_alpha,
    w_beta,
    decay_log,
    decay_bias,
    head_gain,
    w_output,
    mlp_gain,
    w_gate,
    w_up,
    w_down,
):
    total_rows, own_width = tokens.shape
    kv = lax.axis_size("kv")
    seq_dev, heads = memory.shape[:2]
    assert seq_dev == 1
    width = heads * DK
    sequences = lengths.shape[0]
    units = w_gate.shape[1]
    live = sequences * 7 // 4
    packed = -(-live // SUBS) * SUBS
    assert packed <= LANES
    packing = Packing(live, units // LANES, kv)
    columns = 2 * width + LANES

    operands = [lengths, tokens, norm_gain[None], w_alpha.T, w_beta.T, w_query, w_key, w_value, w_outgate]
    *sent, base, pick, place, own = call(
        functools.partial(front_kernel, heads),
        [
            *dealt((SUBS, columns), kv),
            shape((packed, own_width), F32),
            shape((packed, total_rows), BF16),
            shape((1, kv * NEW * heads), jnp.int32),
            shape((SUBS, LANES), jnp.int32),
        ],
        operands,
        [HBM] * len(operands),
        16,
        4 * total_rows * own_width * 4 * width,
        "front",
        [pltpu.SMEM(lengths.shape, jnp.int32), *(room(x) for x in operands[1:]), pltpu.SemaphoreType.DMA((len(operands),)), pltpu.VMEM((kv, SUBS, columns), BF16)],
    )
    got, _ = reduce_scatter(sent, "fold_rows", slice(None), slice(2 * width, columns))
    sent, unit, late, left = call(
        recur_kernel,
        [
            shape((kv, NEW * heads, DV), BF16),
            shape((heads * SUBS, DK), F32),
            shape((heads * SUBS, DV), F32),
            shape((heads, DV), F32),
        ],
        [own, *got, memory[0], decay_log[None], decay_bias[None], head_gain[None]],
        [VMEM] * (1 + len(got)) + [HBM] * 4,
        16,
        4 << 30,
        "recur",
        [
            pltpu.VMEM((LANES, LANES), F32),
            pltpu.VMEM((heads * SUBS, DV), F32),
            pltpu.VMEM((heads * SUBS, DV), F32),
            pltpu.VMEM((NEW * heads, DV), F32),
            pltpu.VMEM((heads, DK, DV), F32),
            pltpu.VMEM((1, heads), F32),
            pltpu.VMEM((1, heads), F32),
            pltpu.VMEM((1, DV), F32),
            pltpu.SemaphoreType.DMA((4,)),
        ],
    )
    (new_memory,) = call(
        advance_kernel,
        [shape((heads, DK, DV), F32)],
        [memory[0], unit, late, left],
        [VMEM] * 4,
        8,
        1 << 30,
        "advance",
        [pltpu.VMEM((heads, DK, DV), F32), pltpu.SemaphoreType.DMA((heads,))],
        [HBM],
    )
    got = exchange(sent).reshape(kv * NEW * heads, DV)
    (attn,) = call(
        project_kernel,
        [shape((packed, own_width), F32)],
        [place, got, w_output],
        [VMEM] * 3,
        8,
        32 << 20,
        "project",
    )
    terms = over_tp(attn)
    early = packing.each // 2 * 16
    block = (early, LANES), (packing.each * 16 + SUBS - early, LANES)
    hidden, *sent = call(
        functools.partial(up_kernel, packing, len(terms) + 4),
        [shape((packed, own_width), BF16), *dealt(block[0], kv), *dealt(block[1], kv)],
        [*terms, base, mlp_gain[None], w_gate, w_up],
        [VMEM] * (len(terms) + 4),
        16,
        4 * packed * own_width * units,
        "up",
        [pltpu.VMEM((kv, packing.each * 16 + SUBS, LANES), BF16)],
    )
    halves = sent[: len(sent) // 2], sent[len(sent) // 2 :]
    got_first, new_memory = reduce_scatter(halves[0], "fold_first", None, None, beside=new_memory)
    got_last, _ = reduce_scatter(halves[1], "fold_last", slice(block[1][0] - SUBS, None), slice(None))
    got = [*got_first, *got_last]
    (sent,) = call(
        functools.partial(active_kernel, packing),
        [shape((kv, packing.each * SUBS, LANES), BF16)],
        got,
        [VMEM] * len(got),
        8,
        1 << 20,
        "active",
    )
    got = exchange(sent)
    (feed,) = call(
        functools.partial(down_kernel, packing),
        [shape((packed, own_width), F32)],
        [got, w_down],
        [VMEM] * 2,
        16,
        2 * packed * own_width * units,
        "down",
    )
    terms = over_tp(feed)
    (layer_out,) = call(
        last_kernel,
        [shape((total_rows, own_width), BF16)],
        [*terms, hidden, pick],
        [VMEM] * (len(terms) + 2),
        8,
        1 << 20,
        "last",
    )
    return (layer_out, new_memory[None])


def solution(mesh):
    placed = (
        P(None, "kv"),
        P(),
        P("kv", "tp", None, None),
        P("kv"),
        P("kv", "tp"),
        P("kv", "tp"),
        P("kv", "tp"),
        P("kv", "tp"),
        P("kv", None),
        P("kv", None),
        P("tp"),
        P("tp"),
        P(),
        P("tp", "kv"),
        P("kv"),
        P("kv", "tp"),
        P("kv", "tp"),
        P("tp", "kv"),
    )
    return jax.shard_map(
        per_device,
        mesh=mesh,
        in_specs=placed,
        out_specs=(P(None, "kv"), P("kv", "tp", None, None)),
        check_vma=False,
    )
```

```python
import functools

import jax
import jax.numpy as jnp
from jax import lax
from jax.experimental import pallas as pl
from jax.experimental.pallas import tpu as pltpu
from jax.sharding import PartitionSpec as P

D = 4096
DK = 128
DV = 128
NEW = 4
LANES = 128
PLANE = 4
SUBS = 8

epsilon = 1e-06


F32 = jnp.float32
BF16 = jnp.bfloat16
VMEM = pl.BlockSpec(memory_space=pltpu.VMEM)
HBM = pl.BlockSpec(memory_space=pltpu.HBM)


def call(body, outs, ins, specs, limit, flops, name, scratch=(), out_specs=None):
    moved = sum(x.size * x.dtype.itemsize for x in (*outs, *ins))
    ins = [pltpu.with_memory_space_constraint(x, pltpu.HBM) if s is HBM else x for x, s in zip(ins, specs)]
    return pl.pallas_call(
        body,
        out_shape=outs,
        in_specs=specs,
        out_specs=out_specs or [VMEM] * len(outs),
        scratch_shapes=list(scratch),
        compiler_params=pltpu.CompilerParams(vmem_limit_bytes=limit << 20),
        cost_estimate=pl.CostEstimate(flops=flops, bytes_accessed=moved, transcendentals=0),
        name=name,
    )(*ins)


def room(x):
    return pltpu.VMEM(x.shape, x.dtype)


def shape(dims, dtype):
    return jax.ShapeDtypeStruct(dims, dtype)


def iota(dims, axis):
    return lax.broadcasted_iota(jnp.int32, dims, axis)


def dot(a, b):
    return jnp.dot(a, b, preferred_element_type=F32)


def dot_nt(a, b):
    return lax.dot_general(a, b, (((1,), (1,)), ((), ())), preferred_element_type=F32)


def places(lengths_ref, sequence_of, slot_of):
    place = jnp.full(sequence_of.shape, -1, jnp.int32)
    start = 0
    for s in range(lengths_ref.shape[0]):
        held = lengths_ref[s]
        mine = (sequence_of == s) & (slot_of < held)
        place = jnp.where(mine, slot_of + start, place)
        start = start + held
    return place


def log2(n):
    assert n & (n - 1) == 0
    return n.bit_length() - 1


def front_kernel(heads, *refs):
    count = 9
    sources, refs = refs[:count], refs[count:]
    *outs, base_ref, pick_ref, place_ref, own_ref = refs[: -count - 2]
    *held, sems, out_ref = refs[-count - 2 :]
    copies = [pltpu.make_async_copy(a, b, sems.at[i]) for i, (a, b) in enumerate(zip(sources, held))]
    for copy in copies:
        copy.start()
    lengths_ref, tokens_ref, gain_ref, wa_ref, wb_ref, wq_ref, wk_ref, wv_ref, wg_ref = held
    total_rows = tokens_ref.shape[0]
    width = wq_ref.shape[1]
    all_heads = wa_ref.shape[0]
    packed = pick_ref.shape[0]
    copies[0].wait()
    own_ref[...] = jnp.full(own_ref.shape, lengths_ref[lax.axis_index("kv")], jnp.int32)
    col = iota(place_ref.shape, 1)
    place_ref[...] = places(
        lengths_ref,
        lax.shift_right_logical(col, log2(NEW * heads)),
        lax.shift_right_logical(col, log2(heads)) & 3,
    )
    pick = picker(lengths_ref, packed, total_rows)
    pick_ref[...] = pick
    dims = (2 * total_rows, total_rows)
    row, col = iota(dims, 0), iota(dims, 1)
    target = lax.shift_left(lax.shift_right_logical(row, 3), 2) + (row & 3)
    hit = target == col
    upper = (row & 7) < NEW
    zero, one = jnp.zeros(dims, F32), jnp.ones(dims, F32)
    place_a = jnp.where(hit & upper, one, zero).astype(BF16)
    place_b = jnp.where(hit & ~upper, one, zero).astype(BF16)
    fill = jnp.zeros((LANES - 2 * all_heads, wa_ref.shape[1]), BF16)
    for copy in copies[1:5]:
        copy.wait()
    tokens = tokens_ref[...]
    base_ref[...] = dot(pick, tokens)
    scaled = (tokens.astype(F32) * gain_ref[...]).astype(BF16)
    left = dot(place_a, scaled).astype(BF16)
    right = dot(place_b, scaled).astype(BF16)
    both = dot(place_a + place_b, tokens)
    squares = jnp.sum(both * both, axis=1, keepdims=True)
    small = dot_nt(left + right, jnp.concatenate([wa_ref[...], wb_ref[...], fill], axis=0))
    lane = iota(small.shape, 1)
    small = jnp.where(lane == 2 * all_heads, jnp.broadcast_to(squares, small.shape), small)
    high = small.astype(BF16).astype(F32)
    first = (iota(small.shape, 0) & 7) < NEW

    def put(columns, values):
        out_ref[:, :, columns] = values.reshape(-1, SUBS, values.shape[1]).astype(BF16)

    put(slice(2 * width, 2 * width + LANES), jnp.where(first, high, small - high))
    copies[5].wait()
    copies[6].wait()
    put(slice(0, width), dot(left, wq_ref[...]) + dot(right, wk_ref[...]))
    copies[7].wait()
    copies[8].wait()
    put(slice(width, 2 * width), dot(left, wv_ref[...]) + dot(right, wg_ref[...]))
    deal(out_ref, outs)


def deal(blocks_ref, outs):
    if len(outs) == 1:
        outs[0][...] = blocks_ref[...]
        return
    plane = lax.axis_index("kv") & (PLANE - 1)
    for d, out in enumerate(outs):
        for z in range(out.shape[0]):
            out[z] = blocks_ref[z * PLANE + (plane ^ d)]


def fold_kernel(rows, columns, axis, half, *refs):
    parts, outs = refs[:PLANE], refs[PLANE:]
    high = lax.shift_right_logical(lax.axis_index("kv"), log2(PLANE))
    for e, out in enumerate(outs):
        total = parts[0][high ^ e].astype(F32)
        for part in parts[1:]:
            total = total + part[high ^ e].astype(F32)
        out[...] = total.astype(out.dtype)
        value = total[rows, columns]
        value = value + pltpu.roll(value, half, axis)
        top = value.astype(BF16).astype(F32)
        value = jnp.where(iota(value.shape, axis) < half, top, value - top)
        out[rows, columns] = value.astype(out.dtype)


def partners(values, shift):
    count = lax.axis_size("kv")
    moved = []
    for d in reversed(range(1, len(values))):
        moved.append(lax.ppermute(values[d], "kv", [(i, i ^ (d << shift)) for i in range(count)]))
    return [values[0], *moved]


def staged():
    return lax.axis_size("kv") == PLANE * PLANE


def dealt(dims, kv):
    if staged():
        return [shape((PLANE, *dims), BF16)] * PLANE
    return [shape((kv, *dims), BF16)]


def reduce_scatter(outs, name, *halves, beside=None):
    if not staged():
        return [exchange(outs[0])], beside
    dims = outs[0].shape[1:]
    parts = partners(outs, 0)
    if beside is not None:
        parts, beside = lax.optimization_barrier((parts, beside))
    sums = call(
        functools.partial(fold_kernel, *halves),
        [shape(dims, F32 if e == 0 else BF16) for e in range(PLANE)],
        parts,
        [VMEM] * PLANE,
        8,
        1 << 20,
        name,
    )
    return [x[None] for x in partners(sums, log2(PLANE))], beside


def block_sum(refs, rows, columns):
    total = None
    for ref in refs:
        for i in range(ref.shape[0]):
            term = ref[i, rows, columns].astype(F32)
            total = term if total is None else total + term
    return total


def row_sum(refs, start, columns):
    return block_sum(refs, slice(None), slice(start, start + columns))


def recur_kernel(*refs):
    own_ref, *got_ref = refs[:-17]
    sources, (mixed_out, unit, late, left_ref) = refs[-17:-13], refs[-13:-9]
    gates, vals, preds, copies, *held, sems = refs[-9:]
    memory_ref, log_ref, bias_ref, gain_ref = held
    heads = memory_ref.shape[0]
    fetches = [pltpu.make_async_copy(a, b, sems.at[i]) for i, (a, b) in enumerate(zip(sources, held))]
    for fetch in fetches[1:] + fetches[:1]:
        fetch.start()
    width = heads * DK
    all_heads = heads * lax.axis_size("tp")
    tp_place = lax.axis_index("tp")
    small = row_sum(got_ref, 2 * width, LANES)
    small = small + pltpu.roll(small, NEW, 0)
    rstd = lax.rsqrt(small[:, 2 * all_heads : 2 * all_heads + 1] / D + epsilon)
    gates[...] = jnp.zeros(gates.shape, F32)
    factor = jnp.where(iota((SUBS, 1), 0) < NEW, DK ** (-0.5), 1.0)
    for h in range(heads):
        block = (row_sum(got_ref, h * DK, DK) * rstd).astype(BF16).astype(F32)
        norm = lax.rsqrt(jnp.sum(block * block, axis=1, keepdims=True) + epsilon)
        unit[h * SUBS : (h + 1) * SUBS, :] = block * norm * factor
        vals[h * SUBS : (h + 1) * SUBS, :] = (
            (row_sum(got_ref, width + h * DV, DV) * rstd).astype(BF16).astype(F32)
        )
    for fetch in fetches[1:]:
        fetch.wait()
    small = small * rstd
    alphas = pltpu.roll(small, LANES - tp_place * heads, 1)[:, :heads]
    betas = pltpu.roll(small, LANES - all_heads - tp_place * heads, 1)[:, :heads]
    x = alphas + bias_ref[...]
    soft = jnp.maximum(x, 0.0) + jnp.log1p(jnp.exp(-jnp.abs(x)))
    decay = -jnp.exp(log_ref[...]) * soft
    slot = iota(decay.shape, 0)
    live = (slot & 3) < own_ref[:, :heads]
    keep = jnp.exp(jnp.where(live, decay, 0.0))
    write = jnp.where(live, 1.0 / (1.0 + jnp.exp(-betas)), 0.0)
    gates[:SUBS, :heads] = jnp.where(slot < NEW, keep, write)
    turned = gates[...].T
    fetches[0].wait()
    for h in range(heads):
        own = slice(h * SUBS, (h + 1) * SUBS)
        preds[own, :] = jnp.dot(
            unit[own, :], memory_ref[h], precision=lax.Precision.HIGHEST, preferred_element_type=F32
        )

    def rows(ref, j):
        return ref[pl.ds(j, heads, stride=SUBS), :]

    queries = [rows(unit, t) for t in range(NEW)]
    keys = [rows(unit, NEW + t) for t in range(NEW)]
    keeps = [turned[:heads, t : t + 1] for t in range(NEW)]
    writes = [turned[:heads, NEW + t : NEW + t + 1] for t in range(NEW)]

    def inner(a, b):
        return jnp.sum(a * b, axis=1, keepdims=True)

    updates, outs = [], []
    passed = []
    total = jnp.ones((heads, 1), F32)
    for t in range(NEW):
        total = total * keeps[t]
        passed = [p * keeps[t] for p in passed]
        said = total * rows(preds, NEW + t)
        for i in range(t):
            said = said + (passed[i] * inner(keys[i], keys[t])) * updates[i]
        updates.append(writes[t] * (rows(vals, t) - said))
        passed.append(jnp.ones((heads, 1), F32))
        out = total * rows(preds, t)
        for i in range(t + 1):
            out = out + (passed[i] * inner(keys[i], queries[t])) * updates[i]
        outs.append(out)
    for i in range(NEW):
        late[pl.ds(i, heads, stride=SUBS), :] = jnp.zeros((heads, DV), F32)
        late[pl.ds(NEW + i, heads, stride=SUBS), :] = passed[i] * updates[i]
    left_ref[...] = jnp.broadcast_to(total, left_ref.shape)
    for t, out in enumerate(outs):
        out = out * lax.rsqrt(jnp.mean(out * out, axis=1, keepdims=True) + epsilon)
        gate = rows(vals, NEW + t)
        silu = gate * (1.0 / (1.0 + jnp.exp(-gate)))
        copies[t * heads : (t + 1) * heads, :] = out * gain_ref[...] * silu
    mixed = copies[...].astype(BF16)
    for d in range(mixed_out.shape[0]):
        mixed_out[d] = mixed


def advance_kernel(memory_ref, unit_ref, late_ref, left_ref, out_ref, fresh_ref, sems):
    stores = []
    for h in range(memory_ref.shape[0]):
        own = slice(h * SUBS, (h + 1) * SUBS)
        added = lax.dot_general(
            unit_ref[own, :],
            late_ref[own, :],
            (((0,), (0,)), ((), ())),
            precision=lax.Precision.HIGHEST,
            preferred_element_type=F32,
        )
        fresh_ref[h] = memory_ref[h] * left_ref[h : h + 1, :] + added
        stores.append(pltpu.make_async_copy(fresh_ref.at[h], out_ref.at[h], sems.at[h]))
        stores[-1].start()
    for store in stores:
        store.wait()


def project_kernel(place_ref, mixed_ref, w_ref, out_ref):
    heads = w_ref.shape[0] // DV
    total = mixed_ref.shape[0]
    packed = out_ref.shape[0]
    place = place_ref[...]
    head_of = iota((1, total), 1) & (heads - 1)
    row = iota((packed, total), 0)
    mixed = mixed_ref[...]
    rows = []
    for h in range(heads):
        pick = jnp.where(row == jnp.where(head_of == h, place, -1), 1.0, 0.0).astype(BF16)
        rows.append(dot(pick, mixed).astype(BF16))
    sum_ = None
    for h in range(heads):
        term = dot(rows[h], w_ref[h * DV : (h + 1) * DV, :])
        sum_ = term if sum_ is None else sum_ + term
    out_ref[...] = sum_


def picker(lengths_ref, packed, total_rows):
    col = iota((1, total_rows), 1)
    place = places(lengths_ref, lax.shift_right_logical(col, 2), col & 3)
    return jnp.where(iota((packed, total_rows), 0) == place, 1.0, 0.0).astype(BF16)


class Packing:
    def __init__(self, live, tiles, receivers, members):
        self.members = members
        self.tiles = tiles // members
        self.receivers = receivers // members
        self.shared = 0 < live % SUBS <= SUBS // 2
        self.whole = live // SUBS if self.shared else -(-live // SUBS)
        self.count = self.whole * self.tiles + (-(-self.tiles // 2) if self.shared else 0)
        self.each = -(-self.count // self.receivers)

    def spot(self, block, tile):
        at = block * self.tiles + (tile if block < self.whole else tile // 2)
        return divmod(at, self.each)


def up_kernel(packing, partner, inputs, *refs):
    *terms, base_ref, gain_ref, wg_ref, wu_ref = refs[:inputs]
    out_ref, hidden_out = refs[inputs:]
    packed = hidden_out.shape[0]
    first = 0
    if packing.members > 1:
        member = (lax.axis_index("kv") & (packing.members - 1)) ^ partner
        first = member * (packing.tiles * LANES)
    hidden = base_ref[...]
    for term in terms:
        hidden = hidden + term[...]
    hidden = hidden.astype(BF16)
    hidden_out[...] = hidden
    hidden_f = hidden.astype(F32)
    scaled = (hidden_f * gain_ref[...]).astype(BF16)
    tiles = packing.tiles
    squares = jnp.broadcast_to(jnp.sum(hidden_f * hidden_f, axis=1, keepdims=True), (packed, LANES))
    own_lane = iota(squares.shape, 0) == iota(squares.shape, 1)
    squares = jnp.sum(jnp.where(own_lane, squares, 0.0), axis=0, keepdims=True)
    squares = jnp.broadcast_to(squares, (SUBS, LANES))
    high = squares.astype(BF16).astype(F32)
    halves = jnp.where(iota(squares.shape, 0) < NEW, high, squares - high).astype(BF16)
    step = 4
    for start in range(0, tiles, step):
        stop = min(start + step, tiles)
        span = pl.ds(pl.multiple_of(first + start * LANES, LANES), (stop - start) * LANES)
        gate = dot(scaled, wg_ref[:, span])
        up = dot(scaled, wu_ref[:, span])
        for t in range(start, stop):
            lanes = slice((t - start) * LANES, (t - start + 1) * LANES)
            for b in range(packed // SUBS):
                rows = slice(b * SUBS, (b + 1) * SUBS)
                one, two = gate[rows, lanes], up[rows, lanes]
                if b == packing.whole:
                    if t % 2 == 0 and t + 1 < tiles:
                        held = one, two
                        continue
                    if t % 2:
                        one = held[0] + pltpu.roll(one, SUBS // 2, 0)
                        two = held[1] + pltpu.roll(two, SUBS // 2, 0)
                d, i = packing.spot(b, t)
                out_ref[d, i * 16 : i * 16 + 16, :] = jnp.concatenate([one, two], axis=0).astype(BF16)
    for at in range(packing.count, out_ref.shape[0] * packing.each):
        d, i = divmod(at, packing.each)
        out_ref[d, i * 16 : i * 16 + 16, :] = jnp.zeros((16, LANES), BF16)
    for d in range(out_ref.shape[0]):
        out_ref[d, packing.each * 16 :, :] = halves


def active_kernel(packing, *refs):
    *got, out_ref = refs
    end = packing.each * 16
    squares = block_sum(got, slice(end, end + SUBS), slice(None))
    squares = squares + pltpu.roll(squares, SUBS // 2, 0)
    rstd = lax.rsqrt(squares / D + epsilon)
    row, lane = iota(rstd.shape, 0), iota(rstd.shape, 1)
    first = lax.shift_right_logical(lax.axis_index("kv"), log2(packing.members)) * packing.each
    for i in range(packing.each):
        block = lax.div(first + i, packing.tiles)
        row_of = block * SUBS + row
        if packing.shared:
            row_of = jnp.where(block >= packing.whole, packing.whole * SUBS + (row & (SUBS // 2 - 1)), row_of)
        scale = jnp.sum(jnp.where(lane == row_of, rstd, 0.0), axis=1, keepdims=True)
        pair = block_sum(got, slice(i * 16, i * 16 + 16), slice(None))
        gate, up = pair[:SUBS] * scale, pair[SUBS:] * scale
        active = (gate * (1.0 / (1.0 + jnp.exp(-gate))) * up).astype(BF16)
        for d in range(out_ref.shape[0]):
            out_ref[d, i * SUBS : (i + 1) * SUBS, :] = active


def down_kernel(packing, got_ref, w_ref, out_ref):
    packed = out_ref.shape[0]
    tiles = w_ref.shape[0] // LANES
    sum_ = None
    for t in range(tiles):
        parts = []
        for b in range(packed // SUBS):
            member, tile = divmod(t, packing.tiles)
            receiver, i = packing.spot(b, tile)
            d = receiver * packing.members + member
            part = got_ref[d, i * SUBS : (i + 1) * SUBS, :].astype(F32)
            parts.append(pltpu.roll(part, SUBS // 2, 0) if b == packing.whole and tile % 2 else part)
        term = dot(jnp.concatenate(parts, axis=0).astype(BF16), w_ref[t * LANES : (t + 1) * LANES, :])
        sum_ = term if sum_ is None else sum_ + term
    out_ref[...] = sum_


def last_kernel(*refs):
    *terms, hidden_ref, pick_ref, out_ref = refs
    result = terms[0][...]
    for term in terms[1:]:
        result = result + term[...]
    result = (hidden_ref[...].astype(F32) + result).astype(BF16)
    out_ref[...] = lax.dot_general(
        pick_ref[...], result, (((0,), (0,)), ((), ())), preferred_element_type=F32
    ).astype(BF16)


def exchange(blocks):
    return lax.all_to_all(blocks, "kv", 0, 0)


def over_tp(terms):
    if lax.axis_size("tp") == 2:
        return [terms, lax.ppermute(terms, "tp", [(0, 1), (1, 0)])]
    return [lax.psum(terms, "tp")]


def per_device(
    tokens,
    lengths,
    memory,
    norm_gain,
    w_query,
    w_key,
    w_value,
    w_outgate,
    w_alpha,
    w_beta,
    decay_log,
    decay_bias,
    head_gain,
    w_output,
    mlp_gain,
    w_gate,
    w_up,
    w_down,
):
    total_rows, own_width = tokens.shape
    kv = lax.axis_size("kv")
    seq_dev, heads = memory.shape[:2]
    assert seq_dev == 1
    width = heads * DK
    sequences = lengths.shape[0]
    units = w_gate.shape[1]
    live = sequences * 7 // 4
    packed = -(-live // SUBS) * SUBS
    assert packed <= LANES
    packing = Packing(live, units // LANES, kv, PLANE if staged() else 1)
    assert units % (packing.members * LANES) == 0
    columns = 2 * width + LANES

    operands = [lengths, tokens, norm_gain[None], w_alpha.T, w_beta.T, w_query, w_key, w_value, w_outgate]
    *sent, base, pick, place, own = call(
        functools.partial(front_kernel, heads),
        [
            *dealt((SUBS, columns), kv),
            shape((packed, own_width), F32),
            shape((packed, total_rows), BF16),
            shape((1, kv * NEW * heads), jnp.int32),
            shape((SUBS, LANES), jnp.int32),
        ],
        operands,
        [HBM] * len(operands),
        16,
        4 * total_rows * own_width * 4 * width,
        "front",
        [pltpu.SMEM(lengths.shape, jnp.int32), *(room(x) for x in operands[1:]), pltpu.SemaphoreType.DMA((len(operands),)), pltpu.VMEM((kv, SUBS, columns), BF16)],
    )
    got, _ = reduce_scatter(sent, "fold_rows", slice(None), slice(2 * width, columns), 0, NEW)
    sent, unit, late, left = call(
        recur_kernel,
        [
            shape((kv, NEW * heads, DV), BF16),
            shape((heads * SUBS, DK), F32),
            shape((heads * SUBS, DV), F32),
            shape((heads, DV), F32),
        ],
        [own, *got, memory[0], decay_log[None], decay_bias[None], head_gain[None]],
        [VMEM] * (1 + len(got)) + [HBM] * 4,
        16,
        4 << 30,
        "recur",
        [
            pltpu.VMEM((LANES, LANES), F32),
            pltpu.VMEM((heads * SUBS, DV), F32),
            pltpu.VMEM((heads * SUBS, DV), F32),
            pltpu.VMEM((NEW * heads, DV), F32),
            pltpu.VMEM((heads, DK, DV), F32),
            pltpu.VMEM((1, heads), F32),
            pltpu.VMEM((1, heads), F32),
            pltpu.VMEM((1, DV), F32),
            pltpu.SemaphoreType.DMA((4,)),
        ],
    )
    (new_memory,) = call(
        advance_kernel,
        [shape((heads, DK, DV), F32)],
        [memory[0], unit, late, left],
        [VMEM] * 4,
        8,
        1 << 30,
        "advance",
        [pltpu.VMEM((heads, DK, DV), F32), pltpu.SemaphoreType.DMA((heads,))],
        [HBM],
    )
    got = exchange(sent).reshape(kv * NEW * heads, DV)
    (attn,) = call(
        project_kernel,
        [shape((packed, own_width), F32)],
        [place, got, w_output],
        [VMEM] * 3,
        8,
        32 << 20,
        "project",
    )
    terms = over_tp(attn)
    outs = [
        shape((packing.receivers, packing.each * 16 + SUBS, LANES), BF16),
        shape((packed, own_width), BF16),
    ]
    sent = []
    for d in range(packing.members):
        part, hidden = call(
            functools.partial(up_kernel, packing, d, len(terms) + 4),
            outs,
            [*terms, base, mlp_gain[None], w_gate, w_up],
            [VMEM] * (len(terms) + 4),
            16,
            4 * packed * own_width * units // packing.members,
            f"up_{d}",
        )
        sent.append(part)
    got, new_memory = reduce_scatter(
        sent, "fold_units", slice(packing.each * 16, None), slice(None), 0, NEW, beside=new_memory
    )
    (sent,) = call(
        functools.partial(active_kernel, packing),
        [shape((kv, packing.each * SUBS, LANES), BF16)],
        got,
        [VMEM] * len(got),
        8,
        1 << 20,
        "active",
    )
    got = exchange(sent)
    (feed,) = call(
        functools.partial(down_kernel, packing),
        [shape((packed, own_width), F32)],
        [got, w_down],
        [VMEM] * 2,
        16,
        2 * packed * own_width * units,
        "down",
    )
    terms = over_tp(feed)
    (layer_out,) = call(
        last_kernel,
        [shape((total_rows, own_width), BF16)],
        [*terms, hidden, pick],
        [VMEM] * (len(terms) + 2),
        8,
        1 << 20,
        "last",
    )
    return (layer_out, new_memory[None])


def solution(mesh):
    placed = (
        P(None, "kv"),
        P(),
        P("kv", "tp", None, None),
        P("kv"),
        P("kv", "tp"),
        P("kv", "tp"),
        P("kv", "tp"),
        P("kv", "tp"),
        P("kv", None),
        P("kv", None),
        P("tp"),
        P("tp"),
        P(),
        P("tp", "kv"),
        P("kv"),
        P("kv", "tp"),
        P("kv", "tp"),
        P("tp", "kv"),
    )
    return jax.shard_map(
        per_device,
        mesh=mesh,
        in_specs=placed,
        out_specs=(P(None, "kv"), P("kv", "tp", None, None)),
        check_vma=False,
    )
```

```python
import functools

import jax
import jax.numpy as jnp
from jax import lax
from jax.experimental import pallas as pl
from jax.experimental.pallas import tpu as pltpu
from jax.sharding import PartitionSpec as P

D = 4096
DK = 128
DV = 128
NEW = 4
LANES = 128
PLANE = 4
SUBS = 8

epsilon = 1e-06


F32 = jnp.float32
BF16 = jnp.bfloat16
VMEM = pl.BlockSpec(memory_space=pltpu.VMEM)
HBM = pl.BlockSpec(memory_space=pltpu.HBM)


def call(body, outs, ins, specs, limit, flops, name, scratch=(), out_specs=None):
    moved = sum(x.size * x.dtype.itemsize for x in (*outs, *ins))
    ins = [pltpu.with_memory_space_constraint(x, pltpu.HBM) if s is HBM else x for x, s in zip(ins, specs)]
    return pl.pallas_call(
        body,
        out_shape=outs,
        in_specs=specs,
        out_specs=out_specs or [VMEM] * len(outs),
        scratch_shapes=list(scratch),
        compiler_params=pltpu.CompilerParams(vmem_limit_bytes=limit << 20),
        cost_estimate=pl.CostEstimate(flops=flops, bytes_accessed=moved, transcendentals=0),
        name=name,
    )(*ins)


def room(x):
    return pltpu.VMEM(x.shape, x.dtype)


def shape(dims, dtype):
    return jax.ShapeDtypeStruct(dims, dtype)


def iota(dims, axis):
    return lax.broadcasted_iota(jnp.int32, dims, axis)


def dot(a, b):
    return jnp.dot(a, b, preferred_element_type=F32)


def dot_nt(a, b):
    return lax.dot_general(a, b, (((1,), (1,)), ((), ())), preferred_element_type=F32)


def places(lengths_ref, sequence_of, slot_of):
    place = jnp.full(sequence_of.shape, -1, jnp.int32)
    start = 0
    for s in range(lengths_ref.shape[0]):
        held = lengths_ref[s]
        mine = (sequence_of == s) & (slot_of < held)
        place = jnp.where(mine, slot_of + start, place)
        start = start + held
    return place


def log2(n):
    assert n & (n - 1) == 0
    return n.bit_length() - 1


def front_kernel(heads, *refs):
    count = 9
    sources, refs = refs[:count], refs[count:]
    *outs, base_ref, pick_ref, place_ref, own_ref = refs[: -count - 2]
    *held, sems, out_ref = refs[-count - 2 :]
    copies = [pltpu.make_async_copy(a, b, sems.at[i]) for i, (a, b) in enumerate(zip(sources, held))]
    for copy in copies:
        copy.start()
    lengths_ref, tokens_ref, gain_ref, wa_ref, wb_ref, wq_ref, wk_ref, wv_ref, wg_ref = held
    total_rows = tokens_ref.shape[0]
    width = wq_ref.shape[1]
    all_heads = wa_ref.shape[0]
    packed = pick_ref.shape[1]
    copies[0].wait()
    own_ref[...] = jnp.full(own_ref.shape, lengths_ref[lax.axis_index("kv")], jnp.int32)
    col = iota(place_ref.shape, 1)
    place_ref[...] = places(
        lengths_ref,
        lax.shift_right_logical(col, log2(NEW * heads)),
        lax.shift_right_logical(col, log2(heads)) & 3,
    )
    pick = picker(lengths_ref, packed, total_rows)
    pick_ref[...] = pick.astype(F32).T.astype(BF16)
    dims = (2 * total_rows, total_rows)
    row, col = iota(dims, 0), iota(dims, 1)
    target = lax.shift_left(lax.shift_right_logical(row, 3), 2) + (row & 3)
    hit = target == col
    upper = (row & 7) < NEW
    zero, one = jnp.zeros(dims, F32), jnp.ones(dims, F32)
    place_a = jnp.where(hit & upper, one, zero).astype(BF16)
    place_b = jnp.where(hit & ~upper, one, zero).astype(BF16)
    fill = jnp.zeros((LANES - 2 * all_heads, wa_ref.shape[1]), BF16)
    for copy in copies[1:5]:
        copy.wait()
    tokens = tokens_ref[...]
    base_ref[...] = dot(pick, tokens)
    scaled = (tokens.astype(F32) * gain_ref[...]).astype(BF16)
    left = dot(place_a, scaled).astype(BF16)
    right = dot(place_b, scaled).astype(BF16)
    both = dot(place_a + place_b, tokens)
    squares = jnp.sum(both * both, axis=1, keepdims=True)
    small = dot_nt(left + right, jnp.concatenate([wa_ref[...], wb_ref[...], fill], axis=0))
    lane = iota(small.shape, 1)
    small = jnp.where(lane == 2 * all_heads, jnp.broadcast_to(squares, small.shape), small)
    high = small.astype(BF16).astype(F32)
    first = (iota(small.shape, 0) & 7) < NEW

    def put(columns, values):
        out_ref[:, :, columns] = values.reshape(-1, SUBS, values.shape[1]).astype(BF16)

    put(slice(2 * width, 2 * width + LANES), jnp.where(first, high, small - high))
    copies[5].wait()
    copies[6].wait()
    put(slice(0, width), dot(left, wq_ref[...]) + dot(right, wk_ref[...]))
    copies[7].wait()
    copies[8].wait()
    put(slice(width, 2 * width), dot(left, wv_ref[...]) + dot(right, wg_ref[...]))
    deal(out_ref, outs)


def deal(blocks_ref, outs):
    if len(outs) == 1:
        outs[0][...] = blocks_ref[...]
        return
    plane = lax.axis_index("kv") & (PLANE - 1)
    for d, out in enumerate(outs):
        for z in range(out.shape[0]):
            out[z] = blocks_ref[z * PLANE + (plane ^ d)]


def fold_kernel(rows, columns, axis, half, *refs):
    parts, outs = refs[:PLANE], refs[PLANE:]
    high = lax.shift_right_logical(lax.axis_index("kv"), log2(PLANE))
    for e, out in enumerate(outs):
        total = parts[0][high ^ e].astype(F32)
        for part in parts[1:]:
            total = total + part[high ^ e].astype(F32)
        out[...] = total.astype(out.dtype)
        value = total[rows, columns]
        value = value + pltpu.roll(value, half, axis)
        top = value.astype(BF16).astype(F32)
        value = jnp.where(iota(value.shape, axis) < half, top, value - top)
        out[rows, columns] = value.astype(out.dtype)


def partners(values, shift, order):
    count = lax.axis_size("kv")
    moved = []
    for d in order:
        moved.append(lax.ppermute(values[d], "kv", [(i, i ^ (d << shift)) for i in range(count)]))
    return [values[0], *moved]


def staged():
    return lax.axis_size("kv") == PLANE * PLANE


def dealt(dims, kv):
    if staged():
        return [shape((PLANE, *dims), BF16)] * PLANE
    return [shape((kv, *dims), BF16)]


def reduce_scatter(outs, name, *halves, order=(3, 2, 1), beside=None):
    if not staged():
        return [exchange(outs[0])], beside
    dims = outs[0].shape[1:]
    parts = partners(outs, 0, (3, 2, 1))
    if beside is not None:
        parts, beside = lax.optimization_barrier((parts, beside))
    sums = call(
        functools.partial(fold_kernel, *halves),
        [shape(dims, F32 if e == 0 else BF16) for e in range(PLANE)],
        parts,
        [VMEM] * PLANE,
        8,
        1 << 20,
        name,
    )
    return [x[None] for x in partners(sums, log2(PLANE), order)], beside


def block_sum(refs, rows, columns):
    total = None
    for ref in refs:
        for i in range(ref.shape[0]):
            term = ref[i, rows, columns].astype(F32)
            total = term if total is None else total + term
    return total


def row_sum(refs, start, columns):
    return block_sum(refs, slice(None), slice(start, start + columns))


def recur_kernel(*refs):
    own_ref, *got_ref = refs[:-17]
    sources, (mixed_out, unit, late, left_ref) = refs[-17:-13], refs[-13:-9]
    gates, vals, preds, copies, *held, sems = refs[-9:]
    memory_ref, log_ref, bias_ref, gain_ref = held
    heads = memory_ref.shape[0]
    fetches = [pltpu.make_async_copy(a, b, sems.at[i]) for i, (a, b) in enumerate(zip(sources, held))]
    for fetch in fetches[1:] + fetches[:1]:
        fetch.start()
    width = heads * DK
    all_heads = heads * lax.axis_size("tp")
    tp_place = lax.axis_index("tp")
    small = row_sum(got_ref, 2 * width, LANES)
    small = small + pltpu.roll(small, NEW, 0)
    rstd = lax.rsqrt(small[:, 2 * all_heads : 2 * all_heads + 1] / D + epsilon)
    gates[...] = jnp.zeros(gates.shape, F32)
    factor = jnp.where(iota((SUBS, 1), 0) < NEW, DK ** (-0.5), 1.0)
    for h in range(heads):
        block = (row_sum(got_ref, h * DK, DK) * rstd).astype(BF16).astype(F32)
        norm = lax.rsqrt(jnp.sum(block * block, axis=1, keepdims=True) + epsilon)
        unit[h * SUBS : (h + 1) * SUBS, :] = block * norm * factor
        vals[h * SUBS : (h + 1) * SUBS, :] = (
            (row_sum(got_ref, width + h * DV, DV) * rstd).astype(BF16).astype(F32)
        )
    for fetch in fetches[1:]:
        fetch.wait()
    small = small * rstd
    alphas = pltpu.roll(small, LANES - tp_place * heads, 1)[:, :heads]
    betas = pltpu.roll(small, LANES - all_heads - tp_place * heads, 1)[:, :heads]
    x = alphas + bias_ref[...]
    soft = jnp.maximum(x, 0.0) + jnp.log1p(jnp.exp(-jnp.abs(x)))
    decay = -jnp.exp(log_ref[...]) * soft
    slot = iota(decay.shape, 0)
    live = (slot & 3) < own_ref[:, :heads]
    keep = jnp.exp(jnp.where(live, decay, 0.0))
    write = jnp.where(live, 1.0 / (1.0 + jnp.exp(-betas)), 0.0)
    gates[:SUBS, :heads] = jnp.where(slot < NEW, keep, write)
    turned = gates[...].T
    fetches[0].wait()
    for h in range(heads):
        own = slice(h * SUBS, (h + 1) * SUBS)
        preds[own, :] = jnp.dot(
            unit[own, :], memory_ref[h], precision=lax.Precision.HIGHEST, preferred_element_type=F32
        )

    def rows(ref, j):
        return ref[pl.ds(j, heads, stride=SUBS), :]

    queries = [rows(unit, t) for t in range(NEW)]
    keys = [rows(unit, NEW + t) for t in range(NEW)]
    keeps = [turned[:heads, t : t + 1] for t in range(NEW)]
    writes = [turned[:heads, NEW + t : NEW + t + 1] for t in range(NEW)]

    def inner(a, b):
        return jnp.sum(a * b, axis=1, keepdims=True)

    updates, outs = [], []
    passed = []
    total = jnp.ones((heads, 1), F32)
    for t in range(NEW):
        total = total * keeps[t]
        passed = [p * keeps[t] for p in passed]
        said = total * rows(preds, NEW + t)
        for i in range(t):
            said = said + (passed[i] * inner(keys[i], keys[t])) * updates[i]
        updates.append(writes[t] * (rows(vals, t) - said))
        passed.append(jnp.ones((heads, 1), F32))
        out = total * rows(preds, t)
        for i in range(t + 1):
            out = out + (passed[i] * inner(keys[i], queries[t])) * updates[i]
        outs.append(out)
    for i in range(NEW):
        late[pl.ds(i, heads, stride=SUBS), :] = jnp.zeros((heads, DV), F32)
        late[pl.ds(NEW + i, heads, stride=SUBS), :] = passed[i] * updates[i]
    left_ref[...] = jnp.broadcast_to(total, left_ref.shape)
    for t, out in enumerate(outs):
        out = out * lax.rsqrt(jnp.mean(out * out, axis=1, keepdims=True) + epsilon)
        gate = rows(vals, NEW + t)
        silu = gate * (1.0 / (1.0 + jnp.exp(-gate)))
        copies[t * heads : (t + 1) * heads, :] = out * gain_ref[...] * silu
    mixed = copies[...].astype(BF16)
    for d in range(mixed_out.shape[0]):
        mixed_out[d] = mixed


def advance_kernel(memory_ref, unit_ref, late_ref, left_ref, out_ref, fresh_ref, sems):
    stores = []
    for h in range(memory_ref.shape[0]):
        own = slice(h * SUBS, (h + 1) * SUBS)
        added = lax.dot_general(
            unit_ref[own, :],
            late_ref[own, :],
            (((0,), (0,)), ((), ())),
            precision=lax.Precision.HIGHEST,
            preferred_element_type=F32,
        )
        fresh_ref[h] = memory_ref[h] * left_ref[h : h + 1, :] + added
        stores.append(pltpu.make_async_copy(fresh_ref.at[h], out_ref.at[h], sems.at[h]))
        stores[-1].start()
    for store in stores:
        store.wait()


def project_kernel(place_ref, mixed_ref, w_ref, out_ref):
    heads = w_ref.shape[0] // DV
    total = mixed_ref.shape[0]
    packed = out_ref.shape[0]
    place = place_ref[...]
    head_of = iota((1, total), 1) & (heads - 1)
    row = iota((packed, total), 0)
    mixed = mixed_ref[...]
    rows = []
    for h in range(heads):
        pick = jnp.where(row == jnp.where(head_of == h, place, -1), 1.0, 0.0).astype(BF16)
        rows.append(dot(pick, mixed).astype(BF16))
    sum_ = None
    for h in range(heads):
        term = dot(rows[h], w_ref[h * DV : (h + 1) * DV, :])
        sum_ = term if sum_ is None else sum_ + term
    out_ref[...] = sum_


def picker(lengths_ref, packed, total_rows):
    col = iota((1, total_rows), 1)
    place = places(lengths_ref, lax.shift_right_logical(col, 2), col & 3)
    return jnp.where(iota((packed, total_rows), 0) == place, 1.0, 0.0).astype(BF16)


class Packing:
    def __init__(self, live, tiles, receivers, members):
        self.members = members
        self.tiles = tiles // members
        self.receivers = receivers // members
        self.shared = 0 < live % SUBS <= SUBS // 2
        self.whole = live // SUBS if self.shared else -(-live // SUBS)
        self.count = self.whole * self.tiles + (-(-self.tiles // 2) if self.shared else 0)
        self.each = -(-self.count // self.receivers)

    def spot(self, block, tile):
        at = block * self.tiles + (tile if block < self.whole else tile // 2)
        return divmod(at, self.each)


def up_kernel(packing, partner, inputs, *refs):
    *terms, base_ref, gain_ref, wg_ref, wu_ref = refs[:inputs]
    out_ref, hidden_out = refs[inputs:]
    packed = hidden_out.shape[0]
    first = 0
    if packing.members > 1:
        member = (lax.axis_index("kv") & (packing.members - 1)) ^ partner
        first = member * (packing.tiles * LANES)
    hidden = base_ref[...]
    for term in terms:
        hidden = hidden + term[...]
    hidden = hidden.astype(BF16)
    hidden_out[...] = hidden
    hidden_f = hidden.astype(F32)
    scaled = (hidden_f * gain_ref[...]).astype(BF16)
    tiles = packing.tiles
    squares = jnp.broadcast_to(jnp.sum(hidden_f * hidden_f, axis=1, keepdims=True), (packed, LANES))
    own_lane = iota(squares.shape, 0) == iota(squares.shape, 1)
    squares = jnp.sum(jnp.where(own_lane, squares, 0.0), axis=0, keepdims=True)
    squares = jnp.broadcast_to(squares, (SUBS, LANES))
    high = squares.astype(BF16).astype(F32)
    halves = jnp.where(iota(squares.shape, 0) < NEW, high, squares - high).astype(BF16)
    step = 4
    for start in range(0, tiles, step):
        stop = min(start + step, tiles)
        span = pl.ds(pl.multiple_of(first + start * LANES, LANES), (stop - start) * LANES)
        gate = dot(scaled, wg_ref[:, span])
        up = dot(scaled, wu_ref[:, span])
        for t in range(start, stop):
            lanes = slice((t - start) * LANES, (t - start + 1) * LANES)
            for b in range(packed // SUBS):
                rows = slice(b * SUBS, (b + 1) * SUBS)
                one, two = gate[rows, lanes], up[rows, lanes]
                if b == packing.whole:
                    if t % 2 == 0 and t + 1 < tiles:
                        held = one, two
                        continue
                    if t % 2:
                        one = held[0] + pltpu.roll(one, SUBS // 2, 0)
                        two = held[1] + pltpu.roll(two, SUBS // 2, 0)
                d, i = packing.spot(b, t)
                out_ref[d, i * 16 : i * 16 + 16, :] = jnp.concatenate([one, two], axis=0).astype(BF16)
    for at in range(packing.count, out_ref.shape[0] * packing.each):
        d, i = divmod(at, packing.each)
        out_ref[d, i * 16 : i * 16 + 16, :] = jnp.zeros((16, LANES), BF16)
    for d in range(out_ref.shape[0]):
        out_ref[d, packing.each * 16 :, :] = halves


def active_kernel(packing, *refs):
    *got, out_ref = refs
    end = packing.each * 16
    squares = block_sum(got, slice(end, end + SUBS), slice(None))
    squares = squares + pltpu.roll(squares, SUBS // 2, 0)
    rstd = lax.rsqrt(squares / D + epsilon)
    row, lane = iota(rstd.shape, 0), iota(rstd.shape, 1)
    first = lax.shift_right_logical(lax.axis_index("kv"), log2(packing.members)) * packing.each
    for i in range(packing.each):
        block = lax.div(first + i, packing.tiles)
        row_of = block * SUBS + row
        if packing.shared:
            row_of = jnp.where(block >= packing.whole, packing.whole * SUBS + (row & (SUBS // 2 - 1)), row_of)
        scale = jnp.sum(jnp.where(lane == row_of, rstd, 0.0), axis=1, keepdims=True)
        pair = block_sum(got, slice(i * 16, i * 16 + 16), slice(None))
        gate, up = pair[:SUBS] * scale, pair[SUBS:] * scale
        active = (gate * (1.0 / (1.0 + jnp.exp(-gate))) * up).astype(BF16)
        for d in range(out_ref.shape[0]):
            out_ref[d, i * SUBS : (i + 1) * SUBS, :] = active


def down_kernel(packing, got_ref, w_ref, out_ref):
    packed = out_ref.shape[0]
    tiles = w_ref.shape[0] // LANES
    sum_ = None
    for t in range(tiles):
        parts = []
        for b in range(packed // SUBS):
            member, tile = divmod(t, packing.tiles)
            receiver, i = packing.spot(b, tile)
            d = receiver * packing.members + member
            part = got_ref[d, i * SUBS : (i + 1) * SUBS, :].astype(F32)
            parts.append(pltpu.roll(part, SUBS // 2, 0) if b == packing.whole and tile % 2 else part)
        term = dot(jnp.concatenate(parts, axis=0).astype(BF16), w_ref[t * LANES : (t + 1) * LANES, :])
        sum_ = term if sum_ is None else sum_ + term
    out_ref[...] = sum_


def last_kernel(*refs):
    *terms, hidden_ref, pick_ref, out_ref = refs
    result = terms[0][...]
    for term in terms[1:]:
        result = result + term[...]
    result = (hidden_ref[...].astype(F32) + result).astype(BF16)
    out_ref[...] = dot(pick_ref[...], result).astype(BF16)


def exchange(blocks):
    return lax.all_to_all(blocks, "kv", 0, 0)


def over_tp(terms):
    if lax.axis_size("tp") == 2:
        return [terms, lax.ppermute(terms, "tp", [(0, 1), (1, 0)])]
    return [lax.psum(terms, "tp")]


def per_device(
    tokens,
    lengths,
    memory,
    norm_gain,
    w_query,
    w_key,
    w_value,
    w_outgate,
    w_alpha,
    w_beta,
    decay_log,
    decay_bias,
    head_gain,
    w_output,
    mlp_gain,
    w_gate,
    w_up,
    w_down,
):
    total_rows, own_width = tokens.shape
    kv = lax.axis_size("kv")
    seq_dev, heads = memory.shape[:2]
    assert seq_dev == 1
    width = heads * DK
    sequences = lengths.shape[0]
    units = w_gate.shape[1]
    live = sequences * 7 // 4
    packed = -(-live // SUBS) * SUBS
    assert packed <= LANES
    packing = Packing(live, units // LANES, kv, PLANE if staged() else 1)
    assert units % (packing.members * LANES) == 0
    columns = 2 * width + LANES

    operands = [lengths, tokens, norm_gain[None], w_alpha.T, w_beta.T, w_query, w_key, w_value, w_outgate]
    *sent, base, pick, place, own = call(
        functools.partial(front_kernel, heads),
        [
            *dealt((SUBS, columns), kv),
            shape((packed, own_width), F32),
            shape((total_rows, packed), BF16),
            shape((1, kv * NEW * heads), jnp.int32),
            shape((SUBS, LANES), jnp.int32),
        ],
        operands,
        [HBM] * len(operands),
        16,
        4 * total_rows * own_width * 4 * width,
        "front",
        [pltpu.SMEM(lengths.shape, jnp.int32), *(room(x) for x in operands[1:]), pltpu.SemaphoreType.DMA((len(operands),)), pltpu.VMEM((kv, SUBS, columns), BF16)],
    )
    got, _ = reduce_scatter(sent, "fold_rows", slice(None), slice(2 * width, columns), 0, NEW)
    sent, unit, late, left = call(
        recur_kernel,
        [
            shape((kv, NEW * heads, DV), BF16),
            shape((heads * SUBS, DK), F32),
            shape((heads * SUBS, DV), F32),
            shape((heads, DV), F32),
        ],
        [own, *got, memory[0], decay_log[None], decay_bias[None], head_gain[None]],
        [VMEM] * (1 + len(got)) + [HBM] * 4,
        16,
        4 << 30,
        "recur",
        [
            pltpu.VMEM((LANES, LANES), F32),
            pltpu.VMEM((heads * SUBS, DV), F32),
            pltpu.VMEM((heads * SUBS, DV), F32),
            pltpu.VMEM((NEW * heads, DV), F32),
            pltpu.VMEM((heads, DK, DV), F32),
            pltpu.VMEM((1, heads), F32),
            pltpu.VMEM((1, heads), F32),
            pltpu.VMEM((1, DV), F32),
            pltpu.SemaphoreType.DMA((4,)),
        ],
    )
    (new_memory,) = call(
        advance_kernel,
        [shape((heads, DK, DV), F32)],
        [memory[0], unit, late, left],
        [VMEM] * 4,
        8,
        1 << 30,
        "advance",
        [pltpu.VMEM((heads, DK, DV), F32), pltpu.SemaphoreType.DMA((heads,))],
        [HBM],
    )
    got = exchange(sent).reshape(kv * NEW * heads, DV)
    (attn,) = call(
        project_kernel,
        [shape((packed, own_width), F32)],
        [place, got, w_output],
        [VMEM] * 3,
        8,
        32 << 20,
        "project",
    )
    terms = over_tp(attn)
    outs = [
        shape((packing.receivers, packing.each * 16 + SUBS, LANES), BF16),
        shape((packed, own_width), BF16),
    ]
    sent = []
    for d in range(packing.members):
        part, hidden = call(
            functools.partial(up_kernel, packing, d, len(terms) + 4),
            outs,
            [*terms, base, mlp_gain[None], w_gate, w_up],
            [VMEM] * (len(terms) + 4),
            16,
            4 * packed * own_width * units // packing.members,
            f"up_{d}",
        )
        sent.append(part)
    got, new_memory = reduce_scatter(
        sent, "fold_units", slice(packing.each * 16, None), slice(None), 0, NEW, order=(1, 2, 3), beside=new_memory
    )
    (sent,) = call(
        functools.partial(active_kernel, packing),
        [shape((kv, packing.each * SUBS, LANES), BF16)],
        got,
        [VMEM] * len(got),
        8,
        1 << 20,
        "active",
    )
    got = exchange(sent)
    (feed,) = call(
        functools.partial(down_kernel, packing),
        [shape((packed, own_width), F32)],
        [got, w_down],
        [VMEM] * 2,
        16,
        2 * packed * own_width * units,
        "down",
    )
    terms = over_tp(feed)
    (layer_out,) = call(
        last_kernel,
        [shape((total_rows, own_width), BF16)],
        [*terms, hidden, pick],
        [VMEM] * (len(terms) + 2),
        8,
        1 << 20,
        "last",
    )
    return (layer_out, new_memory[None])


def solution(mesh):
    placed = (
        P(None, "kv"),
        P(),
        P("kv", "tp", None, None),
        P("kv"),
        P("kv", "tp"),
        P("kv", "tp"),
        P("kv", "tp"),
        P("kv", "tp"),
        P("kv", None),
        P("kv", None),
        P("tp"),
        P("tp"),
        P(),
        P("tp", "kv"),
        P("kv"),
        P("kv", "tp"),
        P("kv", "tp"),
        P("tp", "kv"),
    )
    return jax.shard_map(
        per_device,
        mesh=mesh,
        in_specs=placed,
        out_specs=(P(None, "kv"), P("kv", "tp", None, None)),
        check_vma=False,
    )
```

```python
import functools

import jax
import jax.numpy as jnp
from jax import lax
from jax.experimental import pallas as pl
from jax.experimental.pallas import tpu as pltpu
from jax.sharding import PartitionSpec as P

D = 4096
DK = 128
DV = 128
NEW = 4
LANES = 128
PLANE = 4
SUBS = 8

epsilon = 1e-06


F32 = jnp.float32
BF16 = jnp.bfloat16
VMEM = pl.BlockSpec(memory_space=pltpu.VMEM)
HBM = pl.BlockSpec(memory_space=pltpu.HBM)


def call(body, outs, ins, specs, limit, flops, name, scratch=(), out_specs=None):
    moved = sum(x.size * x.dtype.itemsize for x in (*outs, *ins))
    ins = [pltpu.with_memory_space_constraint(x, pltpu.HBM) if s is HBM else x for x, s in zip(ins, specs)]
    return pl.pallas_call(
        body,
        out_shape=outs,
        in_specs=specs,
        out_specs=out_specs or [VMEM] * len(outs),
        scratch_shapes=list(scratch),
        compiler_params=pltpu.CompilerParams(vmem_limit_bytes=limit << 20),
        cost_estimate=pl.CostEstimate(flops=flops, bytes_accessed=moved, transcendentals=0),
        name=name,
    )(*ins)


def room(x):
    return pltpu.VMEM(x.shape, x.dtype)


def shape(dims, dtype):
    return jax.ShapeDtypeStruct(dims, dtype)


def iota(dims, axis):
    return lax.broadcasted_iota(jnp.int32, dims, axis)


def dot(a, b):
    return jnp.dot(a, b, preferred_element_type=F32)


def dot_nt(a, b):
    return lax.dot_general(a, b, (((1,), (1,)), ((), ())), preferred_element_type=F32)


def places(lengths_ref, sequence_of, slot_of):
    place = jnp.full(sequence_of.shape, -1, jnp.int32)
    start = 0
    for s in range(lengths_ref.shape[0]):
        held = lengths_ref[s]
        mine = (sequence_of == s) & (slot_of < held)
        place = jnp.where(mine, slot_of + start, place)
        start = start + held
    return place


def log2(n):
    assert n & (n - 1) == 0
    return n.bit_length() - 1


def front_kernel(heads, *refs):
    count = 9
    sources, refs = refs[:count], refs[count:]
    *outs, base_ref, pick_ref, place_ref, own_ref = refs[: -count - 2]
    *held, sems, out_ref = refs[-count - 2 :]
    copies = [pltpu.make_async_copy(a, b, sems.at[i]) for i, (a, b) in enumerate(zip(sources, held))]
    for copy in copies:
        copy.start()
    lengths_ref, tokens_ref, gain_ref, wa_ref, wb_ref, wq_ref, wk_ref, wv_ref, wg_ref = held
    total_rows = tokens_ref.shape[0]
    width = wq_ref.shape[1]
    all_heads = wa_ref.shape[0]
    packed = pick_ref.shape[1]
    copies[0].wait()
    own_ref[...] = jnp.full(own_ref.shape, lengths_ref[lax.axis_index("kv")], jnp.int32)
    col = iota(place_ref.shape, 1)
    place_ref[...] = places(
        lengths_ref,
        lax.shift_right_logical(col, log2(NEW * heads)),
        lax.shift_right_logical(col, log2(heads)) & 3,
    )
    pick = picker(lengths_ref, packed, total_rows)
    pick_ref[...] = pick.astype(F32).T.astype(BF16)
    dims = (2 * total_rows, total_rows)
    row, col = iota(dims, 0), iota(dims, 1)
    target = lax.shift_left(lax.shift_right_logical(row, 3), 2) + (row & 3)
    hit = target == col
    upper = (row & 7) < NEW
    zero, one = jnp.zeros(dims, F32), jnp.ones(dims, F32)
    place_a = jnp.where(hit & upper, one, zero).astype(BF16)
    place_b = jnp.where(hit & ~upper, one, zero).astype(BF16)
    fill = jnp.zeros((LANES - 2 * all_heads, wa_ref.shape[1]), BF16)
    for copy in copies[1:5]:
        copy.wait()
    tokens = tokens_ref[...]
    base_ref[...] = dot(pick, tokens)
    scaled = (tokens.astype(F32) * gain_ref[...]).astype(BF16)
    left = dot(place_a, scaled).astype(BF16)
    right = dot(place_b, scaled).astype(BF16)
    both = dot(place_a + place_b, tokens)
    squares = jnp.sum(both * both, axis=1, keepdims=True)
    small = dot_nt(left + right, jnp.concatenate([wa_ref[...], wb_ref[...], fill], axis=0))
    lane = iota(small.shape, 1)
    small = jnp.where(lane == 2 * all_heads, jnp.broadcast_to(squares, small.shape), small)
    high = small.astype(BF16).astype(F32)
    first = (iota(small.shape, 0) & 7) < NEW

    def put(columns, values):
        out_ref[:, :, columns] = values.reshape(-1, SUBS, values.shape[1]).astype(BF16)

    put(slice(2 * width, 2 * width + LANES), jnp.where(first, high, small - high))
    copies[5].wait()
    copies[6].wait()
    put(slice(0, width), dot(left, wq_ref[...]) + dot(right, wk_ref[...]))
    copies[7].wait()
    copies[8].wait()
    put(slice(width, 2 * width), dot(left, wv_ref[...]) + dot(right, wg_ref[...]))
    deal(out_ref, outs)


def deal(blocks_ref, outs):
    if len(outs) == 1:
        outs[0][...] = blocks_ref[...]
        return
    plane = lax.axis_index("kv") & (PLANE - 1)
    for d, out in enumerate(outs):
        for z in range(out.shape[0]):
            out[z] = blocks_ref[z * PLANE + (plane ^ d)]


def fold_kernel(rows, columns, axis, half, *refs):
    parts, outs = refs[:PLANE], refs[PLANE:]
    high = lax.shift_right_logical(lax.axis_index("kv"), log2(PLANE))
    for e, out in enumerate(outs):
        total = parts[0][high ^ e].astype(F32)
        for part in parts[1:]:
            total = total + part[high ^ e].astype(F32)
        out[...] = total.astype(out.dtype)
        value = total[rows, columns]
        value = value + pltpu.roll(value, half, axis)
        top = value.astype(BF16).astype(F32)
        value = jnp.where(iota(value.shape, axis) < half, top, value - top)
        out[rows, columns] = value.astype(out.dtype)


def partners(values, shift):
    count = lax.axis_size("kv")
    moved = []
    for d in reversed(range(1, len(values))):
        moved.append(lax.ppermute(values[d], "kv", [(i, i ^ (d << shift)) for i in range(count)]))
    return [values[0], *moved]


def staged():
    return lax.axis_size("kv") == PLANE * PLANE


def dealt(dims, kv):
    if staged():
        return [shape((PLANE, *dims), BF16)] * PLANE
    return [shape((kv, *dims), BF16)]


def reduce_scatter(outs, name, *halves, beside=None):
    if not staged():
        return [exchange(outs[0])], beside
    dims = outs[0].shape[1:]
    parts = partners(outs, 0)
    if beside is not None:
        parts, beside = lax.optimization_barrier((parts, beside))
    sums = call(
        functools.partial(fold_kernel, *halves),
        [shape(dims, F32 if e == 0 else BF16) for e in range(PLANE)],
        parts,
        [VMEM] * PLANE,
        8,
        1 << 20,
        name,
    )
    return [x[None] for x in partners(sums, log2(PLANE))], beside


def block_sum(refs, rows, columns):
    total = None
    for ref in refs:
        for i in range(ref.shape[0]):
            term = ref[i, rows, columns].astype(F32)
            total = term if total is None else total + term
    return total


def row_sum(refs, start, columns):
    return block_sum(refs, slice(None), slice(start, start + columns))


def recur_kernel(*refs):
    own_ref, *got_ref = refs[:-17]
    sources, (mixed_out, unit, late, left_ref) = refs[-17:-13], refs[-13:-9]
    gates, vals, preds, copies, *held, sems = refs[-9:]
    memory_ref, log_ref, bias_ref, gain_ref = held
    heads = memory_ref.shape[0]
    fetches = [pltpu.make_async_copy(a, b, sems.at[i]) for i, (a, b) in enumerate(zip(sources, held))]
    for fetch in fetches[1:] + fetches[:1]:
        fetch.start()
    width = heads * DK
    all_heads = heads * lax.axis_size("tp")
    tp_place = lax.axis_index("tp")
    small = row_sum(got_ref, 2 * width, LANES)
    small = small + pltpu.roll(small, NEW, 0)
    rstd = lax.rsqrt(small[:, 2 * all_heads : 2 * all_heads + 1] / D + epsilon)
    gates[...] = jnp.zeros(gates.shape, F32)
    factor = jnp.where(iota((SUBS, 1), 0) < NEW, DK ** (-0.5), 1.0)
    for h in range(heads):
        block = (row_sum(got_ref, h * DK, DK) * rstd).astype(BF16).astype(F32)
        norm = lax.rsqrt(jnp.sum(block * block, axis=1, keepdims=True) + epsilon)
        unit[h * SUBS : (h + 1) * SUBS, :] = block * norm * factor
        vals[h * SUBS : (h + 1) * SUBS, :] = (
            (row_sum(got_ref, width + h * DV, DV) * rstd).astype(BF16).astype(F32)
        )
    for fetch in fetches[1:]:
        fetch.wait()
    small = small * rstd
    alphas = pltpu.roll(small, LANES - tp_place * heads, 1)[:, :heads]
    betas = pltpu.roll(small, LANES - all_heads - tp_place * heads, 1)[:, :heads]
    x = alphas + bias_ref[...]
    soft = jnp.maximum(x, 0.0) + jnp.log1p(jnp.exp(-jnp.abs(x)))
    decay = -jnp.exp(log_ref[...]) * soft
    slot = iota(decay.shape, 0)
    live = (slot & 3) < own_ref[:, :heads]
    keep = jnp.exp(jnp.where(live, decay, 0.0))
    write = jnp.where(live, 1.0 / (1.0 + jnp.exp(-betas)), 0.0)
    gates[:SUBS, :heads] = jnp.where(slot < NEW, keep, write)
    turned = gates[...].T
    fetches[0].wait()
    for h in range(heads):
        own = slice(h * SUBS, (h + 1) * SUBS)
        preds[own, :] = jnp.dot(
            unit[own, :], memory_ref[h], precision=lax.Precision.HIGHEST, preferred_element_type=F32
        )

    def rows(ref, j):
        return ref[pl.ds(j, heads, stride=SUBS), :]

    queries = [rows(unit, t) for t in range(NEW)]
    keys = [rows(unit, NEW + t) for t in range(NEW)]
    keeps = [turned[:heads, t : t + 1] for t in range(NEW)]
    writes = [turned[:heads, NEW + t : NEW + t + 1] for t in range(NEW)]

    def inner(a, b):
        return jnp.sum(a * b, axis=1, keepdims=True)

    updates, outs = [], []
    passed = []
    total = jnp.ones((heads, 1), F32)
    for t in range(NEW):
        total = total * keeps[t]
        passed = [p * keeps[t] for p in passed]
        said = total * rows(preds, NEW + t)
        for i in range(t):
            said = said + (passed[i] * inner(keys[i], keys[t])) * updates[i]
        updates.append(writes[t] * (rows(vals, t) - said))
        passed.append(jnp.ones((heads, 1), F32))
        out = total * rows(preds, t)
        for i in range(t + 1):
            out = out + (passed[i] * inner(keys[i], queries[t])) * updates[i]
        outs.append(out)
    for i in range(NEW):
        late[pl.ds(i, heads, stride=SUBS), :] = jnp.zeros((heads, DV), F32)
        late[pl.ds(NEW + i, heads, stride=SUBS), :] = passed[i] * updates[i]
    left_ref[...] = jnp.broadcast_to(total, left_ref.shape)
    for t, out in enumerate(outs):
        out = out * lax.rsqrt(jnp.mean(out * out, axis=1, keepdims=True) + epsilon)
        gate = rows(vals, NEW + t)
        silu = gate * (1.0 / (1.0 + jnp.exp(-gate)))
        copies[t * heads : (t + 1) * heads, :] = out * gain_ref[...] * silu
    mixed = copies[...].astype(BF16)
    for d in range(mixed_out.shape[0]):
        mixed_out[d] = mixed


def advance_kernel(memory_ref, unit_ref, late_ref, left_ref, out_ref, fresh_ref, sems):
    stores = []
    for h in range(memory_ref.shape[0]):
        own = slice(h * SUBS, (h + 1) * SUBS)
        added = lax.dot_general(
            unit_ref[own, :],
            late_ref[own, :],
            (((0,), (0,)), ((), ())),
            precision=lax.Precision.HIGHEST,
            preferred_element_type=F32,
        )
        fresh_ref[h] = memory_ref[h] * left_ref[h : h + 1, :] + added
        stores.append(pltpu.make_async_copy(fresh_ref.at[h], out_ref.at[h], sems.at[h]))
        stores[-1].start()
    for store in stores:
        store.wait()


def project_kernel(place_ref, mixed_ref, w_ref, out_ref):
    heads = w_ref.shape[0] // DV
    total = mixed_ref.shape[0]
    packed = out_ref.shape[0]
    place = place_ref[...]
    head_of = iota((1, total), 1) & (heads - 1)
    row = iota((packed, total), 0)
    mixed = mixed_ref[...]
    rows = []
    for h in range(heads):
        pick = jnp.where(row == jnp.where(head_of == h, place, -1), 1.0, 0.0).astype(BF16)
        rows.append(dot(pick, mixed).astype(BF16))
    sum_ = None
    for h in range(heads):
        term = dot(rows[h], w_ref[h * DV : (h + 1) * DV, :])
        sum_ = term if sum_ is None else sum_ + term
    out_ref[...] = sum_


def picker(lengths_ref, packed, total_rows):
    col = iota((1, total_rows), 1)
    place = places(lengths_ref, lax.shift_right_logical(col, 2), col & 3)
    return jnp.where(iota((packed, total_rows), 0) == place, 1.0, 0.0).astype(BF16)


class Packing:
    def __init__(self, live, tiles, receivers, members):
        self.members = members
        self.tiles = tiles // members
        self.receivers = receivers // members
        self.shared = 0 < live % SUBS <= SUBS // 2
        self.whole = live // SUBS if self.shared else -(-live // SUBS)
        self.count = self.whole * self.tiles + (-(-self.tiles // 2) if self.shared else 0)
        self.each = -(-self.count // self.receivers)

    def spot(self, block, tile):
        at = block * self.tiles + (tile if block < self.whole else tile // 2)
        return divmod(at, self.each)


def up_kernel(packing, partner, inputs, *refs):
    *terms, base_ref, gain_ref, wg_ref, wu_ref = refs[:inputs]
    out_ref, *hidden_out = refs[inputs:]
    packed = base_ref.shape[0]
    first = 0
    if packing.members > 1:
        member = (lax.axis_index("kv") & (packing.members - 1)) ^ partner
        first = member * (packing.tiles * LANES)
    hidden = base_ref[...]
    for term in terms:
        hidden = hidden + term[...]
    hidden = hidden.astype(BF16)
    for out in hidden_out:
        out[...] = hidden
    hidden_f = hidden.astype(F32)
    scaled = (hidden_f * gain_ref[...]).astype(BF16)
    tiles = packing.tiles
    squares = jnp.broadcast_to(jnp.sum(hidden_f * hidden_f, axis=1, keepdims=True), (packed, LANES))
    own_lane = iota(squares.shape, 0) == iota(squares.shape, 1)
    squares = jnp.sum(jnp.where(own_lane, squares, 0.0), axis=0, keepdims=True)
    squares = jnp.broadcast_to(squares, (SUBS, LANES))
    high = squares.astype(BF16).astype(F32)
    halves = jnp.where(iota(squares.shape, 0) < NEW, high, squares - high).astype(BF16)
    step = 4
    for start in range(0, tiles, step):
        stop = min(start + step, tiles)
        span = pl.ds(pl.multiple_of(first + start * LANES, LANES), (stop - start) * LANES)
        gate = dot(scaled, wg_ref[:, span])
        up = dot(scaled, wu_ref[:, span])
        for t in range(start, stop):
            lanes = slice((t - start) * LANES, (t - start + 1) * LANES)
            for b in range(packed // SUBS):
                rows = slice(b * SUBS, (b + 1) * SUBS)
                one, two = gate[rows, lanes], up[rows, lanes]
                if b == packing.whole:
                    if t % 2 == 0 and t + 1 < tiles:
                        held = one, two
                        continue
                    if t % 2:
                        one = held[0] + pltpu.roll(one, SUBS // 2, 0)
                        two = held[1] + pltpu.roll(two, SUBS // 2, 0)
                d, i = packing.spot(b, t)
                out_ref[d, i * 16 : i * 16 + 16, :] = jnp.concatenate([one, two], axis=0).astype(BF16)
    for at in range(packing.count, out_ref.shape[0] * packing.each):
        d, i = divmod(at, packing.each)
        out_ref[d, i * 16 : i * 16 + 16, :] = jnp.zeros((16, LANES), BF16)
    for d in range(out_ref.shape[0]):
        out_ref[d, packing.each * 16 :, :] = halves


def active_kernel(packing, *refs):
    *got, out_ref = refs
    end = packing.each * 16
    squares = block_sum(got, slice(end, end + SUBS), slice(None))
    squares = squares + pltpu.roll(squares, SUBS // 2, 0)
    rstd = lax.rsqrt(squares / D + epsilon)
    row, lane = iota(rstd.shape, 0), iota(rstd.shape, 1)
    first = lax.shift_right_logical(lax.axis_index("kv"), log2(packing.members)) * packing.each
    for i in range(packing.each):
        block = lax.div(first + i, packing.tiles)
        row_of = block * SUBS + row
        if packing.shared:
            row_of = jnp.where(block >= packing.whole, packing.whole * SUBS + (row & (SUBS // 2 - 1)), row_of)
        scale = jnp.sum(jnp.where(lane == row_of, rstd, 0.0), axis=1, keepdims=True)
        pair = block_sum(got, slice(i * 16, i * 16 + 16), slice(None))
        gate, up = pair[:SUBS] * scale, pair[SUBS:] * scale
        active = (gate * (1.0 / (1.0 + jnp.exp(-gate))) * up).astype(BF16)
        for d in range(out_ref.shape[0]):
            out_ref[d, i * SUBS : (i + 1) * SUBS, :] = active


def down_kernel(packing, got_ref, w_ref, out_ref):
    packed = out_ref.shape[0]
    tiles = w_ref.shape[0] // LANES
    sum_ = None
    for t in range(tiles):
        parts = []
        for b in range(packed // SUBS):
            member, tile = divmod(t, packing.tiles)
            receiver, i = packing.spot(b, tile)
            d = receiver * packing.members + member
            part = got_ref[d, i * SUBS : (i + 1) * SUBS, :].astype(F32)
            parts.append(pltpu.roll(part, SUBS // 2, 0) if b == packing.whole and tile % 2 else part)
        term = dot(jnp.concatenate(parts, axis=0).astype(BF16), w_ref[t * LANES : (t + 1) * LANES, :])
        sum_ = term if sum_ is None else sum_ + term
    out_ref[...] = sum_


def last_kernel(*refs):
    *terms, hidden_ref, pick_ref, out_ref = refs
    result = terms[0][...]
    for term in terms[1:]:
        result = result + term[...]
    result = (hidden_ref[...].astype(F32) + result).astype(BF16)
    out_ref[...] = dot(pick_ref[...], result).astype(BF16)


def exchange(blocks):
    return lax.all_to_all(blocks, "kv", 0, 0)


def over_tp(terms):
    if lax.axis_size("tp") == 2:
        return [terms, lax.ppermute(terms, "tp", [(0, 1), (1, 0)])]
    return [lax.psum(terms, "tp")]


def per_device(
    tokens,
    lengths,
    memory,
    norm_gain,
    w_query,
    w_key,
    w_value,
    w_outgate,
    w_alpha,
    w_beta,
    decay_log,
    decay_bias,
    head_gain,
    w_output,
    mlp_gain,
    w_gate,
    w_up,
    w_down,
):
    total_rows, own_width = tokens.shape
    kv = lax.axis_size("kv")
    seq_dev, heads = memory.shape[:2]
    assert seq_dev == 1
    width = heads * DK
    sequences = lengths.shape[0]
    units = w_gate.shape[1]
    live = sequences * 7 // 4
    packed = -(-live // SUBS) * SUBS
    assert packed <= LANES
    packing = Packing(live, units // LANES, kv, PLANE if staged() else 1)
    assert units % (packing.members * LANES) == 0
    columns = 2 * width + LANES

    operands = [lengths, tokens, norm_gain[None], w_alpha.T, w_beta.T, w_query, w_key, w_value, w_outgate]
    *sent, base, pick, place, own = call(
        functools.partial(front_kernel, heads),
        [
            *dealt((SUBS, columns), kv),
            shape((packed, own_width), F32),
            shape((total_rows, packed), BF16),
            shape((1, kv * NEW * heads), jnp.int32),
            shape((SUBS, LANES), jnp.int32),
        ],
        operands,
        [HBM] * len(operands),
        16,
        4 * total_rows * own_width * 4 * width,
        "front",
        [pltpu.SMEM(lengths.shape, jnp.int32), *(room(x) for x in operands[1:]), pltpu.SemaphoreType.DMA((len(operands),)), pltpu.VMEM((kv, SUBS, columns), BF16)],
    )
    got, _ = reduce_scatter(sent, "fold_rows", slice(None), slice(2 * width, columns), 0, NEW)
    sent, unit, late, left = call(
        recur_kernel,
        [
            shape((kv, NEW * heads, DV), BF16),
            shape((heads * SUBS, DK), F32),
            shape((heads * SUBS, DV), F32),
            shape((heads, DV), F32),
        ],
        [own, *got, memory[0], decay_log[None], decay_bias[None], head_gain[None]],
        [VMEM] * (1 + len(got)) + [HBM] * 4,
        16,
        4 << 30,
        "recur",
        [
            pltpu.VMEM((LANES, LANES), F32),
            pltpu.VMEM((heads * SUBS, DV), F32),
            pltpu.VMEM((heads * SUBS, DV), F32),
            pltpu.VMEM((NEW * heads, DV), F32),
            pltpu.VMEM((heads, DK, DV), F32),
            pltpu.VMEM((1, heads), F32),
            pltpu.VMEM((1, heads), F32),
            pltpu.VMEM((1, DV), F32),
            pltpu.SemaphoreType.DMA((4,)),
        ],
    )
    (new_memory,) = call(
        advance_kernel,
        [shape((heads, DK, DV), F32)],
        [memory[0], unit, late, left],
        [VMEM] * 4,
        8,
        1 << 30,
        "advance",
        [pltpu.VMEM((heads, DK, DV), F32), pltpu.SemaphoreType.DMA((heads,))],
        [HBM],
    )
    got = exchange(sent).reshape(kv * NEW * heads, DV)
    (attn,) = call(
        project_kernel,
        [shape((packed, own_width), F32)],
        [place, got, w_output],
        [VMEM] * 3,
        8,
        32 << 20,
        "project",
    )
    terms = over_tp(attn)
    outs = [
        shape((packing.receivers, packing.each * 16 + SUBS, LANES), BF16),
        shape((packed, own_width), BF16),
    ]
    sent = []
    for d in reversed(range(packing.members)):
        part, *hidden = call(
            functools.partial(up_kernel, packing, d, len(terms) + 4),
            outs if d == 0 else outs[:1],
            [*terms, base, mlp_gain[None], w_gate, w_up],
            [VMEM] * (len(terms) + 4),
            16,
            4 * packed * own_width * units // packing.members,
            f"up_{d}",
        )
        sent.insert(0, part)
    got, new_memory = reduce_scatter(
        sent, "fold_units", slice(packing.each * 16, None), slice(None), 0, NEW, beside=new_memory
    )
    (sent,) = call(
        functools.partial(active_kernel, packing),
        [shape((kv, packing.each * SUBS, LANES), BF16)],
        got,
        [VMEM] * len(got),
        8,
        1 << 20,
        "active",
    )
    got = exchange(sent)
    (feed,) = call(
        functools.partial(down_kernel, packing),
        [shape((packed, own_width), F32)],
        [got, w_down],
        [VMEM] * 2,
        16,
        2 * packed * own_width * units,
        "down",
    )
    terms = over_tp(feed)
    (layer_out,) = call(
        last_kernel,
        [shape((total_rows, own_width), BF16)],
        [*terms, *hidden, pick],
        [VMEM] * (len(terms) + 2),
        8,
        1 << 20,
        "last",
    )
    return (layer_out, new_memory[None])


def solution(mesh):
    placed = (
        P(None, "kv"),
        P(),
        P("kv", "tp", None, None),
        P("kv"),
        P("kv", "tp"),
        P("kv", "tp"),
        P("kv", "tp"),
        P("kv", "tp"),
        P("kv", None),
        P("kv", None),
        P("tp"),
        P("tp"),
        P(),
        P("tp", "kv"),
        P("kv"),
        P("kv", "tp"),
        P("kv", "tp"),
        P("tp", "kv"),
    )
    return jax.shard_map(
        per_device,
        mesh=mesh,
        in_specs=placed,
        out_specs=(P(None, "kv"), P("kv", "tp", None, None)),
        check_vma=False,
    )
```

```python
import functools

import jax
import jax.numpy as jnp
from jax import lax
from jax.experimental import pallas as pl
from jax.experimental.pallas import tpu as pltpu
from jax.sharding import PartitionSpec as P

D = 4096
DK = 128
DV = 128
NEW = 4
LANES = 128
PLANE = 4
SUBS = 8

epsilon = 1e-06


F32 = jnp.float32
BF16 = jnp.bfloat16
VMEM = pl.BlockSpec(memory_space=pltpu.VMEM)
HBM = pl.BlockSpec(memory_space=pltpu.HBM)


def call(body, outs, ins, specs, limit, flops, name, scratch=(), out_specs=None):
    moved = sum(x.size * x.dtype.itemsize for x in (*outs, *ins))
    ins = [pltpu.with_memory_space_constraint(x, pltpu.HBM) if s is HBM else x for x, s in zip(ins, specs)]
    return pl.pallas_call(
        body,
        out_shape=outs,
        in_specs=specs,
        out_specs=out_specs or [VMEM] * len(outs),
        scratch_shapes=list(scratch),
        compiler_params=pltpu.CompilerParams(vmem_limit_bytes=limit << 20),
        cost_estimate=pl.CostEstimate(flops=flops, bytes_accessed=moved, transcendentals=0),
        name=name,
    )(*ins)


def room(x):
    return pltpu.VMEM(x.shape, x.dtype)


def shape(dims, dtype):
    return jax.ShapeDtypeStruct(dims, dtype)


def iota(dims, axis):
    return lax.broadcasted_iota(jnp.int32, dims, axis)


def dot(a, b):
    return jnp.dot(a, b, preferred_element_type=F32)


def dot_nt(a, b):
    return lax.dot_general(a, b, (((1,), (1,)), ((), ())), preferred_element_type=F32)


def places(lengths_ref, sequence_of, slot_of):
    place = jnp.full(sequence_of.shape, -1, jnp.int32)
    start = 0
    for s in range(lengths_ref.shape[0]):
        held = lengths_ref[s]
        mine = (sequence_of == s) & (slot_of < held)
        place = jnp.where(mine, slot_of + start, place)
        start = start + held
    return place


def log2(n):
    assert n & (n - 1) == 0
    return n.bit_length() - 1


def front_kernel(heads, *refs):
    count = 9
    sources, refs = refs[:count], refs[count:]
    *outs, base_ref, pick_ref, place_ref, own_ref = refs[: -count - 2]
    *held, sems, out_ref = refs[-count - 2 :]
    copies = [pltpu.make_async_copy(a, b, sems.at[i]) for i, (a, b) in enumerate(zip(sources, held))]
    for copy in copies:
        copy.start()
    lengths_ref, tokens_ref, gain_ref, wa_ref, wb_ref, wq_ref, wk_ref, wv_ref, wg_ref = held
    total_rows = tokens_ref.shape[0]
    width = wq_ref.shape[1]
    all_heads = wa_ref.shape[0]
    packed = pick_ref.shape[0]
    copies[0].wait()
    own_ref[...] = jnp.full(own_ref.shape, lengths_ref[lax.axis_index("kv")], jnp.int32)
    col = iota(place_ref.shape, 1)
    place_ref[...] = places(
        lengths_ref,
        lax.shift_right_logical(col, log2(NEW * heads)),
        lax.shift_right_logical(col, log2(heads)) & 3,
    )
    pick = picker(lengths_ref, packed, total_rows)
    pick_ref[...] = pick
    dims = (2 * total_rows, total_rows)
    row, col = iota(dims, 0), iota(dims, 1)
    target = lax.shift_left(lax.shift_right_logical(row, 3), 2) + (row & 3)
    hit = target == col
    upper = (row & 7) < NEW
    zero, one = jnp.zeros(dims, F32), jnp.ones(dims, F32)
    place_a = jnp.where(hit & upper, one, zero).astype(BF16)
    place_b = jnp.where(hit & ~upper, one, zero).astype(BF16)
    fill = jnp.zeros((LANES - 2 * all_heads, wa_ref.shape[1]), BF16)
    for copy in copies[1:5]:
        copy.wait()
    tokens = tokens_ref[...]
    base_ref[...] = dot(pick, tokens)
    scaled = (tokens.astype(F32) * gain_ref[...]).astype(BF16)
    left = dot(place_a, scaled).astype(BF16)
    right = dot(place_b, scaled).astype(BF16)
    both = dot(place_a + place_b, tokens)
    squares = jnp.sum(both * both, axis=1, keepdims=True)
    small = dot_nt(left + right, jnp.concatenate([wa_ref[...], wb_ref[...], fill], axis=0))
    lane = iota(small.shape, 1)
    small = jnp.where(lane == 2 * all_heads, jnp.broadcast_to(squares, small.shape), small)
    high = small.astype(BF16).astype(F32)
    first = (iota(small.shape, 0) & 7) < NEW

    def put(columns, values):
        out_ref[:, :, columns] = values.reshape(-1, SUBS, values.shape[1]).astype(BF16)

    put(slice(2 * width, 2 * width + LANES), jnp.where(first, high, small - high))
    copies[5].wait()
    copies[6].wait()
    put(slice(0, width), dot(left, wq_ref[...]) + dot(right, wk_ref[...]))
    copies[7].wait()
    copies[8].wait()
    put(slice(width, 2 * width), dot(left, wv_ref[...]) + dot(right, wg_ref[...]))
    deal(out_ref, outs)


def deal(blocks_ref, outs):
    if len(outs) == 1:
        outs[0][...] = blocks_ref[...]
        return
    plane = lax.axis_index("kv") & (PLANE - 1)
    for d, out in enumerate(outs):
        for z in range(out.shape[0]):
            out[z] = blocks_ref[z * PLANE + (plane ^ d)]


def fold_kernel(rows, columns, axis, half, *refs):
    parts, outs = refs[:PLANE], refs[PLANE:]
    high = lax.shift_right_logical(lax.axis_index("kv"), log2(PLANE))
    for e, out in enumerate(outs):
        total = parts[0][high ^ e].astype(F32)
        for part in parts[1:]:
            total = total + part[high ^ e].astype(F32)
        out[...] = total.astype(out.dtype)
        value = total[rows, columns]
        value = value + pltpu.roll(value, half, axis)
        top = value.astype(BF16).astype(F32)
        value = jnp.where(iota(value.shape, axis) < half, top, value - top)
        out[rows, columns] = value.astype(out.dtype)


def partners(values, shift):
    count = lax.axis_size("kv")
    moved = []
    for d in reversed(range(1, len(values))):
        moved.append(lax.ppermute(values[d], "kv", [(i, i ^ (d << shift)) for i in range(count)]))
    return [values[0], *moved]


def staged():
    return lax.axis_size("kv") == PLANE * PLANE


def dealt(dims, kv):
    if staged():
        return [shape((PLANE, *dims), BF16)] * PLANE
    return [shape((kv, *dims), BF16)]


def reduce_scatter(outs, name, *halves, beside=None):
    if not staged():
        return [exchange(outs[0])], beside
    dims = outs[0].shape[1:]
    parts = partners(outs, 0)
    if beside is not None:
        parts, beside = lax.optimization_barrier((parts, beside))
    sums = call(
        functools.partial(fold_kernel, *halves),
        [shape(dims, F32 if e == 0 else BF16) for e in range(PLANE)],
        parts,
        [VMEM] * PLANE,
        8,
        4 << 30,
        name,
    )
    return [x[None] for x in partners(sums, log2(PLANE))], beside


def block_sum(refs, rows, columns):
    total = None
    for ref in refs:
        for i in range(ref.shape[0]):
            term = ref[i, rows, columns].astype(F32)
            total = term if total is None else total + term
    return total


def row_sum(refs, start, columns):
    return block_sum(refs, slice(None), slice(start, start + columns))


def recur_kernel(*refs):
    own_ref, *got_ref = refs[:-16]
    memory_ref, sources, (mixed_out, unit, late, left_ref) = refs[-16], refs[-15:-12], refs[-12:-8]
    gates, vals, preds, copies, *held, sems = refs[-8:]
    log_ref, bias_ref, gain_ref = held
    heads = memory_ref.shape[0]
    fetches = [pltpu.make_async_copy(a, b, sems.at[i]) for i, (a, b) in enumerate(zip(sources, held))]
    for fetch in fetches:
        fetch.start()
    width = heads * DK
    all_heads = heads * lax.axis_size("tp")
    tp_place = lax.axis_index("tp")
    small = row_sum(got_ref, 2 * width, LANES)
    small = small + pltpu.roll(small, NEW, 0)
    rstd = lax.rsqrt(small[:, 2 * all_heads : 2 * all_heads + 1] / D + epsilon)
    gates[...] = jnp.zeros(gates.shape, F32)
    factor = jnp.where(iota((SUBS, 1), 0) < NEW, DK ** (-0.5), 1.0)
    for h in range(heads):
        block = (row_sum(got_ref, h * DK, DK) * rstd).astype(BF16).astype(F32)
        norm = lax.rsqrt(jnp.sum(block * block, axis=1, keepdims=True) + epsilon)
        unit[h * SUBS : (h + 1) * SUBS, :] = block * norm * factor
        vals[h * SUBS : (h + 1) * SUBS, :] = (
            (row_sum(got_ref, width + h * DV, DV) * rstd).astype(BF16).astype(F32)
        )
    for fetch in fetches:
        fetch.wait()
    small = small * rstd
    alphas = pltpu.roll(small, LANES - tp_place * heads, 1)[:, :heads]
    betas = pltpu.roll(small, LANES - all_heads - tp_place * heads, 1)[:, :heads]
    x = alphas + bias_ref[...]
    soft = jnp.maximum(x, 0.0) + jnp.log1p(jnp.exp(-jnp.abs(x)))
    decay = -jnp.exp(log_ref[...]) * soft
    slot = iota(decay.shape, 0)
    live = (slot & 3) < own_ref[:, :heads]
    keep = jnp.exp(jnp.where(live, decay, 0.0))
    write = jnp.where(live, 1.0 / (1.0 + jnp.exp(-betas)), 0.0)
    gates[:SUBS, :heads] = jnp.where(slot < NEW, keep, write)
    turned = gates[...].T
    for h in range(heads):
        own = slice(h * SUBS, (h + 1) * SUBS)
        preds[own, :] = jnp.dot(
            unit[own, :], memory_ref[h], precision=lax.Precision.HIGHEST, preferred_element_type=F32
        )

    def rows(ref, j):
        return ref[pl.ds(j, heads, stride=SUBS), :]

    queries = [rows(unit, t) for t in range(NEW)]
    keys = [rows(unit, NEW + t) for t in range(NEW)]
    keeps = [turned[:heads, t : t + 1] for t in range(NEW)]
    writes = [turned[:heads, NEW + t : NEW + t + 1] for t in range(NEW)]

    def inner(a, b):
        return jnp.sum(a * b, axis=1, keepdims=True)

    updates, outs = [], []
    passed = []
    total = jnp.ones((heads, 1), F32)
    for t in range(NEW):
        total = total * keeps[t]
        passed = [p * keeps[t] for p in passed]
        said = total * rows(preds, NEW + t)
        for i in range(t):
            said = said + (passed[i] * inner(keys[i], keys[t])) * updates[i]
        updates.append(writes[t] * (rows(vals, t) - said))
        passed.append(jnp.ones((heads, 1), F32))
        out = total * rows(preds, t)
        for i in range(t + 1):
            out = out + (passed[i] * inner(keys[i], queries[t])) * updates[i]
        outs.append(out)
    for i in range(NEW):
        late[pl.ds(i, heads, stride=SUBS), :] = jnp.zeros((heads, DV), F32)
        late[pl.ds(NEW + i, heads, stride=SUBS), :] = passed[i] * updates[i]
    left_ref[...] = jnp.broadcast_to(total, left_ref.shape)
    for t, out in enumerate(outs):
        out = out * lax.rsqrt(jnp.mean(out * out, axis=1, keepdims=True) + epsilon)
        gate = rows(vals, NEW + t)
        silu = gate * (1.0 / (1.0 + jnp.exp(-gate)))
        copies[t * heads : (t + 1) * heads, :] = out * gain_ref[...] * silu
    mixed = copies[...].astype(BF16)
    for d in range(mixed_out.shape[0]):
        mixed_out[d] = mixed


def advance_kernel(memory_ref, unit_ref, late_ref, left_ref, out_ref, fresh_ref, sems):
    stores = []
    for h in range(memory_ref.shape[0]):
        own = slice(h * SUBS, (h + 1) * SUBS)
        added = lax.dot_general(
            unit_ref[own, :],
            late_ref[own, :],
            (((0,), (0,)), ((), ())),
            precision=lax.Precision.HIGHEST,
            preferred_element_type=F32,
        )
        fresh_ref[h] = memory_ref[h] * left_ref[h : h + 1, :] + added
        stores.append(pltpu.make_async_copy(fresh_ref.at[h], out_ref.at[h], sems.at[h]))
        stores[-1].start()
    for store in stores:
        store.wait()


def project_kernel(place_ref, mixed_ref, w_ref, out_ref):
    heads = w_ref.shape[0] // DV
    total = mixed_ref.shape[0]
    packed = out_ref.shape[0]
    place = place_ref[...]
    head_of = iota((1, total), 1) & (heads - 1)
    row = iota((packed, total), 0)
    mixed = mixed_ref[...]
    rows = []
    for h in range(heads):
        pick = jnp.where(row == jnp.where(head_of == h, place, -1), 1.0, 0.0).astype(BF16)
        rows.append(dot(pick, mixed).astype(BF16))
    sum_ = None
    for h in range(heads):
        term = dot(rows[h], w_ref[h * DV : (h + 1) * DV, :])
        sum_ = term if sum_ is None else sum_ + term
    out_ref[...] = sum_


def picker(lengths_ref, packed, total_rows):
    col = iota((1, total_rows), 1)
    place = places(lengths_ref, lax.shift_right_logical(col, 2), col & 3)
    return jnp.where(iota((packed, total_rows), 0) == place, 1.0, 0.0).astype(BF16)


class Packing:
    def __init__(self, live, tiles, receivers, members):
        self.members = members
        self.tiles = tiles // members
        self.receivers = receivers // members
        self.shared = 0 < live % SUBS <= SUBS // 2
        self.whole = live // SUBS if self.shared else -(-live // SUBS)
        self.count = self.whole * self.tiles + (-(-self.tiles // 2) if self.shared else 0)
        self.each = -(-self.count // self.receivers)

    def spot(self, block, tile):
        at = block * self.tiles + (tile if block < self.whole else tile // 2)
        return divmod(at, self.each)


def up_kernel(packing, partner, inputs, *refs):
    *terms, base_ref, gain_ref, wg_ref, wu_ref = refs[:inputs]
    out_ref, hidden_out = refs[inputs:]
    packed = hidden_out.shape[0]
    first = 0
    if packing.members > 1:
        member = (lax.axis_index("kv") & (packing.members - 1)) ^ partner
        first = member * (packing.tiles * LANES)
    hidden = base_ref[...]
    for term in terms:
        hidden = hidden + term[...]
    hidden = hidden.astype(BF16)
    hidden_out[...] = hidden
    hidden_f = hidden.astype(F32)
    scaled = (hidden_f * gain_ref[...]).astype(BF16)
    tiles = packing.tiles
    squares = jnp.broadcast_to(jnp.sum(hidden_f * hidden_f, axis=1, keepdims=True), (packed, LANES))
    own_lane = iota(squares.shape, 0) == iota(squares.shape, 1)
    squares = jnp.sum(jnp.where(own_lane, squares, 0.0), axis=0, keepdims=True)
    squares = jnp.broadcast_to(squares, (SUBS, LANES))
    high = squares.astype(BF16).astype(F32)
    halves = jnp.where(iota(squares.shape, 0) < NEW, high, squares - high).astype(BF16)
    step = 4
    for start in range(0, tiles, step):
        stop = min(start + step, tiles)
        span = pl.ds(pl.multiple_of(first + start * LANES, LANES), (stop - start) * LANES)
        gate = dot(scaled, wg_ref[:, span])
        up = dot(scaled, wu_ref[:, span])
        for t in range(start, stop):
            lanes = slice((t - start) * LANES, (t - start + 1) * LANES)
            for b in range(packed // SUBS):
                rows = slice(b * SUBS, (b + 1) * SUBS)
                one, two = gate[rows, lanes], up[rows, lanes]
                if b == packing.whole:
                    if t % 2 == 0 and t + 1 < tiles:
                        held = one, two
                        continue
                    if t % 2:
                        one = held[0] + pltpu.roll(one, SUBS // 2, 0)
                        two = held[1] + pltpu.roll(two, SUBS // 2, 0)
                d, i = packing.spot(b, t)
                out_ref[d, i * 16 : i * 16 + 16, :] = jnp.concatenate([one, two], axis=0).astype(BF16)
    for at in range(packing.count, out_ref.shape[0] * packing.each):
        d, i = divmod(at, packing.each)
        out_ref[d, i * 16 : i * 16 + 16, :] = jnp.zeros((16, LANES), BF16)
    for d in range(out_ref.shape[0]):
        out_ref[d, packing.each * 16 :, :] = halves


def active_kernel(packing, *refs):
    *got, out_ref = refs
    end = packing.each * 16
    squares = block_sum(got, slice(end, end + SUBS), slice(None))
    squares = squares + pltpu.roll(squares, SUBS // 2, 0)
    rstd = lax.rsqrt(squares / D + epsilon)
    row, lane = iota(rstd.shape, 0), iota(rstd.shape, 1)
    first = lax.shift_right_logical(lax.axis_index("kv"), log2(packing.members)) * packing.each
    for i in range(packing.each):
        block = lax.div(first + i, packing.tiles)
        row_of = block * SUBS + row
        if packing.shared:
            row_of = jnp.where(block >= packing.whole, packing.whole * SUBS + (row & (SUBS // 2 - 1)), row_of)
        scale = jnp.sum(jnp.where(lane == row_of, rstd, 0.0), axis=1, keepdims=True)
        pair = block_sum(got, slice(i * 16, i * 16 + 16), slice(None))
        gate, up = pair[:SUBS] * scale, pair[SUBS:] * scale
        active = (gate * (1.0 / (1.0 + jnp.exp(-gate))) * up).astype(BF16)
        for d in range(out_ref.shape[0]):
            out_ref[d, i * SUBS : (i + 1) * SUBS, :] = active


def down_kernel(packing, got_ref, w_ref, out_ref):
    packed = out_ref.shape[0]
    tiles = w_ref.shape[0] // LANES
    sum_ = None
    for t in range(tiles):
        parts = []
        for b in range(packed // SUBS):
            member, tile = divmod(t, packing.tiles)
            receiver, i = packing.spot(b, tile)
            d = receiver * packing.members + member
            part = got_ref[d, i * SUBS : (i + 1) * SUBS, :].astype(F32)
            parts.append(pltpu.roll(part, SUBS // 2, 0) if b == packing.whole and tile % 2 else part)
        term = dot(jnp.concatenate(parts, axis=0).astype(BF16), w_ref[t * LANES : (t + 1) * LANES, :])
        sum_ = term if sum_ is None else sum_ + term
    out_ref[...] = sum_


def last_kernel(*refs):
    *terms, hidden_ref, pick_ref, out_ref = refs
    result = terms[0][...]
    for term in terms[1:]:
        result = result + term[...]
    result = (hidden_ref[...].astype(F32) + result).astype(BF16)
    out_ref[...] = lax.dot_general(
        pick_ref[...], result, (((0,), (0,)), ((), ())), preferred_element_type=F32
    ).astype(BF16)


def exchange(blocks):
    return lax.all_to_all(blocks, "kv", 0, 0)


def over_tp(terms):
    if lax.axis_size("tp") == 2:
        return [terms, lax.ppermute(terms, "tp", [(0, 1), (1, 0)])]
    return [lax.psum(terms, "tp")]


def per_device(
    tokens,
    lengths,
    memory,
    norm_gain,
    w_query,
    w_key,
    w_value,
    w_outgate,
    w_alpha,
    w_beta,
    decay_log,
    decay_bias,
    head_gain,
    w_output,
    mlp_gain,
    w_gate,
    w_up,
    w_down,
):
    total_rows, own_width = tokens.shape
    kv = lax.axis_size("kv")
    seq_dev, heads = memory.shape[:2]
    assert seq_dev == 1
    width = heads * DK
    sequences = lengths.shape[0]
    units = w_gate.shape[1]
    live = sequences * 7 // 4
    packed = -(-live // SUBS) * SUBS
    assert packed <= LANES
    packing = Packing(live, units // LANES, kv, PLANE if staged() else 1)
    assert units % (packing.members * LANES) == 0
    columns = 2 * width + LANES

    operands = [lengths, tokens, norm_gain[None], w_alpha.T, w_beta.T, w_query, w_key, w_value, w_outgate]
    *sent, base, pick, place, own = call(
        functools.partial(front_kernel, heads),
        [
            *dealt((SUBS, columns), kv),
            shape((packed, own_width), F32),
            shape((packed, total_rows), BF16),
            shape((1, kv * NEW * heads), jnp.int32),
            shape((SUBS, LANES), jnp.int32),
        ],
        operands,
        [HBM] * len(operands),
        16,
        4 * total_rows * own_width * 4 * width,
        "front",
        [pltpu.SMEM(lengths.shape, jnp.int32), *(room(x) for x in operands[1:]), pltpu.SemaphoreType.DMA((len(operands),)), pltpu.VMEM((kv, SUBS, columns), BF16)],
    )
    got, _ = reduce_scatter(sent, "fold_rows", slice(None), slice(2 * width, columns), 0, NEW)
    sent, unit, late, left = call(
        recur_kernel,
        [
            shape((kv, NEW * heads, DV), BF16),
            shape((heads * SUBS, DK), F32),
            shape((heads * SUBS, DV), F32),
            shape((heads, DV), F32),
        ],
        [own, *got, memory[0], decay_log[None], decay_bias[None], head_gain[None]],
        [VMEM] * (2 + len(got)) + [HBM] * 3,
        16,
        4 << 30,
        "recur",
        [
            pltpu.VMEM((LANES, LANES), F32),
            pltpu.VMEM((heads * SUBS, DV), F32),
            pltpu.VMEM((heads * SUBS, DV), F32),
            pltpu.VMEM((NEW * heads, DV), F32),
            pltpu.VMEM((1, heads), F32),
            pltpu.VMEM((1, heads), F32),
            pltpu.VMEM((1, DV), F32),
            pltpu.SemaphoreType.DMA((3,)),
        ],
    )
    (new_memory,) = call(
        advance_kernel,
        [shape((heads, DK, DV), F32)],
        [memory[0], unit, late, left],
        [VMEM] * 4,
        8,
        1 << 30,
        "advance",
        [pltpu.VMEM((heads, DK, DV), F32), pltpu.SemaphoreType.DMA((heads,))],
        [HBM],
    )
    got = exchange(sent).reshape(kv * NEW * heads, DV)
    (attn,) = call(
        project_kernel,
        [shape((packed, own_width), F32)],
        [place, got, w_output],
        [VMEM] * 3,
        8,
        32 << 20,
        "project",
    )
    terms = over_tp(attn)
    outs = [
        shape((packing.receivers, packing.each * 16 + SUBS, LANES), BF16),
        shape((packed, own_width), BF16),
    ]
    sent = []
    for d in range(packing.members):
        part, hidden = call(
            functools.partial(up_kernel, packing, d, len(terms) + 4),
            outs,
            [*terms, base, mlp_gain[None], w_gate, w_up],
            [VMEM] * (len(terms) + 4),
            16,
            4 * packed * own_width * units // packing.members,
            f"up_{d}",
        )
        sent.append(part)
    got, new_memory = reduce_scatter(
        sent, "fold_units", slice(packing.each * 16, None), slice(None), 0, NEW, beside=new_memory
    )
    (sent,) = call(
        functools.partial(active_kernel, packing),
        [shape((kv, packing.each * SUBS, LANES), BF16)],
        got,
        [VMEM] * len(got),
        8,
        1 << 20,
        "active",
    )
    got = exchange(sent)
    (feed,) = call(
        functools.partial(down_kernel, packing),
        [shape((packed, own_width), F32)],
        [got, w_down],
        [VMEM] * 2,
        16,
        2 * packed * own_width * units,
        "down",
    )
    terms = over_tp(feed)
    (layer_out,) = call(
        last_kernel,
        [shape((total_rows, own_width), BF16)],
        [*terms, hidden, pick],
        [VMEM] * (len(terms) + 2),
        8,
        1 << 20,
        "last",
    )
    return (layer_out, new_memory[None])


def solution(mesh):
    placed = (
        P(None, "kv"),
        P(),
        P("kv", "tp", None, None),
        P("kv"),
        P("kv", "tp"),
        P("kv", "tp"),
        P("kv", "tp"),
        P("kv", "tp"),
        P("kv", None),
        P("kv", None),
        P("tp"),
        P("tp"),
        P(),
        P("tp", "kv"),
        P("kv"),
        P("kv", "tp"),
        P("kv", "tp"),
        P("tp", "kv"),
    )
    return jax.shard_map(
        per_device,
        mesh=mesh,
        in_specs=placed,
        out_specs=(P(None, "kv"), P("kv", "tp", None, None)),
        check_vma=False,
    )
```
